32 devices in a mesh: sp: 16 (over z, y, x), tp: 2 (over core).
Axes of the slice: x: 2, y: 2, z: 4, core: 2. Of those that a mesh axis runs over, the one named last changes fastest.
Arguments:
- tokens: bfloat16 [4096, 2048], P('sp', 'tp'), may hold values from -6 to 6
- norm_gain: float32 [2048], replicated, may hold values from 0.1 to 1.9
- query_weight: bfloat16 [2048, 1024], P(None, 'tp'), may hold values from -0.18782524 to 0.18782524
- key_weight: bfloat16 [2048, 1024], P(None, 'tp'), may hold values from -0.18782524 to 0.18782524
- value_weight: bfloat16 [2048, 1024], P(None, 'tp'), may hold values from -0.125 to 0.125
- gate_weight: bfloat16 [2048, 1024], P(None, 'tp'), may hold values from -0.125 to 0.125
- outer_weight: bfloat16 [2048, 1024], P(None, 'tp'), may hold values from -0.125 to 0.125
- inner_weight: bfloat16 [2048, 1024], P(None, 'tp'), may hold values from -0.125 to 0.125
- signal_weight: bfloat16 [2048, 1024], P(None, 'tp'), may hold values from -0.125 to 0.125
- conv_taps: float32 [3, 1024], P(None, 'tp'), may hold values from -3.5 to 3.5
- lambdas: float32 [8], P('tp'), may hold values from 0.3 to 0.8
- head_gain: float32 [1024], P('tp'), may hold values from 0.1 to 1.9
- attn_out_weight: bfloat16 [1024, 2048], P('tp'), may hold values from -0.125 to 0.125
- conv_out_weight: bfloat16 [1024, 2048], P('tp'), may hold values from -0.125 to 0.125
Outputs:
- mixed: bfloat16 [4096, 2048], P(('sp', 'tp'))
- log_totals: float32 [8, 2, 4096], P('tp', None, 'sp')
The draws below stay inside these ranges and needn't reach their ends.
All inputs are finite; a program needn't handle non-finite values.
Results may differ from the reference program's by a relative error of at most 0.014.
Values may be sent and summed in bfloat16 or wider, within the bound.
A program may use at most 128 MiB of HBM per device.

```python
import jax
import jax.numpy as jnp
from jax import lax

D = 2048
HEADS = 8
QK = 64
VD = 128
CONV = 1024
KERNEL = 3
TOKENS = 4096
N_TP = 2


def projection_pair(key):
    columns = HEADS * 2 * QK
    spread = 1.4 * D ** (-0.5)
    query_part = jnp.clip(jax.random.normal(jax.random.fold_in(key, 101), (D, columns), jnp.float32), -6.0, 6.0) * spread
    key_part = jnp.clip(jax.random.normal(jax.random.fold_in(key, 102), (D, columns), jnp.float32), -6.0, 6.0) * spread
    return (query_part, key_part)


def draw_query_weight(key, part):
    return projection_pair(key)[0].astype(jnp.bfloat16)


def draw_key_weight(key, part):
    return projection_pair(key)[1].astype(jnp.bfloat16)


def draw_tokens(key, part):
    base = jnp.clip(jax.random.normal(jax.random.fold_in(key, 201), (TOKENS, D), jnp.float32), -6.0, 6.0)
    return base.astype(jnp.bfloat16)


def steps_of(own_key, extent, cuts, smallest, high):
    def one(axis_at, parts):
        heights = jax.random.uniform(jax.random.fold_in(jax.random.fold_in(own_key, 6), axis_at), (parts,), jnp.float32, smallest / len(cuts), high / len(cuts))
        return jnp.repeat(jnp.exp(heights), extent[axis_at] // parts).reshape((-1,) + (1,) * (len(extent) - axis_at - 1))

    loudness = one(*cuts[0])
    for cut in cuts[1:]:
        loudness = loudness * one(*cut)
    return loudness


def noise(key, shape, scale, reach, split=(), kind=jnp.bfloat16):
    factor_of = steps_of(key, shape, split, -0.22, 0.18) if split else 1.0
    array = jax.random.normal(key, shape, jnp.float32) * scale * factor_of
    return jnp.minimum(jnp.maximum(array, -reach), reach).astype(kind)


def setup_inputs(seed: int = 0) -> dict:
    arg_keys = jax.random.split(jax.random.key(seed), 15)
    tokens = draw_tokens(jax.random.fold_in(arg_keys[14], 71), 0)
    norm_gain = jnp.clip(1.0 + 0.18 * jax.random.normal(arg_keys[1], (D,), jnp.float32), 0.1, 1.9)
    query_weight = draw_query_weight(jax.random.fold_in(arg_keys[14], 71), 0)
    key_weight = draw_key_weight(jax.random.fold_in(arg_keys[14], 71), 0)
    value_weight = noise(arg_keys[4], (D, HEADS * VD), D ** -0.5, 0.125, ((1, 2),))
    gate_weight = noise(arg_keys[5], (D, HEADS * VD), D ** -0.5, 0.125, ((1, 2),))
    outer_weight = noise(arg_keys[6], (D, CONV), D ** -0.5, 0.125, ((1, 2),))
    inner_weight = noise(arg_keys[7], (D, CONV), D ** -0.5, 0.125, ((1, 2),))
    signal_weight = noise(arg_keys[8], (D, CONV), D ** -0.5, 0.125, ((1, 2),))
    conv_taps = noise(arg_keys[9], (KERNEL, CONV), KERNEL ** -0.5, 3.5, ((1, 2),), jnp.float32)
    lambdas = jnp.clip(0.3 + 0.5 * jax.random.uniform(arg_keys[10], (HEADS,), jnp.float32) ** steps_of(arg_keys[10], (HEADS,), ((0, 2),), -0.2, 0.2), 0.3, 0.8)
    head_gain = jnp.clip(1.0 + 0.18 * jax.random.normal(arg_keys[11], (HEADS * VD,), jnp.float32), 0.1, 1.9)
    attn_out_weight = noise(arg_keys[12], (HEADS * VD, D), (HEADS * VD + CONV) ** -0.5, 0.125, ((0, 2),))
    conv_out_weight = noise(arg_keys[13], (CONV, D), (HEADS * VD + CONV) ** -0.5, 0.125, ((0, 2),))
    return dict(tokens=tokens, norm_gain=norm_gain, query_weight=query_weight, key_weight=key_weight, value_weight=value_weight, gate_weight=gate_weight, outer_weight=outer_weight, inner_weight=inner_weight, signal_weight=signal_weight, conv_taps=conv_taps, lambdas=lambdas, head_gain=head_gain, attn_out_weight=attn_out_weight, conv_out_weight=conv_out_weight)


def reference(tokens, norm_gain, query_weight, key_weight, value_weight, gate_weight, outer_weight, inner_weight, signal_weight, conv_taps, lambdas, head_gain, attn_out_weight, conv_out_weight):
    tokens_f = tokens.astype(jnp.float32)
    scale = lax.rsqrt(lax.optimization_barrier(jnp.mean(tokens_f * tokens_f, axis=-1, keepdims=True)) + 1e-06)
    normed_in = (tokens_f * norm_gain).astype(jnp.bfloat16)

    def project(weight):
        return (jnp.dot(normed_in.astype(jnp.float32), weight.astype(jnp.float32), preferred_element_type=jnp.float32) * scale).astype(jnp.bfloat16)
    query = project(query_weight)
    key = project(key_weight)
    value = project(value_weight)
    attn_gate = project(gate_weight)
    outer = project(outer_weight)
    inner = project(inner_weight)
    signal = project(signal_weight)
    query_heads = query.reshape(TOKENS, HEADS, 2, QK)
    key_heads = key.reshape(TOKENS, HEADS, 2, QK).astype(jnp.float32)
    value_heads = value.reshape(TOKENS, HEADS, VD).astype(jnp.float32)
    block_rows = 256 if TOKENS % 256 == 0 else 128
    key_pos = jnp.arange(TOKENS, dtype=jnp.int32)

    def one_block(index):
        query_block = lax.dynamic_slice_in_dim(query_heads, (index * block_rows).astype(jnp.int32), block_rows, 0).astype(jnp.float32)
        query_pos = index * block_rows + jnp.arange(block_rows, dtype=jnp.int32)
        score = jnp.einsum('qhmd,khmd->hmqk', query_block, key_heads) * QK ** (-0.5)
        visible = query_pos[:, None] >= key_pos[None, :]
        score = jnp.where(visible, score, -1e+30)
        top = lax.optimization_barrier(jnp.max(score, axis=-1, keepdims=True))
        weights = jnp.exp(score - top)
        total = lax.optimization_barrier(jnp.sum(weights, axis=-1, keepdims=True))
        summed = jnp.einsum('hmqk,khd->hmqd', weights.astype(jnp.bfloat16).astype(jnp.float32), value_heads)
        mapped = summed / total
        diff = mapped[:, 0] - lambdas[:, None, None] * mapped[:, 1]
        log_total = jnp.log(total[..., 0]) + top[..., 0]
        return (jnp.transpose(diff, (1, 0, 2)), log_total)
    diffs, log_parts = lax.map(one_block, jnp.arange(TOKENS // block_rows, dtype=jnp.int32))
    diff = diffs.reshape(TOKENS, HEADS, VD)
    log_totals = jnp.transpose(log_parts, (1, 2, 0, 3)).reshape(HEADS, 2, TOKENS)
    normed = diff * lax.rsqrt(lax.optimization_barrier(jnp.mean(diff * diff, axis=-1, keepdims=True)) + 1e-05) * head_gain.reshape(HEADS, VD)
    head_out = (normed.reshape(TOKENS, HEADS * VD) * jax.nn.silu(attn_gate.astype(jnp.float32))).astype(jnp.bfloat16)
    inner_sig = (inner.astype(jnp.float32) * signal.astype(jnp.float32)).astype(jnp.bfloat16)
    padded = jnp.pad(inner_sig.astype(jnp.float32), ((KERNEL - 1, 0), (0, 0)))
    convolved = jnp.zeros((TOKENS, CONV), jnp.float32)
    for offset in range(KERNEL):
        convolved = convolved + conv_taps[offset] * padded[offset:offset + TOKENS]
    conv_out = (outer.astype(jnp.float32) * convolved).astype(jnp.bfloat16)
    head_cols = HEADS * VD // N_TP
    conv_cols = CONV // N_TP

    def add_group(accum, group):
        head_part = lax.dynamic_slice_in_dim(head_out, (group * head_cols).astype(jnp.int32), head_cols, 1)
        head_rows = lax.dynamic_slice_in_dim(attn_out_weight, (group * head_cols).astype(jnp.int32), head_cols, 0)
        conv_part = lax.dynamic_slice_in_dim(conv_out, (group * conv_cols).astype(jnp.int32), conv_cols, 1)
        conv_rows = lax.dynamic_slice_in_dim(conv_out_weight, (group * conv_cols).astype(jnp.int32), conv_cols, 0)
        partial_value = jnp.dot(head_part.astype(jnp.float32), head_rows.astype(jnp.float32), preferred_element_type=jnp.float32) + jnp.dot(conv_part.astype(jnp.float32), conv_rows.astype(jnp.float32), preferred_element_type=jnp.float32)
        rounded = lax.optimization_barrier(partial_value.astype(jnp.bfloat16))
        return (accum + rounded.astype(jnp.float32), None)
    accum, _ = lax.scan(add_group, jnp.zeros((TOKENS, D), jnp.float32), jnp.arange(N_TP, dtype=jnp.int32))
    return (accum.astype(jnp.bfloat16), log_totals)
```

```python
import functools
import math

import jax
import jax.numpy as jnp
from jax import lax
from jax.experimental import pallas as pl
from jax.experimental.pallas import tpu as pltpu
from jax.sharding import PartitionSpec as P

MESH = pl.DeviceIdType.MESH


def passed_along(shard, axis, by):
    count = lax.axis_size(axis)
    pairs = [(i, i + by) for i in range(count) if 0 <= i + by < count]
    return lax.ppermute(shard, axis, pairs)


def per_device(
    tokens,
    norm_gain,
    query_weight,
    key_weight,
    value_weight,
    gate_weight,
    outer_weight,
    inner_weight,
    signal_weight,
    conv_taps,
    lambdas,
    head_gain,
    attn_out_weight,
    conv_out_weight,
):
    row_count = tokens.shape[0]
    width = norm_gain.shape[0]
    weights = [
        query_weight,
        key_weight,
        value_weight,
        gate_weight,
        outer_weight,
        inner_weight,
        signal_weight,
    ]
    splits = []
    running = 0
    for weight in weights[:-1]:
        running = running + weight.shape[1]
        splits.append(running)
    joined = jnp.concatenate(weights, axis=1)
    empty = jnp.zeros((row_count, joined.shape[1]), jnp.float32)
    piece = lax.all_gather(tokens, "tp", axis=1, tiled=True)
    summed = empty
    piece_f = piece.astype(jnp.float32)
    normed_piece = (piece.astype(jnp.float32) * norm_gain).astype(jnp.bfloat16)
    raw = jnp.dot(normed_piece, joined, preferred_element_type=jnp.float32)
    squares = jnp.sum(piece_f * piece_f, axis=-1)
    scale = lax.rsqrt(squares / width + 1e-06)
    projected = (raw * scale[:, None]).astype(jnp.bfloat16)
    query, key, value, attn_gate, outer, inner, signal = jnp.split(projected, splits, axis=1)
    head_count = lambdas.shape[0]
    key_size = query_weight.shape[1] // (head_count * 2)
    value_size = value_weight.shape[1] // head_count
    score_scale = key_size ** (-0.5)
    own_index = lax.axis_index("sp")
    local_pos = jnp.arange(row_count, dtype=jnp.int32)
    query_parts = [query]
    position_parts = [own_index * row_count + local_pos]
    query_parts = [
        segment.reshape(segment.shape[0], head_count, 2, key_size) for segment in query_parts
    ]

    def absorb(current, query_rows, row_pos, key_block, value_block, key_pos):
        running_max, summed, accum = current
        score = (
            jnp.einsum("qhmd,khmd->hmqk", query_rows, key_block, preferred_element_type=jnp.float32)
            * score_scale
        )
        visible = row_pos[:, None] >= key_pos[None, :]
        masked = jnp.where(visible, score, -1e30)
        new_max = jnp.maximum(running_max, jnp.max(masked, axis=-1, keepdims=True))
        weights_now = jnp.where(visible, jnp.exp(masked - new_max), 0.0)
        factor = jnp.exp(running_max - new_max)
        summed = summed * factor + jnp.sum(weights_now, axis=-1, keepdims=True)
        accum = accum * factor + jnp.einsum(
            "hmqk,khd->hmqd",
            weights_now.astype(jnp.bfloat16),
            value_block,
            preferred_element_type=jnp.float32,
        )
        return (new_max, summed, accum)

    def fresh(rows):
        return (
            jnp.full((head_count, 2, rows, 1), -1e30, jnp.float32),
            jnp.zeros((head_count, 2, rows, 1), jnp.float32),
            jnp.zeros((head_count, 2, rows, value_size), jnp.float32),
        )

    start_states = tuple((fresh(segment.shape[0]) for segment in query_parts))
    carry = start_states
    key_piece = lax.all_gather(key, "sp", axis=0, tiled=True)
    value_piece = lax.all_gather(value, "sp", axis=0, tiled=True)
    length = key_piece.shape[0]
    block_len = 512
    key_blocks = key_piece.reshape(length // block_len, block_len, head_count, 2, key_size)
    value_blocks = value_piece.reshape(length // block_len, block_len, head_count, value_size)

    def one_block(states, item):
        key_block, value_block, block_id = item
        first_key = block_id * block_len
        key_pos = first_key + jnp.arange(block_len, dtype=jnp.int32)
        updated = []
        for current, query_rows, row_pos in zip(states, query_parts, position_parts):

            def compute(held, query_rows=query_rows, row_pos=row_pos):
                return absorb(held, query_rows, row_pos, key_block, value_block, key_pos)

            def unchanged(held):
                return held

            updated.append(
                lax.cond(first_key <= row_pos[row_pos.shape[0] - 1], compute, unchanged, current)
            )
        return (tuple(updated), None)

    carry, _ = lax.scan(
        one_block,
        carry,
        (key_blocks, value_blocks, jnp.arange(length // block_len, dtype=jnp.int32)),
    )
    states = carry
    running_max = jnp.concatenate([held[0] for held in states], axis=2)
    summed = jnp.concatenate([held[1] for held in states], axis=2)
    accum = jnp.concatenate([held[2] for held in states], axis=2)
    mapped = accum / summed
    diff = mapped[:, 0] - lambdas[:, None, None] * mapped[:, 1]
    log_totals = jnp.log(summed[..., 0]) + running_max[..., 0]
    diff = jnp.transpose(diff, (1, 0, 2))
    normed = (
        diff
        * lax.rsqrt(jnp.mean(diff * diff, axis=-1, keepdims=True) + 1e-05)
        * head_gain.reshape(head_count, value_size)
    )
    normed = normed.reshape(row_count, head_count * value_size)
    head_out = (normed * jax.nn.silu(attn_gate.astype(jnp.float32))).astype(jnp.bfloat16)
    taps = conv_taps.shape[0]
    inner_sig = (inner.astype(jnp.float32) * signal.astype(jnp.float32)).astype(jnp.bfloat16)
    before = passed_along(inner_sig[row_count - (taps - 1) :], "sp", 1)
    extended = jnp.concatenate([before, inner_sig], axis=0).astype(jnp.float32)
    convolved = jnp.zeros((row_count, inner_sig.shape[1]), jnp.float32)
    for position in range(taps):
        convolved = convolved + conv_taps[position] * extended[position : position + row_count]
    conv_out = (outer.astype(jnp.float32) * convolved).astype(jnp.bfloat16)
    mixed = lax.psum_scatter(
        (
            jnp.dot(head_out, attn_out_weight, preferred_element_type=jnp.float32)
            + jnp.dot(conv_out, conv_out_weight, preferred_element_type=jnp.float32)
        ).astype(jnp.bfloat16),
        "tp",
        scatter_dimension=0,
        tiled=True,
    )
    return (mixed, log_totals)


RELAY = 4


def fused_kernel(
    sp_count,
    heads,
    tokens_hbm,
    gain_hbm,
    wq_hbm,
    wk_hbm,
    wv_hbm,
    wg_hbm,
    wouter_hbm,
    winner_hbm,
    wsignal_hbm,
    taps_hbm,
    lambdas_hbm,
    head_gain_hbm,
    wo_hbm,
    wc_hbm,
    mixed_ref,
    totals_ref,
    own_tokens,
    other_tokens,
    gain_ref,
    taps_ref,
    head_gain_ref,
    lam_own,
    lam_other,
    normed,
    w_vmem,
    wo_vmem,
    wc_vmem,
    kv_send,
    q_send,
    kv_all,
    q_all,
    row_max,
    accum,
    opened,
    outer,
    inner_sig,
    tail_in,
    extended,
    conv_out,
    head_out,
    conv_part,
    o_send,
    o_all,
    lt_send,
    lt_all,
    part_send,
    part_recv,
    w_sem,
    in_sem,
    tok_sem,
    tail_sem,
    part_sem,
    stage_s,
    stage_r,
    q_s,
    q_r,
    x_s,
    x_r,
    c_s,
    c_r,
    d_s,
    d_r,
    o_s,
    o_r,
    lt_s,
    lt_r,
    pair_sem,
    met_sem,
):
    rows, half = own_tokens.shape
    width = 2 * half
    local = wq_hbm.shape[1]
    lanes = local // heads
    s = lax.axis_index("sp")
    t = lax.axis_index("tp")
    plane = s // RELAY
    place = lax.rem(s, RELAY)
    y = place // 2
    x = lax.rem(place, 2)
    member = 2 * t + x
    home = t == y
    low = plane < heads // 2
    last = sp_count - 1

    def at(sp_index, tp_index=None):
        return {"sp": sp_index, "tp": t if tp_index is None else tp_index}

    def remote(src, dst, send_sem, recv_sem, device):
        return pltpu.make_async_remote_copy(
            src_ref=src,
            dst_ref=dst,
            send_sem=send_sem,
            recv_sem=recv_sem,
            device_id=device,
            device_id_type=MESH,
        )

    def worker(j):
        return at(j * RELAY + member, y)

    x_sp = s + 1 - 2 * x
    x_dev = at(x_sp)
    c_dev = at(s, 1 - t)

    small = [
        pltpu.make_async_copy(ref, dst, in_sem.at[i])
        for i, (ref, dst) in enumerate(
            [
                (tokens_hbm, own_tokens),
                (gain_hbm, gain_ref),
                (lambdas_hbm, lam_own),
                (taps_hbm, taps_ref),
                (head_gain_hbm, head_gain_ref),
            ]
        )
    ]
    for copy in small:
        copy.start()
    sources = [wq_hbm, wk_hbm, wv_hbm, winner_hbm, wsignal_hbm, wouter_hbm, wg_hbm]
    weight_copies = [
        pltpu.make_async_copy(ref, w_vmem.at[i], w_sem.at[i]) for i, ref in enumerate(sources)
    ]
    weight_copies.append(pltpu.make_async_copy(wc_hbm, wc_vmem, w_sem.at[len(sources)]))
    weight_copies.append(pltpu.make_async_copy(wo_hbm, wo_vmem, w_sem.at[len(sources) + 1]))
    for copy in weight_copies:
        copy.start()

    barrier = pltpu.get_barrier_semaphore()

    def signal(sem, device):
        pl.semaphore_signal(sem, inc=1, device_id=device, device_id_type=MESH)

    def greet(sp_index):
        signal(barrier, at(sp_index, 1))

    @pl.when(t == 1)
    def _():
        signal(barrier, at(s, 0))

    for step in range(1, heads):
        greet(lax.rem(plane + step, heads) * RELAY + member)

    @pl.when(t != y)
    def _():
        greet(plane * RELAY + member)

    greet(x_sp)

    @pl.when(s < last)
    def _():
        greet(s + 1)

    @pl.when(s > 0)
    def _():
        greet(s - 1)

    @pl.when(t == 0)
    def _():
        pl.semaphore_wait(barrier, 1)
        signal(pair_sem, at(s, 1))

    @pl.when(t == 1)
    def _():
        pl.semaphore_wait(pair_sem, 1)

    greetings = (
        2 * heads + 1 + 2 * jnp.where(s > 0, 1, 0) + 2 * jnp.where(s < last, 1, 0)
    )

    def meet():
        @pl.when(t == 1)
        def _():
            pl.semaphore_wait(barrier, greetings)
            signal(met_sem, at(s, 0))

        @pl.when(t == 0)
        def _():
            pl.semaphore_wait(met_sem, 1)

    small[0].wait()
    tokens_out = remote(own_tokens, other_tokens, tok_sem.at[0], tok_sem.at[1], c_dev)
    tokens_out.start()
    small[2].wait()
    lam_out = remote(lam_own, lam_other, tok_sem.at[2], tok_sem.at[3], c_dev)
    lam_out.start()

    row_max[...] = jnp.full(row_max.shape, -1e30, jnp.float32)
    accum[...] = jnp.zeros(accum.shape, jnp.float32)

    small[1].wait()
    mine = pl.ds(pl.multiple_of(t * half, half), half)
    theirs = pl.ds(pl.multiple_of((1 - t) * half, half), half)
    own_f = own_tokens[...].astype(jnp.float32)
    squares = jnp.sum(own_f * own_f, axis=-1, keepdims=True)
    normed[:, mine] = (own_f * gain_ref[:, mine]).astype(jnp.bfloat16)
    tokens_out.wait()
    other_f = other_tokens[...].astype(jnp.float32)
    squares = squares + jnp.sum(other_f * other_f, axis=-1, keepdims=True)
    normed[:, theirs] = (other_f * gain_ref[:, theirs]).astype(jnp.bfloat16)
    scale = lax.rsqrt(squares / width + 1e-06)

    def project(index):
        weight_copies[index].wait()
        raw = jnp.dot(normed[...], w_vmem[index], preferred_element_type=jnp.float32)
        return (raw * scale).astype(jnp.bfloat16)

    started = []

    def launch(copy):
        copy.start()
        started.append(copy)

    def farthest_first(i):
        down = heads - 1 - i
        down = down - jnp.where(down <= plane, 1, 0)
        up = i + jnp.where(i >= plane, 1, 0)
        return jnp.where(low, down, up)

    def q_copy(j):
        return remote(q_send.at[j], q_all.at[plane], q_s.at[j], q_r.at[plane], worker(j))

    def kv_copy(j):
        return remote(kv_send.at[j], kv_all.at[s], stage_s.at[j], stage_r.at[plane], worker(j))

    def send_all(copy_of):
        @pl.when(t != y)
        def _():
            copy_of(plane).start()

        for i in range(heads - 1):
            copy_of(farthest_first(i)).start()

    def drain_all(copy_of):
        for i in range(heads - 1):
            copy_of(farthest_first(i)).wait_send()

        @pl.when(t != y)
        def _():
            copy_of(plane).wait_send()

    projected = project(0)
    for h in range(heads):
        q_send[h] = projected[:, h * lanes : (h + 1) * lanes]

    @pl.when(home)
    def _():
        q_all[plane] = q_send[plane]

    @pl.when(plane >= heads // 2)
    def _():
        meet()
        send_all(q_copy)

    for index in range(2):
        projected = project(1 + index)
        for h in range(heads):
            kv_send[h, :, index * lanes : (index + 1) * lanes] = projected[
                :, h * lanes : (h + 1) * lanes
            ]

    @pl.when(home)
    def _():
        kv_all[s] = kv_send[plane]

    @pl.when(low)
    def _():
        meet()

    send_all(kv_copy)

    @pl.when(low)
    def _():
        send_all(q_copy)

    order = [jnp.where(k <= plane, plane - k, k) for k in range(heads)]

    def block(plane_index, which):
        return kv_all.at[plane_index * RELAY + which]

    def arrived(dst, recv_sem):
        remote(dst, dst, stage_s.at[0], recv_sem, x_dev).wait_recv()

    def forward_stage(k):
        c = order[k]
        here = block(c, member)
        if k == 0:

            @pl.when(t != y)
            def _():
                arrived(here, stage_r.at[c])

        else:
            arrived(here, stage_r.at[c])
        launch(remote(here, here, x_s.at[k], x_r.at[c], x_dev))
        launch(remote(here, here, c_s.at[k], c_r.at[c], c_dev))

    def forward_square(k):
        c = order[k]
        from_x = block(c, member + 1 - 2 * x)
        arrived(from_x, x_r.at[c])
        launch(remote(from_x, from_x, d_s.at[k], d_r.at[c], c_dev))

    def finish_plane(k):
        c = order[k]
        arrived(block(c, lax.rem(member + 2, RELAY)), c_r.at[c])
        arrived(block(c, RELAY - 1 - member), d_r.at[c])

    inner = project(3).astype(jnp.float32)
    signal_f = project(4).astype(jnp.float32)
    inner_sig[...] = (inner * signal_f).astype(jnp.bfloat16)
    tail = tail_in.shape[0]
    tail_copy = remote(
        inner_sig.at[pl.ds(rows - tail, tail)],
        tail_in,
        tail_sem.at[0],
        tail_sem.at[1],
        at(lax.rem(s + 1, sp_count)),
    )

    @pl.when(s < last)
    def _():
        tail_copy.start()

    forward_stage(0)
    small[4].wait()
    outer[...] = project(5)
    gate = project(6).astype(jnp.float32)
    opened[...] = gate / (1.0 + jnp.exp(-gate)) * head_gain_ref[...]
    forward_square(0)

    exponent = (lanes // 2) ** (-0.5) * math.log2(math.e)
    span = RELAY * rows
    lane = lax.broadcasted_iota(jnp.int32, (1, lanes), 1)
    masks = [
        of_map.astype(jnp.float32).astype(jnp.bfloat16)
        for of_map in (lane < lanes // 2, lane >= lanes // 2)
    ]

    def attend(qi, c, masked):
        held = kv_all[pl.ds(c * RELAY, RELAY)].reshape(span, 2 * lanes)
        keys = held[:, :lanes]
        values = jnp.concatenate(
            [held[:, lanes:], jnp.ones((span, lanes), jnp.bfloat16)], axis=1
        )
        both = q_all[qi]
        for m in range(2):
            score = (
                lax.dot_general(
                    both * masks[m],
                    keys,
                    (((1,), (1,)), ((), ())),
                    preferred_element_type=jnp.float32,
                )
                * exponent
            )
            if masked:
                row = lax.broadcasted_iota(jnp.int32, (rows, span), 0) + member * rows
                col = lax.broadcasted_iota(jnp.int32, (rows, span), 1)
                score = jnp.where(row >= col, score, -1e30)
            before = row_max[2 * qi + m]
            top = jnp.maximum(before, jnp.max(score, axis=-1, keepdims=True))
            weights = jnp.exp2(score - top[:, :1]).astype(jnp.bfloat16)
            factor = jnp.exp2(before - top)[:, :1]
            row_max[2 * qi + m] = top
            accum[2 * qi + m] = accum[2 * qi + m] * factor + jnp.dot(
                weights, values, preferred_element_type=jnp.float32
            )

    lam_pick = lax.broadcasted_iota(jnp.int32, (1, heads), 1) == plane
    lam_out.wait()
    lam_row = jnp.where(home, lam_own[...], lam_other[...])
    lam = jnp.sum(jnp.where(lam_pick, lam_row, 0.0), axis=-1, keepdims=True)
    column = lax.broadcasted_iota(jnp.int32, (rows, lanes), 1)

    def o_copy(q):
        return remote(o_send.at[q], o_all.at[plane], o_s.at[q], o_r.at[plane], worker(q))

    def lt_copy(q):
        return remote(lt_send.at[q], lt_all.at[plane], lt_s.at[q], lt_r.at[plane], worker(q))

    def finalize(q):
        maps = []
        logs = []
        for m in range(2):
            held = accum[2 * q + m]
            total = held[:, lanes:]
            maps.append(held[:, :lanes] / total)
            logs.append(jnp.log(total) + row_max[2 * q + m] * math.log(2.0))
        diff = maps[0] - lam * maps[1]
        mean = jnp.mean(diff * diff, axis=-1, keepdims=True)
        o_send[q] = (diff * lax.rsqrt(mean + 1e-05)).astype(jnp.bfloat16)
        turned = jnp.where(column == 0, logs[0], logs[1]).T
        lt_send[q] = turned[:2, :]
        away = (q != plane) | (t != y)

        @pl.when(away)
        def _():
            o_copy(q).start()
            lt_copy(q).start()

        @pl.when(jnp.logical_not(away))
        def _():
            o_all[plane] = o_send[q]
            lt_all[plane] = lt_send[q]

    def q_arrived(q):
        @pl.when((q != plane) | (t != y))
        def _():
            arrived(q_all.at[q], q_r.at[q])

    for k in range(heads):
        c = order[k]
        if k + 1 < heads:
            forward_stage(k + 1)
        finish_plane(k)

        @pl.loop(c + 1, heads)
        def _(q, k=k, c=c):
            if k == 0:
                q_arrived(q)
            attend(q, c, False)
            if k > 0:

                @pl.when((k == plane) & (q <= plane))
                def _():
                    finalize(q)

        @pl.when(k <= plane)
        def _(c=c):
            q_arrived(c)

        attend(c, c, True)

        @pl.when(k >= plane)
        def _(c=c):
            finalize(c)

        if k + 1 < heads:
            forward_square(k + 1)
        if k == 0:
            small[3].wait()

            @pl.when(s > 0)
            def _():
                arrived(tail_in, tail_sem.at[1])

            @pl.when(s == 0)
            def _():
                tail_in[...] = jnp.zeros(tail_in.shape, jnp.bfloat16)

            lead = extended.shape[0] - rows
            extended[0:lead, :] = tail_in[tail - lead :, :].astype(jnp.float32)
            extended[lead:, :] = inner_sig[...].astype(jnp.float32)
            tap_count = taps_ref.shape[0]
            convolved = jnp.zeros((rows, local), jnp.float32)
            for position in range(tap_count):
                offset = lead - (tap_count - 1) + position
                convolved = convolved + taps_ref[position : position + 1, :] * extended[
                    offset : offset + rows, :
                ]
            conv_out[...] = (outer[...].astype(jnp.float32) * convolved).astype(jnp.bfloat16)
            weight_copies[len(sources)].wait()
            conv_part[...] = jnp.dot(
                conv_out[...], wc_vmem[...], preferred_element_type=jnp.float32
            )

    weight_copies[len(sources) + 1].wait()
    half_rows = rows // 2
    for j in range(heads):

        @pl.when((j != plane) | (t != y))
        def _(j=j):
            arrived(o_all.at[j], o_r.at[j])
            arrived(lt_all.at[j], lt_r.at[j])

    for h in range(heads):
        totals_ref[h] = lt_all[h]
        part = slice(h * lanes, (h + 1) * lanes)
        head_out[:, part] = (o_all[h].astype(jnp.float32) * opened[:, part]).astype(jnp.bfloat16)

    def partial_rows(which):
        there = pl.ds(pl.multiple_of(which * half_rows, half_rows), half_rows)
        attn = jnp.dot(head_out[there, :], wo_vmem[...], preferred_element_type=jnp.float32)
        return (attn + conv_part[there, :]).astype(jnp.bfloat16)

    part_send[...] = partial_rows(1 - t)
    exchange = remote(part_send, part_recv, part_sem.at[0], part_sem.at[1], c_dev)
    exchange.start()
    own_rows = partial_rows(t).astype(jnp.float32)
    exchange.wait()
    mixed_ref[...] = (own_rows + part_recv[...].astype(jnp.float32)).astype(jnp.bfloat16)
    for copy in started:
        copy.wait_send()
    drain_all(q_copy)
    drain_all(kv_copy)
    drain_all(o_copy)
    drain_all(lt_copy)

    @pl.when(s < last)
    def _():
        tail_copy.wait_send()


def fused(sp_count, *args):
    tokens, norm_gain, wq = args[0], args[1], args[2]
    lambdas, head_gain = args[10], args[11]
    rows, half = tokens.shape
    heads = lambdas.shape[0]
    local = wq.shape[1]
    lanes = local // heads
    out_width = args[12].shape[1]
    bf16, f32 = jnp.bfloat16, jnp.float32
    vmem = pl.BlockSpec(memory_space=pltpu.VMEM)
    hbm = pl.BlockSpec(memory_space=pl.ANY)
    dma = pltpu.SemaphoreType.DMA
    operands = list(args)
    operands[1] = norm_gain.reshape(1, -1)
    operands[10] = lambdas.reshape(1, -1)
    operands[11] = head_gain.reshape(1, -1)
    return pl.pallas_call(
        functools.partial(fused_kernel, sp_count, heads),
        out_shape=(
            jax.ShapeDtypeStruct((rows // 2, out_width), bf16),
            jax.ShapeDtypeStruct((heads, 2, rows), f32),
        ),
        in_specs=[hbm] * len(operands),
        out_specs=(vmem, vmem),
        scratch_shapes=[
            pltpu.VMEM((rows, half), bf16),
            pltpu.VMEM((rows, half), bf16),
            pltpu.VMEM((1, 2 * half), f32),
            pltpu.VMEM(args[9].shape, f32),
            pltpu.VMEM((1, local), f32),
            pltpu.VMEM((1, heads), f32),
            pltpu.VMEM((1, heads), f32),
            pltpu.VMEM((rows, 2 * half), bf16),
            pltpu.VMEM((7,) + wq.shape, bf16),
            pltpu.VMEM(args[12].shape, bf16),
            pltpu.VMEM(args[13].shape, bf16),
            pltpu.VMEM((heads, rows, 2 * lanes), bf16),
            pltpu.VMEM((heads, rows, lanes), bf16),
            pltpu.VMEM((sp_count, rows, 2 * lanes), bf16),
            pltpu.VMEM((heads, rows, lanes), bf16),
            pltpu.VMEM((2 * heads, rows, lanes), f32),
            pltpu.VMEM((2 * heads, rows, 2 * lanes), f32),
            pltpu.VMEM((rows, local), f32),
            pltpu.VMEM((rows, local), bf16),
            pltpu.VMEM((rows, local), bf16),
            pltpu.VMEM((16, local), bf16),
            pltpu.VMEM((rows + 8, local), f32),
            pltpu.VMEM((rows, local), bf16),
            pltpu.VMEM((rows, local), bf16),
            pltpu.VMEM((rows, out_width), f32),
            pltpu.VMEM((heads, rows, lanes), bf16),
            pltpu.VMEM((heads, rows, lanes), bf16),
            pltpu.VMEM((heads, 2, rows), f32),
            pltpu.VMEM((heads, 2, rows), f32),
            pltpu.VMEM((rows // 2, out_width), bf16),
            pltpu.VMEM((rows // 2, out_width), bf16),
            dma((9,)),
            dma((5,)),
            dma((4,)),
            dma((2,)),
            dma((2,)),
        ]
        + [dma((heads,)) for _ in range(14)]
        + [pltpu.SemaphoreType.REGULAR, pltpu.SemaphoreType.REGULAR],
        compiler_params=pltpu.CompilerParams(
            collective_id=0, has_side_effects=True, vmem_limit_bytes=60 * 1024 * 1024
        ),
    )(*operands)


def fits_square(mesh, heads, rows, key_columns, value_columns):
    return (
        mesh.shape["tp"] == 2
        and mesh.shape["sp"] == heads * RELAY
        and heads > 1
        and rows % 32 == 0
        and key_columns == value_columns == heads * 128
    )


def solution(mesh):
    placed = (
        P("sp", "tp"),
        P(),
        P(None, "tp"),
        P(None, "tp"),
        P(None, "tp"),
        P(None, "tp"),
        P(None, "tp"),
        P(None, "tp"),
        P(None, "tp"),
        P(None, "tp"),
        P("tp"),
        P("tp"),
        P("tp", None),
        P("tp", None),
    )

    def step(*args):
        heads = args[10].shape[0]
        if fits_square(mesh, heads, args[0].shape[0], args[2].shape[1], args[4].shape[1]):
            return fused(mesh.shape["sp"], *args)
        return per_device(*args)

    return jax.shard_map(
        step,
        mesh=mesh,
        in_specs=placed,
        out_specs=(P(("sp", "tp"), None), P("tp", None, "sp")),
        check_vma=False,
    )
```

```python
import functools
import math

import jax
import jax.numpy as jnp
from jax import lax
from jax.experimental import pallas as pl
from jax.experimental.pallas import tpu as pltpu
from jax.sharding import PartitionSpec as P

MESH = pl.DeviceIdType.MESH


def passed_along(shard, axis, by):
    count = lax.axis_size(axis)
    pairs = [(i, i + by) for i in range(count) if 0 <= i + by < count]
    return lax.ppermute(shard, axis, pairs)


def per_device(
    tokens,
    norm_gain,
    query_weight,
    key_weight,
    value_weight,
    gate_weight,
    outer_weight,
    inner_weight,
    signal_weight,
    conv_taps,
    lambdas,
    head_gain,
    attn_out_weight,
    conv_out_weight,
):
    row_count = tokens.shape[0]
    width = norm_gain.shape[0]
    weights = [
        query_weight,
        key_weight,
        value_weight,
        gate_weight,
        outer_weight,
        inner_weight,
        signal_weight,
    ]
    splits = []
    running = 0
    for weight in weights[:-1]:
        running = running + weight.shape[1]
        splits.append(running)
    joined = jnp.concatenate(weights, axis=1)
    empty = jnp.zeros((row_count, joined.shape[1]), jnp.float32)
    piece = lax.all_gather(tokens, "tp", axis=1, tiled=True)
    summed = empty
    piece_f = piece.astype(jnp.float32)
    normed_piece = (piece.astype(jnp.float32) * norm_gain).astype(jnp.bfloat16)
    raw = jnp.dot(normed_piece, joined, preferred_element_type=jnp.float32)
    squares = jnp.sum(piece_f * piece_f, axis=-1)
    scale = lax.rsqrt(squares / width + 1e-06)
    projected = (raw * scale[:, None]).astype(jnp.bfloat16)
    query, key, value, attn_gate, outer, inner, signal = jnp.split(projected, splits, axis=1)
    head_count = lambdas.shape[0]
    key_size = query_weight.shape[1] // (head_count * 2)
    value_size = value_weight.shape[1] // head_count
    score_scale = key_size ** (-0.5)
    own_index = lax.axis_index("sp")
    local_pos = jnp.arange(row_count, dtype=jnp.int32)
    query_parts = [query]
    position_parts = [own_index * row_count + local_pos]
    query_parts = [
        segment.reshape(segment.shape[0], head_count, 2, key_size) for segment in query_parts
    ]

    def absorb(current, query_rows, row_pos, key_block, value_block, key_pos):
        running_max, summed, accum = current
        score = (
            jnp.einsum("qhmd,khmd->hmqk", query_rows, key_block, preferred_element_type=jnp.float32)
            * score_scale
        )
        visible = row_pos[:, None] >= key_pos[None, :]
        masked = jnp.where(visible, score, -1e30)
        new_max = jnp.maximum(running_max, jnp.max(masked, axis=-1, keepdims=True))
        weights_now = jnp.where(visible, jnp.exp(masked - new_max), 0.0)
        factor = jnp.exp(running_max - new_max)
        summed = summed * factor + jnp.sum(weights_now, axis=-1, keepdims=True)
        accum = accum * factor + jnp.einsum(
            "hmqk,khd->hmqd",
            weights_now.astype(jnp.bfloat16),
            value_block,
            preferred_element_type=jnp.float32,
        )
        return (new_max, summed, accum)

    def fresh(rows):
        return (
            jnp.full((head_count, 2, rows, 1), -1e30, jnp.float32),
            jnp.zeros((head_count, 2, rows, 1), jnp.float32),
            jnp.zeros((head_count, 2, rows, value_size), jnp.float32),
        )

    start_states = tuple((fresh(segment.shape[0]) for segment in query_parts))
    carry = start_states
    key_piece = lax.all_gather(key, "sp", axis=0, tiled=True)
    value_piece = lax.all_gather(value, "sp", axis=0, tiled=True)
    length = key_piece.shape[0]
    block_len = 512
    key_blocks = key_piece.reshape(length // block_len, block_len, head_count, 2, key_size)
    value_blocks = value_piece.reshape(length // block_len, block_len, head_count, value_size)

    def one_block(states, item):
        key_block, value_block, block_id = item
        first_key = block_id * block_len
        key_pos = first_key + jnp.arange(block_len, dtype=jnp.int32)
        updated = []
        for current, query_rows, row_pos in zip(states, query_parts, position_parts):

            def compute(held, query_rows=query_rows, row_pos=row_pos):
                return absorb(held, query_rows, row_pos, key_block, value_block, key_pos)

            def unchanged(held):
                return held

            updated.append(
                lax.cond(first_key <= row_pos[row_pos.shape[0] - 1], compute, unchanged, current)
            )
        return (tuple(updated), None)

    carry, _ = lax.scan(
        one_block,
        carry,
        (key_blocks, value_blocks, jnp.arange(length // block_len, dtype=jnp.int32)),
    )
    states = carry
    running_max = jnp.concatenate([held[0] for held in states], axis=2)
    summed = jnp.concatenate([held[1] for held in states], axis=2)
    accum = jnp.concatenate([held[2] for held in states], axis=2)
    mapped = accum / summed
    diff = mapped[:, 0] - lambdas[:, None, None] * mapped[:, 1]
    log_totals = jnp.log(summed[..., 0]) + running_max[..., 0]
    diff = jnp.transpose(diff, (1, 0, 2))
    normed = (
        diff
        * lax.rsqrt(jnp.mean(diff * diff, axis=-1, keepdims=True) + 1e-05)
        * head_gain.reshape(head_count, value_size)
    )
    normed = normed.reshape(row_count, head_count * value_size)
    head_out = (normed * jax.nn.silu(attn_gate.astype(jnp.float32))).astype(jnp.bfloat16)
    taps = conv_taps.shape[0]
    inner_sig = (inner.astype(jnp.float32) * signal.astype(jnp.float32)).astype(jnp.bfloat16)
    before = passed_along(inner_sig[row_count - (taps - 1) :], "sp", 1)
    extended = jnp.concatenate([before, inner_sig], axis=0).astype(jnp.float32)
    convolved = jnp.zeros((row_count, inner_sig.shape[1]), jnp.float32)
    for position in range(taps):
        convolved = convolved + conv_taps[position] * extended[position : position + row_count]
    conv_out = (outer.astype(jnp.float32) * convolved).astype(jnp.bfloat16)
    mixed = lax.psum_scatter(
        (
            jnp.dot(head_out, attn_out_weight, preferred_element_type=jnp.float32)
            + jnp.dot(conv_out, conv_out_weight, preferred_element_type=jnp.float32)
        ).astype(jnp.bfloat16),
        "tp",
        scatter_dimension=0,
        tiled=True,
    )
    return (mixed, log_totals)


RELAY = 4


def fused_kernel(
    sp_count,
    heads,
    tokens_hbm,
    gain_hbm,
    wq_hbm,
    wk_hbm,
    wv_hbm,
    wg_hbm,
    wouter_hbm,
    winner_hbm,
    wsignal_hbm,
    taps_hbm,
    lambdas_hbm,
    head_gain_hbm,
    wo_hbm,
    wc_hbm,
    mixed_ref,
    totals_ref,
    own_tokens,
    other_tokens,
    gain_ref,
    taps_ref,
    head_gain_ref,
    lam_own,
    lam_other,
    normed,
    w_vmem,
    wo_vmem,
    wc_vmem,
    kv_send,
    q_send,
    kv_all,
    q_all,
    row_max,
    accum,
    opened,
    outer,
    inner_sig,
    tail_in,
    extended,
    conv_out,
    head_out,
    conv_part,
    o_send,
    o_all,
    lt_send,
    lt_all,
    part_send,
    part_recv,
    w_sem,
    in_sem,
    tok_sem,
    tail_sem,
    part_sem,
    stage_s,
    stage_r,
    q_s,
    q_r,
    x_s,
    x_r,
    c_s,
    c_r,
    d_s,
    d_r,
    o_s,
    o_r,
    lt_s,
    lt_r,
    pair_sem,
    met_sem,
):
    rows, half = own_tokens.shape
    width = 2 * half
    local = wq_hbm.shape[1]
    lanes = local // heads
    s = lax.axis_index("sp")
    t = lax.axis_index("tp")
    plane = s // RELAY
    place = lax.rem(s, RELAY)
    y = place // 2
    x = lax.rem(place, 2)
    member = 2 * t + x
    home = t == y
    low = plane < heads // 2
    last = sp_count - 1

    def at(sp_index, tp_index=None):
        return {"sp": sp_index, "tp": t if tp_index is None else tp_index}

    def remote(src, dst, send_sem, recv_sem, device):
        return pltpu.make_async_remote_copy(
            src_ref=src,
            dst_ref=dst,
            send_sem=send_sem,
            recv_sem=recv_sem,
            device_id=device,
            device_id_type=MESH,
        )

    def worker(j):
        return at(j * RELAY + member, y)

    x_sp = s + 1 - 2 * x
    x_dev = at(x_sp)
    c_dev = at(s, 1 - t)

    small = [
        pltpu.make_async_copy(ref, dst, in_sem.at[i])
        for i, (ref, dst) in enumerate(
            [
                (tokens_hbm, own_tokens),
                (gain_hbm, gain_ref),
                (lambdas_hbm, lam_own),
                (taps_hbm, taps_ref),
                (head_gain_hbm, head_gain_ref),
            ]
        )
    ]
    for copy in small:
        copy.start()
    sources = [wq_hbm, wk_hbm, wv_hbm, winner_hbm, wsignal_hbm, wouter_hbm, wg_hbm]
    weight_copies = [
        pltpu.make_async_copy(ref, w_vmem.at[i], w_sem.at[i]) for i, ref in enumerate(sources)
    ]
    weight_copies.append(pltpu.make_async_copy(wc_hbm, wc_vmem, w_sem.at[len(sources)]))
    weight_copies.append(pltpu.make_async_copy(wo_hbm, wo_vmem, w_sem.at[len(sources) + 1]))
    weight_copies[0].start()

    barrier = pltpu.get_barrier_semaphore()

    def signal(sem, device):
        pl.semaphore_signal(sem, inc=1, device_id=device, device_id_type=MESH)

    def greet(sp_index):
        signal(barrier, at(sp_index, 1))

    @pl.when(t == 1)
    def _():
        signal(barrier, at(s, 0))

    for step in range(1, heads):
        greet(lax.rem(plane + step, heads) * RELAY + member)

    @pl.when(t != y)
    def _():
        greet(plane * RELAY + member)

    greet(x_sp)

    @pl.when(s < last)
    def _():
        greet(s + 1)

    @pl.when(s > 0)
    def _():
        greet(s - 1)

    @pl.when(t == 0)
    def _():
        pl.semaphore_wait(barrier, 1)
        signal(pair_sem, at(s, 1))

    @pl.when(t == 1)
    def _():
        pl.semaphore_wait(pair_sem, 1)

    greetings = (
        2 * heads + 1 + 2 * jnp.where(s > 0, 1, 0) + 2 * jnp.where(s < last, 1, 0)
    )

    def meet():
        @pl.when(t == 1)
        def _():
            pl.semaphore_wait(barrier, greetings)
            signal(met_sem, at(s, 0))

        @pl.when(t == 0)
        def _():
            pl.semaphore_wait(met_sem, 1)

    small[0].wait()
    tokens_out = remote(own_tokens, other_tokens, tok_sem.at[0], tok_sem.at[1], c_dev)
    tokens_out.start()
    for copy in weight_copies[1:]:
        copy.start()
    small[2].wait()
    lam_out = remote(lam_own, lam_other, tok_sem.at[2], tok_sem.at[3], c_dev)
    lam_out.start()

    row_max[...] = jnp.full(row_max.shape, -1e30, jnp.float32)
    accum[...] = jnp.zeros(accum.shape, jnp.float32)

    small[1].wait()
    mine = pl.ds(pl.multiple_of(t * half, half), half)
    theirs = pl.ds(pl.multiple_of((1 - t) * half, half), half)
    own_f = own_tokens[...].astype(jnp.float32)
    squares = jnp.sum(own_f * own_f, axis=-1, keepdims=True)
    normed[:, mine] = (own_f * gain_ref[:, mine]).astype(jnp.bfloat16)
    tokens_out.wait()
    other_f = other_tokens[...].astype(jnp.float32)
    squares = squares + jnp.sum(other_f * other_f, axis=-1, keepdims=True)
    normed[:, theirs] = (other_f * gain_ref[:, theirs]).astype(jnp.bfloat16)
    scale = lax.rsqrt(squares / width + 1e-06)

    def project(index, scale=scale):
        weight_copies[index].wait()
        raw = jnp.dot(normed[...], w_vmem[index], preferred_element_type=jnp.float32)
        return (raw * scale).astype(jnp.bfloat16)

    def nearest_first(i):
        rising = jnp.where(i < plane, plane - 1 - i, i + 1)
        falling = jnp.where(i < heads - 1 - plane, plane + 1 + i, heads - 2 - i)
        return jnp.where(low, falling, rising)

    def q_copy(j):
        return remote(q_send.at[j], q_all.at[plane], q_s.at[j], q_r.at[plane], worker(j))

    def kv_copy(j):
        return remote(kv_send.at[j], kv_all.at[s], stage_s.at[j], stage_r.at[plane], worker(j))

    def send_all(copy_of):
        @pl.when(t != y)
        def _():
            copy_of(plane).start()

        for i in range(heads - 1):
            copy_of(nearest_first(i)).start()

    def drain_all(copy_of):
        for i in range(heads - 1):
            copy_of(nearest_first(i)).wait_send()

        @pl.when(t != y)
        def _():
            copy_of(plane).wait_send()

    exponent = (lanes // 2) ** (-0.5) * math.log2(math.e)
    projected = project(0, scale * exponent)
    for h in range(heads):
        q_send[h] = projected[:, h * lanes : (h + 1) * lanes]

    @pl.when(home)
    def _():
        q_all[plane] = q_send[plane]

    @pl.when(plane >= heads // 2)
    def _():
        meet()
        send_all(q_copy)

    for index in range(2):
        projected = project(1 + index)
        for h in range(heads):
            kv_send[h, :, index * lanes : (index + 1) * lanes] = projected[
                :, h * lanes : (h + 1) * lanes
            ]

    @pl.when(home)
    def _():
        kv_all[s] = kv_send[plane]

    @pl.when(low)
    def _():
        meet()

    send_all(kv_copy)

    @pl.when(low)
    def _():
        send_all(q_copy)

    def order(k):
        return jnp.where(k <= plane, plane - k, k)

    def block(plane_index, which):
        return kv_all.at[plane_index * RELAY + which]

    def arrived(dst, recv_sem):
        remote(dst, dst, stage_s.at[0], recv_sem, x_dev).wait_recv()

    def along_x(k):
        here = block(order(k), member)
        return remote(here, here, x_s.at[k], x_r.at[order(k)], x_dev)

    def across(k):
        here = block(order(k), member)
        return remote(here, here, c_s.at[k], c_r.at[order(k)], c_dev)

    def onward(k):
        from_x = block(order(k), member + 1 - 2 * x)
        return remote(from_x, from_x, d_s.at[k], d_r.at[order(k)], c_dev)

    def forward_stage(k):
        along_x(k).start()
        across(k).start()

    def forward_square(k):
        c = order(k)
        arrived(block(c, member + 1 - 2 * x), x_r.at[c])
        onward(k).start()

    def finish_plane(k):
        c = order(k)
        arrived(block(c, lax.rem(member + 2, RELAY)), c_r.at[c])
        arrived(block(c, RELAY - 1 - member), d_r.at[c])

    @pl.when(home)
    def _():
        forward_stage(0)

    inner = project(3).astype(jnp.float32)
    signal_f = project(4).astype(jnp.float32)
    inner_sig[...] = (inner * signal_f).astype(jnp.bfloat16)
    tail = tail_in.shape[0]
    tail_copy = remote(
        inner_sig.at[pl.ds(rows - tail, tail)],
        tail_in,
        tail_sem.at[0],
        tail_sem.at[1],
        at(lax.rem(s + 1, sp_count)),
    )

    @pl.when(s < last)
    def _():
        tail_copy.start()

    @pl.when(t != y)
    def _():
        arrived(block(plane, member), stage_r.at[plane])
        forward_stage(0)

    small[4].wait()
    outer[...] = project(5)
    gate = project(6).astype(jnp.float32)
    opened[...] = gate / (1.0 + jnp.exp(-gate)) * head_gain_ref[...]
    forward_square(0)

    span = RELAY * rows
    lane = lax.broadcasted_iota(jnp.int32, (1, lanes), 1)
    masks = [
        of_map.astype(jnp.float32).astype(jnp.bfloat16)
        for of_map in (lane < lanes // 2, lane >= lanes // 2)
    ]

    def attend_plane(c):
        held = kv_all[c * RELAY : (c + 1) * RELAY].reshape(span, 2 * lanes)
        keys = held[:, :lanes]
        values = jnp.concatenate(
            [held[:, lanes:], jnp.ones((span, lanes), jnp.bfloat16)], axis=1
        )

        def scores(qi, m):
            score = lax.dot_general(
                q_all[qi] * masks[m],
                keys,
                (((1,), (1,)), ((), ())),
                preferred_element_type=jnp.float32,
            )
            if qi == c:
                row = lax.broadcasted_iota(jnp.int32, (rows, span), 0) + member * rows
                col = lax.broadcasted_iota(jnp.int32, (rows, span), 1)
                score = jnp.where(row >= col, score, -1e30)
            return score

        def absorb(at_row, score):
            before = row_max[at_row]
            top = jnp.maximum(before, jnp.max(score, axis=-1, keepdims=True))
            weights = jnp.exp2(score - top[:, :1]).astype(jnp.bfloat16)
            factor = jnp.exp2(before - top)
            row_max[at_row] = top
            update = jnp.dot(weights, values, preferred_element_type=jnp.float32)
            for part in (slice(0, lanes), slice(lanes, 2 * lanes)):
                accum[at_row, :, part] = accum[at_row, :, part] * factor + update[:, part]

        items = [(qi, m) for qi in range(heads - 1, c - 1, -1) for m in range(2)]
        upcoming = scores(*items[0])
        for i, (qi, m) in enumerate(items):
            score = upcoming
            if i + 1 < len(items):
                upcoming = scores(*items[i + 1])
            absorb(2 * qi + m, score)

    lam_pick = lax.broadcasted_iota(jnp.int32, (1, heads), 1) == plane
    lam_out.wait()
    lam_row = jnp.where(home, lam_own[...], lam_other[...])
    lam = jnp.sum(jnp.where(lam_pick, lam_row, 0.0), axis=-1, keepdims=True)
    column = lax.broadcasted_iota(jnp.int32, (rows, lanes), 1)

    def o_copy(q):
        return remote(o_send.at[q], o_all.at[plane], o_s.at[q], o_r.at[plane], worker(q))

    def lt_copy(q):
        return remote(lt_send.at[q], lt_all.at[plane], lt_s.at[q], lt_r.at[plane], worker(q))

    def finalize(q):
        maps = []
        logs = []
        for m in range(2):
            held = accum[2 * q + m]
            total = held[:, lanes:]
            maps.append(held[:, :lanes] / total)
            logs.append(jnp.log(total) + row_max[2 * q + m] * math.log(2.0))
        diff = maps[0] - lam * maps[1]
        mean = jnp.mean(diff * diff, axis=-1, keepdims=True)
        o_send[q] = (diff * lax.rsqrt(mean + 1e-05)).astype(jnp.bfloat16)
        turned = jnp.where(column == 0, logs[0], logs[1]).T
        lt_send[q] = turned[:2, :]
        away = (q != plane) | (t != y)

        @pl.when(away)
        def _():
            o_copy(q).start()
            lt_copy(q).start()

        @pl.when(jnp.logical_not(away))
        def _():
            o_all[plane] = o_send[q]
            lt_all[plane] = lt_send[q]

    def q_arrived(q):
        @pl.when((q != plane) | (t != y))
        def _():
            arrived(q_all.at[q], q_r.at[q])

    def convolve():
        small[3].wait()

        @pl.when(s > 0)
        def _():
            arrived(tail_in, tail_sem.at[1])

        @pl.when(s == 0)
        def _():
            tail_in[...] = jnp.zeros(tail_in.shape, jnp.bfloat16)

        lead = extended.shape[0] - rows
        extended[0:lead, :] = tail_in[tail - lead :, :].astype(jnp.float32)
        extended[lead:, :] = inner_sig[...].astype(jnp.float32)
        tap_count = taps_ref.shape[0]
        convolved = jnp.zeros((rows, local), jnp.float32)
        for position in range(tap_count):
            offset = lead - (tap_count - 1) + position
            convolved = convolved + taps_ref[position : position + 1, :] * extended[
                offset : offset + rows, :
            ]
        conv_out[...] = (outer[...].astype(jnp.float32) * convolved).astype(jnp.bfloat16)
        weight_copies[len(sources)].wait()
        conv_part[...] = jnp.dot(
            conv_out[...], wc_vmem[...], preferred_element_type=jnp.float32
        )

    @pl.loop(0, heads)
    def _(k):
        c = order(k)

        @pl.when(k + 1 < heads)
        def _():
            following = order(k + 1)
            arrived(block(following, member), stage_r.at[following])
            forward_stage(k + 1)

        @pl.loop(c, heads)
        def _(q):
            @pl.when((k == 0) | ((q == c) & (k <= plane)))
            def _():
                q_arrived(q)

        finish_plane(k)
        for cc in range(heads):

            @pl.when(c == cc)
            def _(cc=cc):
                attend_plane(cc)

        @pl.when(k + 1 < heads)
        def _():
            forward_square(k + 1)

        @pl.loop(0, heads)
        def _(q):
            @pl.when(((k == plane) & (q <= plane)) | ((k > plane) & (q == c)))
            def _():
                finalize(q)

        @pl.when(k == 0)
        def _():
            convolve()

    weight_copies[len(sources) + 1].wait()
    half_rows = rows // 2
    for j in range(heads):

        @pl.when((j != plane) | (t != y))
        def _(j=j):
            arrived(o_all.at[j], o_r.at[j])
            arrived(lt_all.at[j], lt_r.at[j])

    for h in range(heads):
        totals_ref[h] = lt_all[h]
        part = slice(h * lanes, (h + 1) * lanes)
        head_out[:, part] = (o_all[h].astype(jnp.float32) * opened[:, part]).astype(jnp.bfloat16)

    def partial_rows(which):
        there = pl.ds(pl.multiple_of(which * half_rows, half_rows), half_rows)
        attn = jnp.dot(head_out[there, :], wo_vmem[...], preferred_element_type=jnp.float32)
        return (attn + conv_part[there, :]).astype(jnp.bfloat16)

    part_send[...] = partial_rows(1 - t)
    exchange = remote(part_send, part_recv, part_sem.at[0], part_sem.at[1], c_dev)
    exchange.start()
    own_rows = partial_rows(t).astype(jnp.float32)
    exchange.wait()
    mixed_ref[...] = (own_rows + part_recv[...].astype(jnp.float32)).astype(jnp.bfloat16)
    for k in range(heads):
        along_x(k).wait_send()
        across(k).wait_send()
        onward(k).wait_send()
    drain_all(q_copy)
    drain_all(kv_copy)
    drain_all(o_copy)
    drain_all(lt_copy)

    @pl.when(s < last)
    def _():
        tail_copy.wait_send()


def fused(sp_count, *args):
    tokens, norm_gain, wq = args[0], args[1], args[2]
    lambdas, head_gain = args[10], args[11]
    rows, half = tokens.shape
    heads = lambdas.shape[0]
    local = wq.shape[1]
    lanes = local // heads
    out_width = args[12].shape[1]
    bf16, f32 = jnp.bfloat16, jnp.float32
    vmem = pl.BlockSpec(memory_space=pltpu.VMEM)
    hbm = pl.BlockSpec(memory_space=pl.ANY)
    dma = pltpu.SemaphoreType.DMA
    operands = list(args)
    operands[1] = norm_gain.reshape(1, -1)
    operands[10] = lambdas.reshape(1, -1)
    operands[11] = head_gain.reshape(1, -1)
    return pl.pallas_call(
        functools.partial(fused_kernel, sp_count, heads),
        out_shape=(
            jax.ShapeDtypeStruct((rows // 2, out_width), bf16),
            jax.ShapeDtypeStruct((heads, 2, rows), f32),
        ),
        in_specs=[hbm] * len(operands),
        out_specs=(vmem, vmem),
        scratch_shapes=[
            pltpu.VMEM((rows, half), bf16),
            pltpu.VMEM((rows, half), bf16),
            pltpu.VMEM((1, 2 * half), f32),
            pltpu.VMEM(args[9].shape, f32),
            pltpu.VMEM((1, local), f32),
            pltpu.VMEM((1, heads), f32),
            pltpu.VMEM((1, heads), f32),
            pltpu.VMEM((rows, 2 * half), bf16),
            pltpu.VMEM((7,) + wq.shape, bf16),
            pltpu.VMEM(args[12].shape, bf16),
            pltpu.VMEM(args[13].shape, bf16),
            pltpu.VMEM((heads, rows, 2 * lanes), bf16),
            pltpu.VMEM((heads, rows, lanes), bf16),
            pltpu.VMEM((sp_count, rows, 2 * lanes), bf16),
            pltpu.VMEM((heads, rows, lanes), bf16),
            pltpu.VMEM((2 * heads, rows, lanes), f32),
            pltpu.VMEM((2 * heads, rows, 2 * lanes), f32),
            pltpu.VMEM((rows, local), f32),
            pltpu.VMEM((rows, local), bf16),
            pltpu.VMEM((rows, local), bf16),
            pltpu.VMEM((16, local), bf16),
            pltpu.VMEM((rows + 8, local), f32),
            pltpu.VMEM((rows, local), bf16),
            pltpu.VMEM((rows, local), bf16),
            pltpu.VMEM((rows, out_width), f32),
            pltpu.VMEM((heads, rows, lanes), bf16),
            pltpu.VMEM((heads, rows, lanes), bf16),
            pltpu.VMEM((heads, 2, rows), f32),
            pltpu.VMEM((heads, 2, rows), f32),
            pltpu.VMEM((rows // 2, out_width), bf16),
            pltpu.VMEM((rows // 2, out_width), bf16),
            dma((9,)),
            dma((5,)),
            dma((4,)),
            dma((2,)),
            dma((2,)),
        ]
        + [dma((heads,)) for _ in range(14)]
        + [pltpu.SemaphoreType.REGULAR, pltpu.SemaphoreType.REGULAR],
        compiler_params=pltpu.CompilerParams(
            collective_id=0, has_side_effects=True, vmem_limit_bytes=60 * 1024 * 1024
        ),
    )(*operands)


def fits_square(mesh, heads, rows, key_columns, value_columns):
    return (
        mesh.shape["tp"] == 2
        and mesh.shape["sp"] == heads * RELAY
        and heads > 1
        and rows % 32 == 0
        and key_columns == value_columns == heads * 128
    )


def solution(mesh):
    placed = (
        P("sp", "tp"),
        P(),
        P(None, "tp"),
        P(None, "tp"),
        P(None, "tp"),
        P(None, "tp"),
        P(None, "tp"),
        P(None, "tp"),
        P(None, "tp"),
        P(None, "tp"),
        P("tp"),
        P("tp"),
        P("tp", None),
        P("tp", None),
    )

    def step(*args):
        heads = args[10].shape[0]
        if fits_square(mesh, heads, args[0].shape[0], args[2].shape[1], args[4].shape[1]):
            return fused(mesh.shape["sp"], *args)
        return per_device(*args)

    return jax.shard_map(
        step,
        mesh=mesh,
        in_specs=placed,
        out_specs=(P(("sp", "tp"), None), P("tp", None, "sp")),
        check_vma=False,
    )
```

```python
import functools
import math

import jax
import jax.numpy as jnp
from jax import lax
from jax.experimental import pallas as pl
from jax.experimental.pallas import tpu as pltpu
from jax.sharding import PartitionSpec as P

MESH = pl.DeviceIdType.MESH


def passed_along(shard, axis, by):
    count = lax.axis_size(axis)
    pairs = [(i, i + by) for i in range(count) if 0 <= i + by < count]
    return lax.ppermute(shard, axis, pairs)


def per_device(
    tokens,
    norm_gain,
    query_weight,
    key_weight,
    value_weight,
    gate_weight,
    outer_weight,
    inner_weight,
    signal_weight,
    conv_taps,
    lambdas,
    head_gain,
    attn_out_weight,
    conv_out_weight,
):
    row_count = tokens.shape[0]
    width = norm_gain.shape[0]
    weights = [
        query_weight,
        key_weight,
        value_weight,
        gate_weight,
        outer_weight,
        inner_weight,
        signal_weight,
    ]
    splits = []
    running = 0
    for weight in weights[:-1]:
        running = running + weight.shape[1]
        splits.append(running)
    joined = jnp.concatenate(weights, axis=1)
    empty = jnp.zeros((row_count, joined.shape[1]), jnp.float32)
    piece = lax.all_gather(tokens, "tp", axis=1, tiled=True)
    summed = empty
    piece_f = piece.astype(jnp.float32)
    normed_piece = (piece.astype(jnp.float32) * norm_gain).astype(jnp.bfloat16)
    raw = jnp.dot(normed_piece, joined, preferred_element_type=jnp.float32)
    squares = jnp.sum(piece_f * piece_f, axis=-1)
    scale = lax.rsqrt(squares / width + 1e-06)
    projected = (raw * scale[:, None]).astype(jnp.bfloat16)
    query, key, value, attn_gate, outer, inner, signal = jnp.split(projected, splits, axis=1)
    head_count = lambdas.shape[0]
    key_size = query_weight.shape[1] // (head_count * 2)
    value_size = value_weight.shape[1] // head_count
    score_scale = key_size ** (-0.5)
    own_index = lax.axis_index("sp")
    local_pos = jnp.arange(row_count, dtype=jnp.int32)
    query_parts = [query]
    position_parts = [own_index * row_count + local_pos]
    query_parts = [
        segment.reshape(segment.shape[0], head_count, 2, key_size) for segment in query_parts
    ]

    def absorb(current, query_rows, row_pos, key_block, value_block, key_pos):
        running_max, summed, accum = current
        score = (
            jnp.einsum("qhmd,khmd->hmqk", query_rows, key_block, preferred_element_type=jnp.float32)
            * score_scale
        )
        visible = row_pos[:, None] >= key_pos[None, :]
        masked = jnp.where(visible, score, -1e30)
        new_max = jnp.maximum(running_max, jnp.max(masked, axis=-1, keepdims=True))
        weights_now = jnp.where(visible, jnp.exp(masked - new_max), 0.0)
        factor = jnp.exp(running_max - new_max)
        summed = summed * factor + jnp.sum(weights_now, axis=-1, keepdims=True)
        accum = accum * factor + jnp.einsum(
            "hmqk,khd->hmqd",
            weights_now.astype(jnp.bfloat16),
            value_block,
            preferred_element_type=jnp.float32,
        )
        return (new_max, summed, accum)

    def fresh(rows):
        return (
            jnp.full((head_count, 2, rows, 1), -1e30, jnp.float32),
            jnp.zeros((head_count, 2, rows, 1), jnp.float32),
            jnp.zeros((head_count, 2, rows, value_size), jnp.float32),
        )

    start_states = tuple((fresh(segment.shape[0]) for segment in query_parts))
    carry = start_states
    key_piece = lax.all_gather(key, "sp", axis=0, tiled=True)
    value_piece = lax.all_gather(value, "sp", axis=0, tiled=True)
    length = key_piece.shape[0]
    block_len = 512
    key_blocks = key_piece.reshape(length // block_len, block_len, head_count, 2, key_size)
    value_blocks = value_piece.reshape(length // block_len, block_len, head_count, value_size)

    def one_block(states, item):
        key_block, value_block, block_id = item
        first_key = block_id * block_len
        key_pos = first_key + jnp.arange(block_len, dtype=jnp.int32)
        updated = []
        for current, query_rows, row_pos in zip(states, query_parts, position_parts):

            def compute(held, query_rows=query_rows, row_pos=row_pos):
                return absorb(held, query_rows, row_pos, key_block, value_block, key_pos)

            def unchanged(held):
                return held

            updated.append(
                lax.cond(first_key <= row_pos[row_pos.shape[0] - 1], compute, unchanged, current)
            )
        return (tuple(updated), None)

    carry, _ = lax.scan(
        one_block,
        carry,
        (key_blocks, value_blocks, jnp.arange(length // block_len, dtype=jnp.int32)),
    )
    states = carry
    running_max = jnp.concatenate([held[0] for held in states], axis=2)
    summed = jnp.concatenate([held[1] for held in states], axis=2)
    accum = jnp.concatenate([held[2] for held in states], axis=2)
    mapped = accum / summed
    diff = mapped[:, 0] - lambdas[:, None, None] * mapped[:, 1]
    log_totals = jnp.log(summed[..., 0]) + running_max[..., 0]
    diff = jnp.transpose(diff, (1, 0, 2))
    normed = (
        diff
        * lax.rsqrt(jnp.mean(diff * diff, axis=-1, keepdims=True) + 1e-05)
        * head_gain.reshape(head_count, value_size)
    )
    normed = normed.reshape(row_count, head_count * value_size)
    head_out = (normed * jax.nn.silu(attn_gate.astype(jnp.float32))).astype(jnp.bfloat16)
    taps = conv_taps.shape[0]
    inner_sig = (inner.astype(jnp.float32) * signal.astype(jnp.float32)).astype(jnp.bfloat16)
    before = passed_along(inner_sig[row_count - (taps - 1) :], "sp", 1)
    extended = jnp.concatenate([before, inner_sig], axis=0).astype(jnp.float32)
    convolved = jnp.zeros((row_count, inner_sig.shape[1]), jnp.float32)
    for position in range(taps):
        convolved = convolved + conv_taps[position] * extended[position : position + row_count]
    conv_out = (outer.astype(jnp.float32) * convolved).astype(jnp.bfloat16)
    mixed = lax.psum_scatter(
        (
            jnp.dot(head_out, attn_out_weight, preferred_element_type=jnp.float32)
            + jnp.dot(conv_out, conv_out_weight, preferred_element_type=jnp.float32)
        ).astype(jnp.bfloat16),
        "tp",
        scatter_dimension=0,
        tiled=True,
    )
    return (mixed, log_totals)


RELAY = 4


def fused_kernel(
    sp_count,
    heads,
    tokens_hbm,
    gain_hbm,
    wq_hbm,
    wk_hbm,
    wv_hbm,
    wg_hbm,
    wouter_hbm,
    winner_hbm,
    wsignal_hbm,
    taps_hbm,
    lambdas_hbm,
    head_gain_hbm,
    wo_hbm,
    wc_hbm,
    mixed_ref,
    totals_ref,
    own_tokens,
    other_tokens,
    gain_ref,
    taps_ref,
    head_gain_ref,
    lam_own,
    lam_other,
    normed,
    w_vmem,
    wo_vmem,
    wc_vmem,
    kv_send,
    q_send,
    kv_all,
    q_all,
    row_max,
    accum,
    opened,
    outer,
    inner_sig,
    tail_in,
    extended,
    conv_out,
    head_out,
    conv_part,
    o_send,
    o_all,
    lt_send,
    lt_all,
    p_send,
    p_all,
    pl_send,
    pl_all,
    part_send,
    part_recv,
    w_sem,
    in_sem,
    tok_sem,
    tail_sem,
    part_sem,
    stage_s,
    stage_r,
    q_s,
    q_r,
    x_s,
    x_r,
    c_s,
    c_r,
    d_s,
    d_r,
    o_s,
    o_r,
    lt_s,
    lt_r,
    p_s,
    p_r,
    pl_s,
    pl_r,
    pair_sem,
    met_sem,
):
    rows, half = own_tokens.shape
    width = 2 * half
    local = wq_hbm.shape[1]
    lanes = local // heads
    s = lax.axis_index("sp")
    t = lax.axis_index("tp")
    plane = s // RELAY
    place = lax.rem(s, RELAY)
    y = place // 2
    x = lax.rem(place, 2)
    member = 2 * t + x
    home = t == y
    low = plane < heads // 2
    high = plane >= heads // 2
    mirror = heads - 1 - plane
    last = sp_count - 1

    def at(sp_index, tp_index=None):
        return {"sp": sp_index, "tp": t if tp_index is None else tp_index}

    def remote(src, dst, send_sem, recv_sem, device):
        return pltpu.make_async_remote_copy(
            src_ref=src,
            dst_ref=dst,
            send_sem=send_sem,
            recv_sem=recv_sem,
            device_id=device,
            device_id_type=MESH,
        )

    def worker(j):
        return at(j * RELAY + member, y)

    x_sp = s + 1 - 2 * x
    x_dev = at(x_sp)
    c_dev = at(s, 1 - t)

    small = [
        pltpu.make_async_copy(ref, dst, in_sem.at[i])
        for i, (ref, dst) in enumerate(
            [
                (tokens_hbm, own_tokens),
                (gain_hbm, gain_ref),
                (lambdas_hbm, lam_own),
                (taps_hbm, taps_ref),
                (head_gain_hbm, head_gain_ref),
            ]
        )
    ]
    for copy in small:
        copy.start()
    sources = [wk_hbm, wv_hbm, wq_hbm, winner_hbm, wsignal_hbm, wouter_hbm, wg_hbm]
    weight_copies = [
        pltpu.make_async_copy(ref, w_vmem.at[i], w_sem.at[i]) for i, ref in enumerate(sources)
    ]
    weight_copies.append(pltpu.make_async_copy(wc_hbm, wc_vmem, w_sem.at[len(sources)]))
    weight_copies.append(pltpu.make_async_copy(wo_hbm, wo_vmem, w_sem.at[len(sources) + 1]))
    weight_copies[0].start()

    barrier = pltpu.get_barrier_semaphore()

    def signal(sem, device):
        pl.semaphore_signal(sem, inc=1, device_id=device, device_id_type=MESH)

    def greet(sp_index):
        signal(barrier, at(sp_index, 1))

    @pl.when(t == 1)
    def _():
        signal(barrier, at(s, 0))

    for step in range(1, heads):
        greet(lax.rem(plane + step, heads) * RELAY + member)

    @pl.when(t != y)
    def _():
        greet(plane * RELAY + member)

    greet(x_sp)

    @pl.when(s < last)
    def _():
        greet(s + 1)

    @pl.when(s > 0)
    def _():
        greet(s - 1)

    @pl.when(t == 0)
    def _():
        pl.semaphore_wait(barrier, 1)
        signal(pair_sem, at(s, 1))

    @pl.when(t == 1)
    def _():
        pl.semaphore_wait(pair_sem, 1)

    greetings = (
        2 * heads + 1 + 2 * jnp.where(s > 0, 1, 0) + 2 * jnp.where(s < last, 1, 0)
    )

    def meet():
        @pl.when(t == 1)
        def _():
            pl.semaphore_wait(barrier, greetings)
            signal(met_sem, at(s, 0))

        @pl.when(t == 0)
        def _():
            pl.semaphore_wait(met_sem, 1)

    small[0].wait()
    tokens_out = remote(own_tokens, other_tokens, tok_sem.at[0], tok_sem.at[1], c_dev)
    tokens_out.start()
    for copy in weight_copies[1:]:
        copy.start()
    small[2].wait()
    lam_out = remote(lam_own, lam_other, tok_sem.at[2], tok_sem.at[3], c_dev)
    lam_out.start()

    row_max[...] = jnp.full(row_max.shape, -1e30, jnp.float32)
    accum[...] = jnp.zeros(accum.shape, jnp.float32)

    small[1].wait()
    mine = pl.ds(pl.multiple_of(t * half, half), half)
    theirs = pl.ds(pl.multiple_of((1 - t) * half, half), half)
    own_f = own_tokens[...].astype(jnp.float32)
    squares = jnp.sum(own_f * own_f, axis=-1, keepdims=True)
    normed[:, mine] = (own_f * gain_ref[:, mine]).astype(jnp.bfloat16)
    tokens_out.wait()
    other_f = other_tokens[...].astype(jnp.float32)
    squares = squares + jnp.sum(other_f * other_f, axis=-1, keepdims=True)
    normed[:, theirs] = (other_f * gain_ref[:, theirs]).astype(jnp.bfloat16)
    scale = lax.rsqrt(squares / width + 1e-06)

    def project(index, scale=scale):
        weight_copies[index].wait()
        raw = jnp.dot(normed[...], w_vmem[index], preferred_element_type=jnp.float32)
        return (raw * scale).astype(jnp.bfloat16)

    half_planes = heads // 2
    own_base = jnp.where(low, 0, half_planes)
    far_base = half_planes - own_base

    def order(k):
        if k < half_planes:
            return own_base + lax.rem(plane - own_base + k, half_planes)
        return far_base + lax.rem(mirror - far_base + k - half_planes, half_planes)

    def q_copy(j):
        return remote(q_send.at[j], q_all.at[plane], q_s.at[j], q_r.at[plane], worker(j))

    def kv_copy(j):
        return remote(kv_send.at[j], kv_all.at[s], stage_s.at[j], stage_r.at[plane], worker(j))

    spare = heads + plane - own_base
    spare_block = spare * RELAY + place

    def near(k):
        return heads + order(k) - own_base

    def kv_mirror(i):
        peer = order(i)
        return remote(
            kv_send.at[heads - 1 - peer],
            kv_all.at[spare_block],
            stage_s.at[near(i)],
            stage_r.at[spare],
            worker(peer),
        )

    def q_mirror(i):
        peer = order(i)
        return remote(
            q_send.at[heads - 1 - peer],
            q_all.at[spare],
            q_s.at[near(i)],
            q_r.at[spare],
            worker(peer),
        )

    def away_only(action):
        @pl.when(t != y)
        def _():
            action()

    for index in range(2):
        projected = project(index)
        for h in range(heads):
            kv_send[h, :, index * lanes : (index + 1) * lanes] = projected[
                :, h * lanes : (h + 1) * lanes
            ]

    @pl.when(home)
    def _():
        kv_all[s] = kv_send[plane]

    @pl.when(home)
    def _():
        kv_all[spare_block] = kv_send[mirror]

    meet()

    def block(slot, which):
        return kv_all.at[slot * RELAY + which]

    def arrived(dst, recv_sem):
        remote(dst, dst, stage_s.at[0], recv_sem, x_dev).wait_recv()

    def along_x(slot):
        here = block(slot, member)
        return remote(here, here, x_s.at[slot], x_r.at[slot], x_dev)

    def across(slot):
        here = block(slot, member)
        return remote(here, here, c_s.at[slot], c_r.at[slot], c_dev)

    def onward(slot):
        from_x = block(slot, member + 1 - 2 * x)
        return remote(from_x, from_x, d_s.at[slot], d_r.at[slot], c_dev)

    def forward_stage(slot):
        along_x(slot).start()
        across(slot).start()

    def receive(slot):
        arrived(block(slot, member), stage_r.at[slot])
        forward_stage(slot)

    def forward_square(slot):
        arrived(block(slot, member + 1 - 2 * x), x_r.at[slot])
        onward(slot).start()

    def finish_plane(slot):
        arrived(block(slot, lax.rem(member + 2, RELAY)), c_r.at[slot])
        arrived(block(slot, RELAY - 1 - member), d_r.at[slot])

    def first_sends():
        for k in range(1, half_planes):
            kv_copy(order(k)).start()

        @pl.when(low)
        def _():
            kv_copy(mirror).start()

    @pl.when(home)
    def _():
        forward_stage(plane)
        first_sends()

    away_only(lambda: kv_copy(plane).start())

    exponent = (lanes // 2) ** (-0.5) * math.log2(math.e)
    projected = project(2, scale * exponent)
    for h in range(heads):
        q_send[h] = projected[:, h * lanes : (h + 1) * lanes]

    @pl.when(home)
    def _():
        q_all[plane] = q_send[plane]

    @pl.when(home)
    def _():
        q_all[spare] = q_send[mirror]

    @pl.when(t != y)
    def _():
        q_copy(plane).start()
        first_sends()

    for k in range(1, half_planes):
        q_copy(order(k)).start()

    @pl.when(high)
    def _():
        for k in range(half_planes, heads):
            q_copy(order(k)).start()

    inner = project(3).astype(jnp.float32)
    signal_f = project(4).astype(jnp.float32)
    inner_sig[...] = (inner * signal_f).astype(jnp.bfloat16)
    tail = tail_in.shape[0]
    tail_copy = remote(
        inner_sig.at[pl.ds(rows - tail, tail)],
        tail_in,
        tail_sem.at[0],
        tail_sem.at[1],
        at(lax.rem(s + 1, sp_count)),
    )

    @pl.when(s < last)
    def _():
        tail_copy.start()

    @pl.when(low)
    def _():
        for k in range(half_planes + 1, heads):
            kv_copy(order(k)).start()

    @pl.when(home)
    def _():
        forward_stage(spare)

    @pl.when(t != y)
    def _():
        kv_mirror(0).start()
        q_mirror(0).start()

    for i in range(1, half_planes):
        kv_mirror(i).start()
        q_mirror(i).start()

    away_only(lambda: receive(plane))
    small[4].wait()
    outer[...] = project(5)
    gate = project(6).astype(jnp.float32)
    opened[...] = gate / (1.0 + jnp.exp(-gate)) * head_gain_ref[...]
    forward_square(plane)

    span = RELAY * rows
    lane = lax.broadcasted_iota(jnp.int32, (1, lanes), 1)
    masks = [
        of_map.astype(jnp.float32).astype(jnp.bfloat16)
        for of_map in (lane < lanes // 2, lane >= lanes // 2)
    ]

    def attend(tiles):
        def scores(qi, c, diagonal, m):
            keys = kv_all[pl.ds(c * RELAY, RELAY)].reshape(span, 2 * lanes)[:, :lanes]
            score = lax.dot_general(
                q_all[qi] * masks[m],
                keys,
                (((1,), (1,)), ((), ())),
                preferred_element_type=jnp.float32,
            )
            if diagonal:
                row = lax.broadcasted_iota(jnp.int32, (rows, span), 0) + member * rows
                col = lax.broadcasted_iota(jnp.int32, (rows, span), 1)
                score = jnp.where(row >= col, score, -1e30)
            return score

        def absorb(at_row, c, score):
            held = kv_all[pl.ds(c * RELAY, RELAY)].reshape(span, 2 * lanes)
            values = jnp.concatenate(
                [held[:, lanes:], jnp.ones((span, lanes), jnp.bfloat16)], axis=1
            )
            before = row_max[at_row]
            top = jnp.maximum(before, jnp.max(score, axis=-1, keepdims=True))
            weights = jnp.exp2(score - top[:, :1]).astype(jnp.bfloat16)
            factor = jnp.exp2(before - top)
            row_max[at_row] = top
            update = jnp.dot(weights, values, preferred_element_type=jnp.float32)
            for part in (slice(0, lanes), slice(lanes, 2 * lanes)):
                accum[at_row, :, part] = accum[at_row, :, part] * factor + update[:, part]

        items = [(*tile, m) for tile in tiles for m in range(2)]
        upcoming = scores(*items[0])
        for i, (qi, c, _, m) in enumerate(items):
            score = upcoming
            if i + 1 < len(items):
                upcoming = scores(*items[i + 1])
            absorb(2 * qi + m, c, score)

    def attend_triangle(base):
        below = [
            (base + i, base + j, False)
            for j in range(half_planes)
            for i in range(j + 1, half_planes)
        ]
        attend(below + [(base + i, base + i, True) for i in range(half_planes)])

    def attend_row(q):
        attend([(q, j, False) for j in range(half_planes)])

    lam_index = lax.broadcasted_iota(jnp.int32, (1, heads), 1)
    lam_out.wait()
    lam_row = jnp.where(home, lam_own[...], lam_other[...])

    def lambda_of(head):
        return jnp.sum(jnp.where(lam_index == head, lam_row, 0.0), axis=-1, keepdims=True)

    column = lax.broadcasted_iota(jnp.int32, (rows, lanes), 1)

    def slot_of(q, mirrored):
        return heads + q - own_base if mirrored else q

    def o_copies(q, mirrored):
        slot = slot_of(q, mirrored)
        head = mirror if mirrored else plane
        return [
            remote(o_send.at[slot], o_all.at[head], o_s.at[slot], o_r.at[head], worker(q)),
            remote(lt_send.at[slot], lt_all.at[head], lt_s.at[slot], lt_r.at[head], worker(q)),
        ]

    def p_copies(q, mirrored):
        at_row = q - half_planes
        to = half_planes + mirror if mirrored else plane
        return [
            remote(p_send.at[at_row], p_all.at[to], p_s.at[at_row], p_r.at[to], worker(q)),
            remote(pl_send.at[at_row], pl_all.at[to], pl_s.at[at_row], pl_r.at[to], worker(q)),
        ]

    def settle(q, copies, pairs):
        away = (q != plane) | (t != y)

        @pl.when(away)
        def _():
            for copy in copies:
                copy.start()

        @pl.when(jnp.logical_not(away))
        def _():
            for into, index, value in pairs:
                into[index] = value[...]

    def partial(q, mirrored):
        slot = slot_of(q, mirrored)
        at_row = q - half_planes
        logs = []
        for m in range(2):
            held = accum[2 * slot + m]
            total = held[:, lanes:]
            p_send[at_row, m * rows : (m + 1) * rows, :] = (held[:, :lanes] / total).astype(
                jnp.bfloat16
            )
            logs.append(jnp.log(total) + row_max[2 * slot + m] * math.log(2.0))
        turned = jnp.where(column == 0, logs[0], logs[1]).T
        pl_send[at_row] = turned[:2, :]
        if mirrored:
            to = half_planes + mirror
            settle(
                q,
                p_copies(q, mirrored),
                [(p_all, to, p_send.at[at_row]), (pl_all, to, pl_send.at[at_row])],
            )
        else:
            for copy in p_copies(q, mirrored):
                copy.start()

    def finalize(q, mirrored):
        slot = slot_of(q, mirrored)
        head = mirror if mirrored else plane
        maps = []
        logs = []
        for m in range(2):
            held = accum[2 * slot + m]
            total = held[:, lanes:]
            maps.append(held[:, :lanes] / total)
            logs.append(jnp.log(total) + row_max[2 * slot + m] * math.log(2.0))
        diff = maps[0] - lambda_of(head) * maps[1]
        mean = jnp.mean(diff * diff, axis=-1, keepdims=True)
        o_send[slot] = (diff * lax.rsqrt(mean + 1e-05)).astype(jnp.bfloat16)
        turned = jnp.where(column == 0, logs[0], logs[1]).T
        lt_send[slot] = turned[:2, :]
        settle(
            q,
            o_copies(q, mirrored),
            [(o_all, head, o_send.at[slot]), (lt_all, head, lt_send.at[slot])],
        )

    def q_arrived(slot):
        arrived(q_all.at[slot], q_r.at[slot])

    def convolve():
        small[3].wait()

        @pl.when(s > 0)
        def _():
            arrived(tail_in, tail_sem.at[1])

        @pl.when(s == 0)
        def _():
            tail_in[...] = jnp.zeros(tail_in.shape, jnp.bfloat16)

        lead = extended.shape[0] - rows
        extended[0:lead, :] = tail_in[tail - lead :, :].astype(jnp.float32)
        extended[lead:, :] = inner_sig[...].astype(jnp.float32)
        tap_count = taps_ref.shape[0]
        convolved = jnp.zeros((rows, local), jnp.float32)
        for position in range(tap_count):
            offset = lead - (tap_count - 1) + position
            convolved = convolved + taps_ref[position : position + 1, :] * extended[
                offset : offset + rows, :
            ]
        conv_out[...] = (outer[...].astype(jnp.float32) * convolved).astype(jnp.bfloat16)
        weight_copies[len(sources)].wait()
        conv_part[...] = jnp.dot(
            conv_out[...], wc_vmem[...], preferred_element_type=jnp.float32
        )

    def far_slots():
        return [order(k) for k in range(half_planes, heads)]

    for k in range(1, half_planes):
        receive(order(k))
    for k in range(1, half_planes):
        forward_square(order(k))
    for k in range(half_planes):
        finish_plane(order(k))

    @pl.when(low)
    def _():
        for slot in far_slots():
            q_arrived(slot)

        @pl.loop(half_planes, heads)
        def _(q):
            attend_row(q)
            partial(q, False)

    away_only(lambda: q_arrived(plane))
    for k in range(1, half_planes):
        q_arrived(order(k))
    attend_triangle(own_base)

    @pl.when(low)
    def _():
        @pl.loop(0, half_planes)
        def _(q):
            finalize(q, False)

    away_only(lambda: receive(spare))
    for k in range(1, half_planes):
        receive(near(k))

    @pl.when(high)
    def _():
        for slot in far_slots():
            receive(slot)

    convolve()
    for k in range(half_planes):
        forward_square(near(k))
    for k in range(half_planes):
        finish_plane(near(k))
        if k == 0:
            away_only(lambda: q_arrived(spare))
        else:
            q_arrived(near(k))
    attend_triangle(heads)

    @pl.when(low)
    def _():
        @pl.loop(0, half_planes)
        def _(q):
            finalize(q, True)

    @pl.when(high)
    def _():
        for slot in far_slots():
            forward_square(slot)

        @pl.loop(half_planes, heads)
        def _(q):
            partial(q, True)

        for slot in far_slots():
            finish_plane(slot)

        @pl.loop(half_planes, heads)
        def _(q):
            attend_row(q)
            finalize(q, False)

    weight_copies[len(sources) + 1].wait()
    half_rows = rows // 2

    def from_elsewhere(j):
        return (t != y) | ((j != plane) & (j != mirror))

    for j in range(heads):

        @pl.when(from_elsewhere(j) if j >= half_planes else (low & ((t != y) | (j != plane))))
        def _(j=j):
            arrived(o_all.at[j], o_r.at[j])
            arrived(lt_all.at[j], lt_r.at[j])

    def whole(h):
        totals_ref[h] = lt_all[h]
        part = slice(h * lanes, (h + 1) * lanes)
        head_out[:, part] = (o_all[h].astype(jnp.float32) * opened[:, part]).astype(jnp.bfloat16)

    def merged(h):
        arrived(p_all.at[h], p_r.at[h])
        arrived(pl_all.at[h], pl_r.at[h])
        second = half_planes + h

        @pl.when((t != y) | (h != mirror))
        def _():
            arrived(p_all.at[second], p_r.at[second])
            arrived(pl_all.at[second], pl_r.at[second])

        top = jnp.maximum(pl_all[h], pl_all[second])
        shares = [jnp.exp(pl_all[h] - top), jnp.exp(pl_all[second] - top)]
        total = shares[0] + shares[1]
        totals_ref[h] = top + jnp.log(total)
        turned = jnp.concatenate(
            [shares[0] / total, shares[1] / total, jnp.zeros((4, rows), jnp.float32)], axis=0
        ).T
        maps = []
        for m in range(2):
            held = slice(m * rows, (m + 1) * rows)
            maps.append(
                turned[:, m : m + 1] * p_all[h, held, :].astype(jnp.float32)
                + turned[:, 2 + m : 3 + m] * p_all[second, held, :].astype(jnp.float32)
            )
        diff = maps[0] - lam_own[:, h : h + 1] * maps[1]
        mean = jnp.mean(diff * diff, axis=-1, keepdims=True)
        part = slice(h * lanes, (h + 1) * lanes)
        head_out[:, part] = (diff * lax.rsqrt(mean + 1e-05) * opened[:, part]).astype(
            jnp.bfloat16
        )

    for h in range(half_planes, heads):
        whole(h)

    @pl.when(low)
    def _():
        for h in range(half_planes):
            whole(h)

    @pl.when(high)
    def _():
        for h in range(half_planes):
            merged(h)

    def partial_rows(which):
        there = pl.ds(pl.multiple_of(which * half_rows, half_rows), half_rows)
        attn = jnp.dot(head_out[there, :], wo_vmem[...], preferred_element_type=jnp.float32)
        return (attn + conv_part[there, :]).astype(jnp.bfloat16)

    part_send[...] = partial_rows(1 - t)
    exchange = remote(part_send, part_recv, part_sem.at[0], part_sem.at[1], c_dev)
    exchange.start()
    own_rows = partial_rows(t).astype(jnp.float32)
    exchange.wait()
    mixed_ref[...] = (own_rows + part_recv[...].astype(jnp.float32)).astype(jnp.bfloat16)
    def drain(slot):
        along_x(slot).wait_send()
        across(slot).wait_send()
        onward(slot).wait_send()

    def drain_o(q, copies):
        @pl.when((q != plane) | (t != y))
        def _():
            for copy in copies:
                copy.wait_send()

    for k in range(half_planes):

        def sent(k=k):
            kv_copy(order(k)).wait_send()
            q_copy(order(k)).wait_send()
            kv_mirror(k).wait_send()
            q_mirror(k).wait_send()

        if k == 0:
            away_only(sent)
        else:
            sent()
        drain(order(k))
        drain(near(k))

    @pl.when(low)
    def _():
        for slot in far_slots():
            kv_copy(slot).wait_send()
        for q in range(half_planes):
            drain_o(q, o_copies(q, False))
            drain_o(q, o_copies(q, True))
            for copy in p_copies(half_planes + q, False):
                copy.wait_send()

    @pl.when(high)
    def _():
        for slot in far_slots():
            q_copy(slot).wait_send()
            drain(slot)
        for q in range(half_planes, heads):
            drain_o(q, o_copies(q, False))
            drain_o(q, p_copies(q, True))

    @pl.when(s < last)
    def _():
        tail_copy.wait_send()


def fused(sp_count, *args):
    tokens, norm_gain, wq = args[0], args[1], args[2]
    lambdas, head_gain = args[10], args[11]
    rows, half = tokens.shape
    heads = lambdas.shape[0]
    local = wq.shape[1]
    lanes = local // heads
    slots = heads + heads // 2
    out_width = args[12].shape[1]
    bf16, f32 = jnp.bfloat16, jnp.float32
    vmem = pl.BlockSpec(memory_space=pltpu.VMEM)
    hbm = pl.BlockSpec(memory_space=pl.ANY)
    dma = pltpu.SemaphoreType.DMA
    operands = list(args)
    operands[1] = norm_gain.reshape(1, -1)
    operands[10] = lambdas.reshape(1, -1)
    operands[11] = head_gain.reshape(1, -1)
    return pl.pallas_call(
        functools.partial(fused_kernel, sp_count, heads),
        out_shape=(
            jax.ShapeDtypeStruct((rows // 2, out_width), bf16),
            jax.ShapeDtypeStruct((heads, 2, rows), f32),
        ),
        in_specs=[hbm] * len(operands),
        out_specs=(vmem, vmem),
        scratch_shapes=[
            pltpu.VMEM((rows, half), bf16),
            pltpu.VMEM((rows, half), bf16),
            pltpu.VMEM((1, 2 * half), f32),
            pltpu.VMEM(args[9].shape, f32),
            pltpu.VMEM((1, local), f32),
            pltpu.VMEM((1, heads), f32),
            pltpu.VMEM((1, heads), f32),
            pltpu.VMEM((rows, 2 * half), bf16),
            pltpu.VMEM((7,) + wq.shape, bf16),
            pltpu.VMEM(args[12].shape, bf16),
            pltpu.VMEM(args[13].shape, bf16),
            pltpu.VMEM((heads, rows, 2 * lanes), bf16),
            pltpu.VMEM((heads, rows, lanes), bf16),
            pltpu.VMEM((slots * RELAY, rows, 2 * lanes), bf16),
            pltpu.VMEM((slots, rows, lanes), bf16),
            pltpu.VMEM((2 * slots, rows, lanes), f32),
            pltpu.VMEM((2 * slots, rows, 2 * lanes), f32),
            pltpu.VMEM((rows, local), f32),
            pltpu.VMEM((rows, local), bf16),
            pltpu.VMEM((rows, local), bf16),
            pltpu.VMEM((16, local), bf16),
            pltpu.VMEM((rows + 8, local), f32),
            pltpu.VMEM((rows, local), bf16),
            pltpu.VMEM((rows, local), bf16),
            pltpu.VMEM((rows, out_width), f32),
            pltpu.VMEM((slots, rows, lanes), bf16),
            pltpu.VMEM((heads, rows, lanes), bf16),
            pltpu.VMEM((slots, 2, rows), f32),
            pltpu.VMEM((heads, 2, rows), f32),
            pltpu.VMEM((heads // 2, 2 * rows, lanes), bf16),
            pltpu.VMEM((heads, 2 * rows, lanes), bf16),
            pltpu.VMEM((heads // 2, 2, rows), f32),
            pltpu.VMEM((heads, 2, rows), f32),
            pltpu.VMEM((rows // 2, out_width), bf16),
            pltpu.VMEM((rows // 2, out_width), bf16),
            dma((9,)),
            dma((5,)),
            dma((4,)),
            dma((2,)),
            dma((2,)),
        ]
        + [dma((slots,)) for _ in range(18)]
        + [pltpu.SemaphoreType.REGULAR, pltpu.SemaphoreType.REGULAR],
        compiler_params=pltpu.CompilerParams(
            collective_id=0, has_side_effects=True, vmem_limit_bytes=60 * 1024 * 1024
        ),
    )(*operands)


def fits_square(mesh, heads, rows, key_columns, value_columns):
    return (
        mesh.shape["tp"] == 2
        and mesh.shape["sp"] == heads * RELAY
        and heads > 1
        and heads % 2 == 0
        and rows % 32 == 0
        and key_columns == value_columns == heads * 128
    )


def solution(mesh):
    placed = (
        P("sp", "tp"),
        P(),
        P(None, "tp"),
        P(None, "tp"),
        P(None, "tp"),
        P(None, "tp"),
        P(None, "tp"),
        P(None, "tp"),
        P(None, "tp"),
        P(None, "tp"),
        P("tp"),
        P("tp"),
        P("tp", None),
        P("tp", None),
    )

    def step(*args):
        heads = args[10].shape[0]
        if fits_square(mesh, heads, args[0].shape[0], args[2].shape[1], args[4].shape[1]):
            return fused(mesh.shape["sp"], *args)
        return per_device(*args)

    return jax.shard_map(
        step,
        mesh=mesh,
        in_specs=placed,
        out_specs=(P(("sp", "tp"), None), P("tp", None, "sp")),
        check_vma=False,
    )
```

```python
import functools
import math

import jax
import jax.numpy as jnp
from jax import lax
from jax.experimental import pallas as pl
from jax.experimental.pallas import tpu as pltpu
from jax.sharding import PartitionSpec as P

MESH = pl.DeviceIdType.MESH


def passed_along(shard, axis, by):
    count = lax.axis_size(axis)
    pairs = [(i, i + by) for i in range(count) if 0 <= i + by < count]
    return lax.ppermute(shard, axis, pairs)


def per_device(
    tokens,
    norm_gain,
    query_weight,
    key_weight,
    value_weight,
    gate_weight,
    outer_weight,
    inner_weight,
    signal_weight,
    conv_taps,
    lambdas,
    head_gain,
    attn_out_weight,
    conv_out_weight,
):
    row_count = tokens.shape[0]
    width = norm_gain.shape[0]
    weights = [
        query_weight,
        key_weight,
        value_weight,
        gate_weight,
        outer_weight,
        inner_weight,
        signal_weight,
    ]
    splits = []
    running = 0
    for weight in weights[:-1]:
        running = running + weight.shape[1]
        splits.append(running)
    joined = jnp.concatenate(weights, axis=1)
    empty = jnp.zeros((row_count, joined.shape[1]), jnp.float32)
    piece = lax.all_gather(tokens, "tp", axis=1, tiled=True)
    summed = empty
    piece_f = piece.astype(jnp.float32)
    normed_piece = (piece.astype(jnp.float32) * norm_gain).astype(jnp.bfloat16)
    raw = jnp.dot(normed_piece, joined, preferred_element_type=jnp.float32)
    squares = jnp.sum(piece_f * piece_f, axis=-1)
    scale = lax.rsqrt(squares / width + 1e-06)
    projected = (raw * scale[:, None]).astype(jnp.bfloat16)
    query, key, value, attn_gate, outer, inner, signal = jnp.split(projected, splits, axis=1)
    head_count = lambdas.shape[0]
    key_size = query_weight.shape[1] // (head_count * 2)
    value_size = value_weight.shape[1] // head_count
    score_scale = key_size ** (-0.5)
    own_index = lax.axis_index("sp")
    local_pos = jnp.arange(row_count, dtype=jnp.int32)
    query_parts = [query]
    position_parts = [own_index * row_count + local_pos]
    query_parts = [
        segment.reshape(segment.shape[0], head_count, 2, key_size) for segment in query_parts
    ]

    def absorb(current, query_rows, row_pos, key_block, value_block, key_pos):
        running_max, summed, accum = current
        score = (
            jnp.einsum("qhmd,khmd->hmqk", query_rows, key_block, preferred_element_type=jnp.float32)
            * score_scale
        )
        visible = row_pos[:, None] >= key_pos[None, :]
        masked = jnp.where(visible, score, -1e30)
        new_max = jnp.maximum(running_max, jnp.max(masked, axis=-1, keepdims=True))
        weights_now = jnp.where(visible, jnp.exp(masked - new_max), 0.0)
        factor = jnp.exp(running_max - new_max)
        summed = summed * factor + jnp.sum(weights_now, axis=-1, keepdims=True)
        accum = accum * factor + jnp.einsum(
            "hmqk,khd->hmqd",
            weights_now.astype(jnp.bfloat16),
            value_block,
            preferred_element_type=jnp.float32,
        )
        return (new_max, summed, accum)

    def fresh(rows):
        return (
            jnp.full((head_count, 2, rows, 1), -1e30, jnp.float32),
            jnp.zeros((head_count, 2, rows, 1), jnp.float32),
            jnp.zeros((head_count, 2, rows, value_size), jnp.float32),
        )

    start_states = tuple((fresh(segment.shape[0]) for segment in query_parts))
    carry = start_states
    key_piece = lax.all_gather(key, "sp", axis=0, tiled=True)
    value_piece = lax.all_gather(value, "sp", axis=0, tiled=True)
    length = key_piece.shape[0]
    block_len = 512
    key_blocks = key_piece.reshape(length // block_len, block_len, head_count, 2, key_size)
    value_blocks = value_piece.reshape(length // block_len, block_len, head_count, value_size)

    def one_block(states, item):
        key_block, value_block, block_id = item
        first_key = block_id * block_len
        key_pos = first_key + jnp.arange(block_len, dtype=jnp.int32)
        updated = []
        for current, query_rows, row_pos in zip(states, query_parts, position_parts):

            def compute(held, query_rows=query_rows, row_pos=row_pos):
                return absorb(held, query_rows, row_pos, key_block, value_block, key_pos)

            def unchanged(held):
                return held

            updated.append(
                lax.cond(first_key <= row_pos[row_pos.shape[0] - 1], compute, unchanged, current)
            )
        return (tuple(updated), None)

    carry, _ = lax.scan(
        one_block,
        carry,
        (key_blocks, value_blocks, jnp.arange(length // block_len, dtype=jnp.int32)),
    )
    states = carry
    running_max = jnp.concatenate([held[0] for held in states], axis=2)
    summed = jnp.concatenate([held[1] for held in states], axis=2)
    accum = jnp.concatenate([held[2] for held in states], axis=2)
    mapped = accum / summed
    diff = mapped[:, 0] - lambdas[:, None, None] * mapped[:, 1]
    log_totals = jnp.log(summed[..., 0]) + running_max[..., 0]
    diff = jnp.transpose(diff, (1, 0, 2))
    normed = (
        diff
        * lax.rsqrt(jnp.mean(diff * diff, axis=-1, keepdims=True) + 1e-05)
        * head_gain.reshape(head_count, value_size)
    )
    normed = normed.reshape(row_count, head_count * value_size)
    head_out = (normed * jax.nn.silu(attn_gate.astype(jnp.float32))).astype(jnp.bfloat16)
    taps = conv_taps.shape[0]
    inner_sig = (inner.astype(jnp.float32) * signal.astype(jnp.float32)).astype(jnp.bfloat16)
    before = passed_along(inner_sig[row_count - (taps - 1) :], "sp", 1)
    extended = jnp.concatenate([before, inner_sig], axis=0).astype(jnp.float32)
    convolved = jnp.zeros((row_count, inner_sig.shape[1]), jnp.float32)
    for position in range(taps):
        convolved = convolved + conv_taps[position] * extended[position : position + row_count]
    conv_out = (outer.astype(jnp.float32) * convolved).astype(jnp.bfloat16)
    mixed = lax.psum_scatter(
        (
            jnp.dot(head_out, attn_out_weight, preferred_element_type=jnp.float32)
            + jnp.dot(conv_out, conv_out_weight, preferred_element_type=jnp.float32)
        ).astype(jnp.bfloat16),
        "tp",
        scatter_dimension=0,
        tiled=True,
    )
    return (mixed, log_totals)


RELAY = 4
PIECES = 4


def fused_kernel(
    sp_count,
    heads,
    tokens_hbm,
    gain_hbm,
    wq_hbm,
    wk_hbm,
    wv_hbm,
    wg_hbm,
    wouter_hbm,
    winner_hbm,
    wsignal_hbm,
    taps_hbm,
    lambdas_hbm,
    head_gain_hbm,
    wo_hbm,
    wc_hbm,
    mixed_ref,
    totals_ref,
    own_tokens,
    other_tokens,
    gain_ref,
    taps_ref,
    head_gain_ref,
    lam_own,
    lam_other,
    normed,
    w_vmem,
    wo_vmem,
    wc_vmem,
    kv_send,
    q_send,
    kv_all,
    q_all,
    row_max,
    accum,
    opened,
    outer,
    inner_sig,
    tail_in,
    extended,
    conv_out,
    head_out,
    conv_part,
    o_send,
    o_all,
    lt_send,
    lt_all,
    p_send,
    p_all,
    pl_send,
    pl_all,
    part_send,
    part_recv,
    w_sem,
    in_sem,
    tok_sem,
    tail_sem,
    part_sem,
    stage_s,
    stage_r,
    q_s,
    q_r,
    x_s,
    x_r,
    c_s,
    c_r,
    d_s,
    d_r,
    o_s,
    o_r,
    lt_s,
    lt_r,
    p_s,
    p_r,
    pl_s,
    pl_r,
    pair_sem,
    met_sem,
):
    rows, half = own_tokens.shape
    width = 2 * half
    local = wq_hbm.shape[1]
    lanes = local // heads
    s = lax.axis_index("sp")
    t = lax.axis_index("tp")
    plane = s // RELAY
    place = lax.rem(s, RELAY)
    y = place // 2
    x = lax.rem(place, 2)
    member = 2 * t + x
    home = t == y
    low = plane < heads // 2
    high = plane >= heads // 2
    mirror = heads - 1 - plane
    last = sp_count - 1

    def at(sp_index, tp_index=None):
        return {"sp": sp_index, "tp": t if tp_index is None else tp_index}

    def remote(src, dst, send_sem, recv_sem, device):
        return pltpu.make_async_remote_copy(
            src_ref=src,
            dst_ref=dst,
            send_sem=send_sem,
            recv_sem=recv_sem,
            device_id=device,
            device_id_type=MESH,
        )

    def worker(j):
        return at(j * RELAY + member, y)

    x_sp = s + 1 - 2 * x
    x_dev = at(x_sp)
    c_dev = at(s, 1 - t)

    small = [
        pltpu.make_async_copy(ref, dst, in_sem.at[i])
        for i, (ref, dst) in enumerate(
            [
                (tokens_hbm, own_tokens),
                (gain_hbm, gain_ref),
                (lambdas_hbm, lam_own),
                (taps_hbm, taps_ref),
                (head_gain_hbm, head_gain_ref),
            ]
        )
    ]
    for copy in small:
        copy.start()
    sources = [wk_hbm, wv_hbm, wq_hbm, winner_hbm, wsignal_hbm, wouter_hbm, wg_hbm]
    weight_copies = [
        pltpu.make_async_copy(ref, w_vmem.at[i], w_sem.at[i]) for i, ref in enumerate(sources)
    ]
    weight_copies.append(pltpu.make_async_copy(wc_hbm, wc_vmem, w_sem.at[len(sources)]))
    weight_copies.append(pltpu.make_async_copy(wo_hbm, wo_vmem, w_sem.at[len(sources) + 1]))
    weight_copies[0].start()

    barrier = pltpu.get_barrier_semaphore()

    def signal(sem, device):
        pl.semaphore_signal(sem, inc=1, device_id=device, device_id_type=MESH)

    def greet(sp_index):
        signal(barrier, at(sp_index, 1))

    @pl.when(t == 1)
    def _():
        signal(barrier, at(s, 0))

    for step in range(1, heads):
        greet(lax.rem(plane + step, heads) * RELAY + member)

    @pl.when(t != y)
    def _():
        greet(plane * RELAY + member)

    greet(x_sp)

    @pl.when(s < last)
    def _():
        greet(s + 1)

    @pl.when(s > 0)
    def _():
        greet(s - 1)

    @pl.when(t == 0)
    def _():
        pl.semaphore_wait(barrier, 1)
        signal(pair_sem, at(s, 1))

    @pl.when(t == 1)
    def _():
        pl.semaphore_wait(pair_sem, 1)

    greetings = (
        2 * heads + 1 + 2 * jnp.where(s > 0, 1, 0) + 2 * jnp.where(s < last, 1, 0)
    )

    def meet():
        @pl.when(t == 1)
        def _():
            pl.semaphore_wait(barrier, greetings)
            signal(met_sem, at(s, 0))

        @pl.when(t == 0)
        def _():
            pl.semaphore_wait(met_sem, 1)

    small[0].wait()
    tokens_out = remote(own_tokens, other_tokens, tok_sem.at[0], tok_sem.at[1], c_dev)
    tokens_out.start()
    for copy in weight_copies[1:]:
        copy.start()
    small[2].wait()
    lam_out = remote(lam_own, lam_other, tok_sem.at[2], tok_sem.at[3], c_dev)
    lam_out.start()

    row_max[...] = jnp.full(row_max.shape, -1e30, jnp.float32)
    accum[...] = jnp.zeros(accum.shape, jnp.float32)

    small[1].wait()
    mine = pl.ds(pl.multiple_of(t * half, half), half)
    theirs = pl.ds(pl.multiple_of((1 - t) * half, half), half)
    own_f = own_tokens[...].astype(jnp.float32)
    squares = jnp.sum(own_f * own_f, axis=-1, keepdims=True)
    normed[:, mine] = (own_f * gain_ref[:, mine]).astype(jnp.bfloat16)
    tokens_out.wait()
    other_f = other_tokens[...].astype(jnp.float32)
    squares = squares + jnp.sum(other_f * other_f, axis=-1, keepdims=True)
    normed[:, theirs] = (other_f * gain_ref[:, theirs]).astype(jnp.bfloat16)
    scale = lax.rsqrt(squares / width + 1e-06)

    def project(index, scale=scale):
        weight_copies[index].wait()
        raw = jnp.dot(normed[...], w_vmem[index], preferred_element_type=jnp.float32)
        return (raw * scale).astype(jnp.bfloat16)

    half_planes = heads // 2
    own_base = jnp.where(low, 0, half_planes)
    far_base = half_planes - own_base

    def order(k):
        if k < half_planes:
            return own_base + lax.rem(plane - own_base + k, half_planes)
        return far_base + lax.rem(mirror - far_base + k - half_planes, half_planes)

    def q_copy(j):
        return remote(q_send.at[j], q_all.at[plane], q_s.at[j], q_r.at[plane], worker(j))

    def kv_copy(j):
        return remote(kv_send.at[j], kv_all.at[s], stage_s.at[j], stage_r.at[plane], worker(j))

    spare = heads + plane - own_base
    spare_block = spare * RELAY + place

    def near(k):
        return heads + order(k) - own_base

    def kv_mirror(i):
        peer = order(i)
        return remote(
            kv_send.at[heads - 1 - peer],
            kv_all.at[spare_block],
            stage_s.at[near(i)],
            stage_r.at[spare],
            worker(peer),
        )

    def q_mirror(i):
        peer = order(i)
        return remote(
            q_send.at[heads - 1 - peer],
            q_all.at[spare],
            q_s.at[near(i)],
            q_r.at[spare],
            worker(peer),
        )

    def away_only(action):
        @pl.when(t != y)
        def _():
            action()

    for index in range(2):
        projected = project(index)
        for h in range(heads):
            kv_send[h, :, index * lanes : (index + 1) * lanes] = projected[
                :, h * lanes : (h + 1) * lanes
            ]

    @pl.when(home)
    def _():
        kv_all[s] = kv_send[plane]

    @pl.when(home)
    def _():
        kv_all[spare_block] = kv_send[mirror]

    meet()

    def block(slot, which):
        return kv_all.at[slot * RELAY + which]

    def arrived(dst, recv_sem):
        remote(dst, dst, stage_s.at[0], recv_sem, x_dev).wait_recv()

    def along_x(slot):
        here = block(slot, member)
        return remote(here, here, x_s.at[slot], x_r.at[slot], x_dev)

    def across(slot):
        here = block(slot, member)
        return remote(here, here, c_s.at[slot], c_r.at[slot], c_dev)

    def onward(slot):
        from_x = block(slot, member + 1 - 2 * x)
        return remote(from_x, from_x, d_s.at[slot], d_r.at[slot], c_dev)

    def forward_stage(slot):
        along_x(slot).start()
        across(slot).start()

    def receive(slot):
        arrived(block(slot, member), stage_r.at[slot])
        forward_stage(slot)

    def forward_square(slot):
        arrived(block(slot, member + 1 - 2 * x), x_r.at[slot])
        onward(slot).start()

    def finish_plane(slot):
        arrived(block(slot, lax.rem(member + 2, RELAY)), c_r.at[slot])
        arrived(block(slot, RELAY - 1 - member), d_r.at[slot])

    def first_sends():
        for k in range(1, half_planes):
            kv_copy(order(k)).start()

        @pl.when(low)
        def _():
            kv_copy(mirror).start()

    @pl.when(home)
    def _():
        forward_stage(plane)
        first_sends()

    away_only(lambda: kv_copy(plane).start())

    exponent = (lanes // 2) ** (-0.5) * math.log2(math.e)
    projected = project(2, scale * exponent)
    for h in range(heads):
        q_send[h] = projected[:, h * lanes : (h + 1) * lanes]

    @pl.when(home)
    def _():
        q_all[plane] = q_send[plane]

    @pl.when(home)
    def _():
        q_all[spare] = q_send[mirror]

    @pl.when(t != y)
    def _():
        q_copy(plane).start()
        first_sends()

    for k in range(1, half_planes):
        q_copy(order(k)).start()

    @pl.when(high)
    def _():
        for k in range(half_planes, heads):
            q_copy(order(k)).start()

    inner = project(3).astype(jnp.float32)
    signal_f = project(4).astype(jnp.float32)
    inner_sig[...] = (inner * signal_f).astype(jnp.bfloat16)
    tail = tail_in.shape[0]
    tail_copy = remote(
        inner_sig.at[pl.ds(rows - tail, tail)],
        tail_in,
        tail_sem.at[0],
        tail_sem.at[1],
        at(lax.rem(s + 1, sp_count)),
    )

    @pl.when(s < last)
    def _():
        tail_copy.start()

    small[4].wait()
    outer[...] = project(5)
    gate = project(6).astype(jnp.float32)
    opened[...] = gate / (1.0 + jnp.exp(-gate)) * head_gain_ref[...]
    @pl.when(low)
    def _():
        for k in range(half_planes + 1, heads):
            kv_copy(order(k)).start()

    @pl.when(home)
    def _():
        forward_stage(spare)

    @pl.when(t != y)
    def _():
        kv_mirror(0).start()
        q_mirror(0).start()

    for i in range(1, half_planes):
        kv_mirror(i).start()
        q_mirror(i).start()

    away_only(lambda: receive(plane))
    for k in range(1, half_planes):
        receive(order(k))
    forward_square(plane)
    away_only(lambda: receive(spare))

    @pl.when(high)
    def _():
        receive(mirror)

    for k in range(1, half_planes):
        forward_square(order(k))
    for k in range(1, half_planes):
        receive(near(k))

    @pl.when(high)
    def _():
        for k in range(half_planes + 1, heads):
            receive(order(k))

    forward_square(spare)

    span = RELAY * rows
    lane = lax.broadcasted_iota(jnp.int32, (1, lanes), 1)
    masks = [
        of_map.astype(jnp.float32).astype(jnp.bfloat16)
        for of_map in (lane < lanes // 2, lane >= lanes // 2)
    ]

    def attend(tiles):
        def scores(qi, c, diagonal, m):
            keys = kv_all[pl.ds(c * RELAY, RELAY)].reshape(span, 2 * lanes)[:, :lanes]
            score = lax.dot_general(
                q_all[qi] * masks[m],
                keys,
                (((1,), (1,)), ((), ())),
                preferred_element_type=jnp.float32,
            )
            if diagonal:
                row = lax.broadcasted_iota(jnp.int32, (rows, span), 0) + member * rows
                col = lax.broadcasted_iota(jnp.int32, (rows, span), 1)
                score = jnp.where(row >= col, score, -1e30)
            return score

        def absorb(at_row, c, score):
            held = kv_all[pl.ds(c * RELAY, RELAY)].reshape(span, 2 * lanes)
            values = jnp.concatenate(
                [held[:, lanes:], jnp.ones((span, lanes), jnp.bfloat16)], axis=1
            )
            before = row_max[at_row]
            top = jnp.maximum(before, jnp.max(score, axis=-1, keepdims=True))
            weights = jnp.exp2(score - top[:, :1]).astype(jnp.bfloat16)
            factor = jnp.exp2(before - top)
            row_max[at_row] = top
            update = jnp.dot(weights, values, preferred_element_type=jnp.float32)
            for part in (slice(0, lanes), slice(lanes, 2 * lanes)):
                accum[at_row, :, part] = accum[at_row, :, part] * factor + update[:, part]

        items = [(*tile, m) for tile in tiles for m in range(2)]
        upcoming = scores(*items[0])
        for i, (qi, c, _, m) in enumerate(items):
            score = upcoming
            if i + 1 < len(items):
                upcoming = scores(*items[i + 1])
            absorb(2 * qi + m, c, score)

    def attend_triangle(base):
        below = [
            (base + i, base + j, False)
            for j in range(half_planes)
            for i in range(j + 1, half_planes)
        ]
        attend(below + [(base + i, base + i, True) for i in range(half_planes)])

    def attend_row(q):
        attend([(q, j, False) for j in range(half_planes)])

    lam_index = lax.broadcasted_iota(jnp.int32, (1, heads), 1)
    lam_out.wait()
    lam_row = jnp.where(home, lam_own[...], lam_other[...])

    def lambda_of(head):
        return jnp.sum(jnp.where(lam_index == head, lam_row, 0.0), axis=-1, keepdims=True)

    column = lax.broadcasted_iota(jnp.int32, (rows, lanes), 1)

    def slot_of(q, mirrored):
        return heads + q - own_base if mirrored else q

    def o_copies(q, mirrored):
        slot = slot_of(q, mirrored)
        head = mirror if mirrored else plane
        return [
            remote(o_send.at[slot], o_all.at[head], o_s.at[slot], o_r.at[head], worker(q)),
            remote(lt_send.at[slot], lt_all.at[head], lt_s.at[slot], lt_r.at[head], worker(q)),
        ]

    def p_copies(q, mirrored):
        at_row = q - half_planes
        to = half_planes + mirror if mirrored else plane
        return [
            remote(p_send.at[at_row], p_all.at[to], p_s.at[at_row], p_r.at[to], worker(q)),
            remote(pl_send.at[at_row], pl_all.at[to], pl_s.at[at_row], pl_r.at[to], worker(q)),
        ]

    def settle(q, copies, pairs):
        away = (q != plane) | (t != y)

        @pl.when(away)
        def _():
            for copy in copies:
                copy.start()

        @pl.when(jnp.logical_not(away))
        def _():
            for into, index, value in pairs:
                into[index] = value[...]

    def partial(q, mirrored):
        slot = slot_of(q, mirrored)
        at_row = q - half_planes
        logs = []
        for m in range(2):
            held = accum[2 * slot + m]
            total = held[:, lanes:]
            p_send[at_row, m * rows : (m + 1) * rows, :] = (held[:, :lanes] / total).astype(
                jnp.bfloat16
            )
            logs.append(jnp.log(total) + row_max[2 * slot + m] * math.log(2.0))
        turned = jnp.where(column == 0, logs[0], logs[1]).T
        pl_send[at_row] = turned[:2, :]
        if mirrored:
            to = half_planes + mirror
            settle(
                q,
                p_copies(q, mirrored),
                [(p_all, to, p_send.at[at_row]), (pl_all, to, pl_send.at[at_row])],
            )
        else:
            for copy in p_copies(q, mirrored):
                copy.start()

    def finalize(q, mirrored):
        slot = slot_of(q, mirrored)
        head = mirror if mirrored else plane
        maps = []
        logs = []
        for m in range(2):
            held = accum[2 * slot + m]
            total = held[:, lanes:]
            maps.append(held[:, :lanes] / total)
            logs.append(jnp.log(total) + row_max[2 * slot + m] * math.log(2.0))
        diff = maps[0] - lambda_of(head) * maps[1]
        mean = jnp.mean(diff * diff, axis=-1, keepdims=True)
        o_send[slot] = (diff * lax.rsqrt(mean + 1e-05)).astype(jnp.bfloat16)
        turned = jnp.where(column == 0, logs[0], logs[1]).T
        lt_send[slot] = turned[:2, :]
        settle(
            q,
            o_copies(q, mirrored),
            [(o_all, head, o_send.at[slot]), (lt_all, head, lt_send.at[slot])],
        )

    def q_arrived(slot):
        arrived(q_all.at[slot], q_r.at[slot])

    def convolve():
        small[3].wait()

        @pl.when(s > 0)
        def _():
            arrived(tail_in, tail_sem.at[1])

        @pl.when(s == 0)
        def _():
            tail_in[...] = jnp.zeros(tail_in.shape, jnp.bfloat16)

        lead = extended.shape[0] - rows
        extended[0:lead, :] = tail_in[tail - lead :, :].astype(jnp.float32)
        extended[lead:, :] = inner_sig[...].astype(jnp.float32)
        tap_count = taps_ref.shape[0]
        convolved = jnp.zeros((rows, local), jnp.float32)
        for position in range(tap_count):
            offset = lead - (tap_count - 1) + position
            convolved = convolved + taps_ref[position : position + 1, :] * extended[
                offset : offset + rows, :
            ]
        conv_out[...] = (outer[...].astype(jnp.float32) * convolved).astype(jnp.bfloat16)
        weight_copies[len(sources)].wait()
        conv_part[...] = jnp.dot(
            conv_out[...], wc_vmem[...], preferred_element_type=jnp.float32
        )

    def far_slots():
        return [order(k) for k in range(half_planes, heads)]

    for k in range(half_planes):
        finish_plane(order(k))

    @pl.when(low)
    def _():
        for slot in far_slots():
            q_arrived(slot)

        @pl.loop(half_planes, heads)
        def _(q):
            attend_row(q)
            partial(q, False)

    away_only(lambda: q_arrived(plane))
    for k in range(1, half_planes):
        q_arrived(order(k))
    attend_triangle(own_base)

    @pl.when(low)
    def _():
        @pl.loop(0, half_planes)
        def _(q):
            finalize(q, False)

    convolve()
    for k in range(1, half_planes):
        forward_square(near(k))
    for k in range(half_planes):
        finish_plane(near(k))
        if k == 0:
            away_only(lambda: q_arrived(spare))
        else:
            q_arrived(near(k))
    attend_triangle(heads)

    @pl.when(low)
    def _():
        @pl.loop(0, half_planes)
        def _(q):
            finalize(q, True)

    @pl.when(high)
    def _():
        for slot in far_slots():
            forward_square(slot)

        @pl.loop(half_planes, heads)
        def _(q):
            partial(q, True)

        for slot in far_slots():
            finish_plane(slot)

        attend([(half_planes + i, j, False) for j in range(half_planes) for i in range(half_planes)])

        @pl.loop(half_planes, heads)
        def _(q):
            finalize(q, False)

    weight_copies[len(sources) + 1].wait()
    half_rows = rows // 2

    def from_worker(j, here):
        @pl.when((t != y) | (plane != here))
        def _():
            arrived(o_all.at[j], o_r.at[j])
            arrived(lt_all.at[j], lt_r.at[j])

    def whole(h):
        totals_ref[h] = lt_all[h]
        part = slice(h * lanes, (h + 1) * lanes)
        head_out[:, part] = (o_all[h].astype(jnp.float32) * opened[:, part]).astype(jnp.bfloat16)

    def merged(h):
        arrived(p_all.at[h], p_r.at[h])
        arrived(pl_all.at[h], pl_r.at[h])
        second = half_planes + h

        @pl.when((t != y) | (h != mirror))
        def _():
            arrived(p_all.at[second], p_r.at[second])
            arrived(pl_all.at[second], pl_r.at[second])

        top = jnp.maximum(pl_all[h], pl_all[second])
        shares = [jnp.exp(pl_all[h] - top), jnp.exp(pl_all[second] - top)]
        total = shares[0] + shares[1]
        totals_ref[h] = top + jnp.log(total)
        turned = jnp.concatenate(
            [shares[0] / total, shares[1] / total, jnp.zeros((4, rows), jnp.float32)], axis=0
        ).T
        maps = []
        for m in range(2):
            held = slice(m * rows, (m + 1) * rows)
            maps.append(
                turned[:, m : m + 1] * p_all[h, held, :].astype(jnp.float32)
                + turned[:, 2 + m : 3 + m] * p_all[second, held, :].astype(jnp.float32)
            )
        diff = maps[0] - lam_own[:, h : h + 1] * maps[1]
        mean = jnp.mean(diff * diff, axis=-1, keepdims=True)
        part = slice(h * lanes, (h + 1) * lanes)
        head_out[:, part] = (diff * lax.rsqrt(mean + 1e-05) * opened[:, part]).astype(
            jnp.bfloat16
        )

    split = half_planes * lanes

    @pl.when(low)
    def _():
        for h in range(half_planes):
            from_worker(h, h)
            whole(h)

    @pl.when(high)
    def _():
        for h in range(half_planes):
            merged(h)

    conv_part[...] += jnp.dot(
        head_out[:, :split], wo_vmem[:split, :], preferred_element_type=jnp.float32
    )
    for h in range(half_planes, heads):

        @pl.when(low)
        def _(h=h):
            from_worker(h, heads - 1 - h)

        @pl.when(high)
        def _(h=h):
            from_worker(h, h)

        whole(h)

    pieces, _, breadth = part_send.shape

    def partial_rows(which, piece):
        there = pl.ds(pl.multiple_of(which * half_rows, half_rows), half_rows)
        columns = slice(piece * breadth, (piece + 1) * breadth)
        attn = jnp.dot(
            head_out[there, split:], wo_vmem[split:, columns], preferred_element_type=jnp.float32
        )
        return (attn + conv_part[there, columns]).astype(jnp.bfloat16)

    exchanges = [
        remote(part_send.at[i], part_recv.at[i], part_sem.at[i], part_sem.at[pieces + i], c_dev)
        for i in range(pieces)
    ]
    for i in range(pieces):
        part_send[i] = partial_rows(1 - t, i)
        exchanges[i].start()
    for i in range(pieces):
        own_rows = partial_rows(t, i).astype(jnp.float32)
        exchanges[i].wait()
        mixed_ref[:, i * breadth : (i + 1) * breadth] = (
            own_rows + part_recv[i].astype(jnp.float32)
        ).astype(jnp.bfloat16)

    def drain(slot):
        along_x(slot).wait_send()
        across(slot).wait_send()
        onward(slot).wait_send()

    def drain_o(q, copies):
        @pl.when((q != plane) | (t != y))
        def _():
            for copy in copies:
                copy.wait_send()

    for k in range(half_planes):

        def sent(k=k):
            kv_copy(order(k)).wait_send()
            q_copy(order(k)).wait_send()
            kv_mirror(k).wait_send()
            q_mirror(k).wait_send()

        if k == 0:
            away_only(sent)
        else:
            sent()
        drain(order(k))
        drain(near(k))

    @pl.when(low)
    def _():
        for slot in far_slots():
            kv_copy(slot).wait_send()
        for q in range(half_planes):
            drain_o(q, o_copies(q, False))
            drain_o(q, o_copies(q, True))
            for copy in p_copies(half_planes + q, False):
                copy.wait_send()

    @pl.when(high)
    def _():
        for slot in far_slots():
            q_copy(slot).wait_send()
            drain(slot)
        for q in range(half_planes, heads):
            drain_o(q, o_copies(q, False))
            drain_o(q, p_copies(q, True))

    @pl.when(s < last)
    def _():
        tail_copy.wait_send()


def fused(sp_count, *args):
    tokens, norm_gain, wq = args[0], args[1], args[2]
    lambdas, head_gain = args[10], args[11]
    rows, half = tokens.shape
    heads = lambdas.shape[0]
    local = wq.shape[1]
    lanes = local // heads
    slots = heads + heads // 2
    out_width = args[12].shape[1]
    bf16, f32 = jnp.bfloat16, jnp.float32
    vmem = pl.BlockSpec(memory_space=pltpu.VMEM)
    hbm = pl.BlockSpec(memory_space=pl.ANY)
    dma = pltpu.SemaphoreType.DMA
    operands = list(args)
    operands[1] = norm_gain.reshape(1, -1)
    operands[10] = lambdas.reshape(1, -1)
    operands[11] = head_gain.reshape(1, -1)
    return pl.pallas_call(
        functools.partial(fused_kernel, sp_count, heads),
        out_shape=(
            jax.ShapeDtypeStruct((rows // 2, out_width), bf16),
            jax.ShapeDtypeStruct((heads, 2, rows), f32),
        ),
        in_specs=[hbm] * len(operands),
        out_specs=(vmem, vmem),
        scratch_shapes=[
            pltpu.VMEM((rows, half), bf16),
            pltpu.VMEM((rows, half), bf16),
            pltpu.VMEM((1, 2 * half), f32),
            pltpu.VMEM(args[9].shape, f32),
            pltpu.VMEM((1, local), f32),
            pltpu.VMEM((1, heads), f32),
            pltpu.VMEM((1, heads), f32),
            pltpu.VMEM((rows, 2 * half), bf16),
            pltpu.VMEM((7,) + wq.shape, bf16),
            pltpu.VMEM(args[12].shape, bf16),
            pltpu.VMEM(args[13].shape, bf16),
            pltpu.VMEM((heads, rows, 2 * lanes), bf16),
            pltpu.VMEM((heads, rows, lanes), bf16),
            pltpu.VMEM((slots * RELAY, rows, 2 * lanes), bf16),
            pltpu.VMEM((slots, rows, lanes), bf16),
            pltpu.VMEM((2 * slots, rows, lanes), f32),
            pltpu.VMEM((2 * slots, rows, 2 * lanes), f32),
            pltpu.VMEM((rows, local), f32),
            pltpu.VMEM((rows, local), bf16),
            pltpu.VMEM((rows, local), bf16),
            pltpu.VMEM((16, local), bf16),
            pltpu.VMEM((rows + 8, local), f32),
            pltpu.VMEM((rows, local), bf16),
            pltpu.VMEM((rows, local), bf16),
            pltpu.VMEM((rows, out_width), f32),
            pltpu.VMEM((slots, rows, lanes), bf16),
            pltpu.VMEM((heads, rows, lanes), bf16),
            pltpu.VMEM((slots, 2, rows), f32),
            pltpu.VMEM((heads, 2, rows), f32),
            pltpu.VMEM((heads // 2, 2 * rows, lanes), bf16),
            pltpu.VMEM((heads, 2 * rows, lanes), bf16),
            pltpu.VMEM((heads // 2, 2, rows), f32),
            pltpu.VMEM((heads, 2, rows), f32),
            pltpu.VMEM((PIECES, rows // 2, out_width // PIECES), bf16),
            pltpu.VMEM((PIECES, rows // 2, out_width // PIECES), bf16),
            dma((9,)),
            dma((5,)),
            dma((4,)),
            dma((2,)),
            dma((2 * PIECES,)),
        ]
        + [dma((slots,)) for _ in range(18)]
        + [pltpu.SemaphoreType.REGULAR, pltpu.SemaphoreType.REGULAR],
        compiler_params=pltpu.CompilerParams(
            collective_id=0, has_side_effects=True, vmem_limit_bytes=60 * 1024 * 1024
        ),
    )(*operands)


def fits_square(mesh, heads, rows, key_columns, value_columns):
    return (
        mesh.shape["tp"] == 2
        and mesh.shape["sp"] == heads * RELAY
        and heads > 1
        and heads % 2 == 0
        and rows % 32 == 0
        and key_columns == value_columns == heads * 128
    )


def solution(mesh):
    placed = (
        P("sp", "tp"),
        P(),
        P(None, "tp"),
        P(None, "tp"),
        P(None, "tp"),
        P(None, "tp"),
        P(None, "tp"),
        P(None, "tp"),
        P(None, "tp"),
        P(None, "tp"),
        P("tp"),
        P("tp"),
        P("tp", None),
        P("tp", None),
    )

    def step(*args):
        heads = args[10].shape[0]
        if fits_square(mesh, heads, args[0].shape[0], args[2].shape[1], args[4].shape[1]):
            return fused(mesh.shape["sp"], *args)
        return per_device(*args)

    return jax.shard_map(
        step,
        mesh=mesh,
        in_specs=placed,
        out_specs=(P(("sp", "tp"), None), P("tp", None, "sp")),
        check_vma=False,
    )
```

```python
import functools
import math

import jax
import jax.numpy as jnp
from jax import lax
from jax.experimental import pallas as pl
from jax.experimental.pallas import tpu as pltpu
from jax.sharding import PartitionSpec as P

MESH = pl.DeviceIdType.MESH


def passed_along(shard, axis, by):
    count = lax.axis_size(axis)
    pairs = [(i, i + by) for i in range(count) if 0 <= i + by < count]
    return lax.ppermute(shard, axis, pairs)


def per_device(
    tokens,
    norm_gain,
    query_weight,
    key_weight,
    value_weight,
    gate_weight,
    outer_weight,
    inner_weight,
    signal_weight,
    conv_taps,
    lambdas,
    head_gain,
    attn_out_weight,
    conv_out_weight,
):
    row_count = tokens.shape[0]
    width = norm_gain.shape[0]
    weights = [
        query_weight,
        key_weight,
        value_weight,
        gate_weight,
        outer_weight,
        inner_weight,
        signal_weight,
    ]
    splits = []
    running = 0
    for weight in weights[:-1]:
        running = running + weight.shape[1]
        splits.append(running)
    joined = jnp.concatenate(weights, axis=1)
    empty = jnp.zeros((row_count, joined.shape[1]), jnp.float32)
    piece = lax.all_gather(tokens, "tp", axis=1, tiled=True)
    summed = empty
    piece_f = piece.astype(jnp.float32)
    normed_piece = (piece.astype(jnp.float32) * norm_gain).astype(jnp.bfloat16)
    raw = jnp.dot(normed_piece, joined, preferred_element_type=jnp.float32)
    squares = jnp.sum(piece_f * piece_f, axis=-1)
    scale = lax.rsqrt(squares / width + 1e-06)
    projected = (raw * scale[:, None]).astype(jnp.bfloat16)
    query, key, value, attn_gate, outer, inner, signal = jnp.split(projected, splits, axis=1)
    head_count = lambdas.shape[0]
    key_size = query_weight.shape[1] // (head_count * 2)
    value_size = value_weight.shape[1] // head_count
    score_scale = key_size ** (-0.5)
    own_index = lax.axis_index("sp")
    local_pos = jnp.arange(row_count, dtype=jnp.int32)
    query_parts = [query]
    position_parts = [own_index * row_count + local_pos]
    query_parts = [
        segment.reshape(segment.shape[0], head_count, 2, key_size) for segment in query_parts
    ]

    def absorb(current, query_rows, row_pos, key_block, value_block, key_pos):
        running_max, summed, accum = current
        score = (
            jnp.einsum("qhmd,khmd->hmqk", query_rows, key_block, preferred_element_type=jnp.float32)
            * score_scale
        )
        visible = row_pos[:, None] >= key_pos[None, :]
        masked = jnp.where(visible, score, -1e30)
        new_max = jnp.maximum(running_max, jnp.max(masked, axis=-1, keepdims=True))
        weights_now = jnp.where(visible, jnp.exp(masked - new_max), 0.0)
        factor = jnp.exp(running_max - new_max)
        summed = summed * factor + jnp.sum(weights_now, axis=-1, keepdims=True)
        accum = accum * factor + jnp.einsum(
            "hmqk,khd->hmqd",
            weights_now.astype(jnp.bfloat16),
            value_block,
            preferred_element_type=jnp.float32,
        )
        return (new_max, summed, accum)

    def fresh(rows):
        return (
            jnp.full((head_count, 2, rows, 1), -1e30, jnp.float32),
            jnp.zeros((head_count, 2, rows, 1), jnp.float32),
            jnp.zeros((head_count, 2, rows, value_size), jnp.float32),
        )

    start_states = tuple((fresh(segment.shape[0]) for segment in query_parts))
    carry = start_states
    key_piece = lax.all_gather(key, "sp", axis=0, tiled=True)
    value_piece = lax.all_gather(value, "sp", axis=0, tiled=True)
    length = key_piece.shape[0]
    block_len = 512
    key_blocks = key_piece.reshape(length // block_len, block_len, head_count, 2, key_size)
    value_blocks = value_piece.reshape(length // block_len, block_len, head_count, value_size)

    def one_block(states, item):
        key_block, value_block, block_id = item
        first_key = block_id * block_len
        key_pos = first_key + jnp.arange(block_len, dtype=jnp.int32)
        updated = []
        for current, query_rows, row_pos in zip(states, query_parts, position_parts):

            def compute(held, query_rows=query_rows, row_pos=row_pos):
                return absorb(held, query_rows, row_pos, key_block, value_block, key_pos)

            def unchanged(held):
                return held

            updated.append(
                lax.cond(first_key <= row_pos[row_pos.shape[0] - 1], compute, unchanged, current)
            )
        return (tuple(updated), None)

    carry, _ = lax.scan(
        one_block,
        carry,
        (key_blocks, value_blocks, jnp.arange(length // block_len, dtype=jnp.int32)),
    )
    states = carry
    running_max = jnp.concatenate([held[0] for held in states], axis=2)
    summed = jnp.concatenate([held[1] for held in states], axis=2)
    accum = jnp.concatenate([held[2] for held in states], axis=2)
    mapped = accum / summed
    diff = mapped[:, 0] - lambdas[:, None, None] * mapped[:, 1]
    log_totals = jnp.log(summed[..., 0]) + running_max[..., 0]
    diff = jnp.transpose(diff, (1, 0, 2))
    normed = (
        diff
        * lax.rsqrt(jnp.mean(diff * diff, axis=-1, keepdims=True) + 1e-05)
        * head_gain.reshape(head_count, value_size)
    )
    normed = normed.reshape(row_count, head_count * value_size)
    head_out = (normed * jax.nn.silu(attn_gate.astype(jnp.float32))).astype(jnp.bfloat16)
    taps = conv_taps.shape[0]
    inner_sig = (inner.astype(jnp.float32) * signal.astype(jnp.float32)).astype(jnp.bfloat16)
    before = passed_along(inner_sig[row_count - (taps - 1) :], "sp", 1)
    extended = jnp.concatenate([before, inner_sig], axis=0).astype(jnp.float32)
    convolved = jnp.zeros((row_count, inner_sig.shape[1]), jnp.float32)
    for position in range(taps):
        convolved = convolved + conv_taps[position] * extended[position : position + row_count]
    conv_out = (outer.astype(jnp.float32) * convolved).astype(jnp.bfloat16)
    mixed = lax.psum_scatter(
        (
            jnp.dot(head_out, attn_out_weight, preferred_element_type=jnp.float32)
            + jnp.dot(conv_out, conv_out_weight, preferred_element_type=jnp.float32)
        ).astype(jnp.bfloat16),
        "tp",
        scatter_dimension=0,
        tiled=True,
    )
    return (mixed, log_totals)


RELAY = 4
PIECES = 4


def fused_kernel(
    sp_count,
    heads,
    tokens_hbm,
    gain_hbm,
    wq_hbm,
    wk_hbm,
    wv_hbm,
    wg_hbm,
    wouter_hbm,
    winner_hbm,
    wsignal_hbm,
    taps_hbm,
    lambdas_hbm,
    head_gain_hbm,
    wo_hbm,
    wc_hbm,
    mixed_ref,
    totals_ref,
    own_tokens,
    other_tokens,
    gain_ref,
    taps_ref,
    head_gain_ref,
    lam_own,
    lam_other,
    normed,
    w_vmem,
    wo_vmem,
    wc_vmem,
    kv_send,
    q_send,
    kv_all,
    q_all,
    row_max,
    accum,
    opened,
    outer,
    inner_sig,
    tail_in,
    extended,
    conv_out,
    head_out,
    conv_part,
    o_send,
    o_all,
    lt_send,
    lt_all,
    p_send,
    p_all,
    pl_send,
    pl_all,
    part_send,
    part_recv,
    w_sem,
    in_sem,
    tok_sem,
    tail_sem,
    part_sem,
    stage_s,
    stage_r,
    q_s,
    q_r,
    x_s,
    x_r,
    c_s,
    c_r,
    d_s,
    d_r,
    o_s,
    o_r,
    lt_s,
    lt_r,
    p_s,
    p_r,
    pl_s,
    pl_r,
    pair_sem,
    met_sem,
):
    rows, half = own_tokens.shape
    width = 2 * half
    local = wq_hbm.shape[1]
    lanes = local // heads
    s = lax.axis_index("sp")
    t = lax.axis_index("tp")
    plane = s // RELAY
    place = lax.rem(s, RELAY)
    y = place // 2
    x = lax.rem(place, 2)
    member = 2 * t + x
    home = t == y
    low = plane < heads // 2
    high = plane >= heads // 2
    mirror = heads - 1 - plane
    last = sp_count - 1

    def at(sp_index, tp_index=None):
        return {"sp": sp_index, "tp": t if tp_index is None else tp_index}

    def remote(src, dst, send_sem, recv_sem, device):
        return pltpu.make_async_remote_copy(
            src_ref=src,
            dst_ref=dst,
            send_sem=send_sem,
            recv_sem=recv_sem,
            device_id=device,
            device_id_type=MESH,
        )

    def worker(j):
        return at(j * RELAY + member, y)

    x_sp = s + 1 - 2 * x
    x_dev = at(x_sp)
    c_dev = at(s, 1 - t)

    small = [
        pltpu.make_async_copy(ref, dst, in_sem.at[i])
        for i, (ref, dst) in enumerate(
            [
                (tokens_hbm, own_tokens),
                (gain_hbm, gain_ref),
                (lambdas_hbm, lam_own),
                (taps_hbm, taps_ref),
                (head_gain_hbm, head_gain_ref),
            ]
        )
    ]
    for copy in small:
        copy.start()
    sources = [wk_hbm, wv_hbm, wq_hbm, winner_hbm, wsignal_hbm, wouter_hbm, wg_hbm]
    weight_copies = [
        pltpu.make_async_copy(ref, w_vmem.at[i], w_sem.at[i]) for i, ref in enumerate(sources)
    ]
    weight_copies.append(pltpu.make_async_copy(wc_hbm, wc_vmem, w_sem.at[len(sources)]))
    weight_copies.append(pltpu.make_async_copy(wo_hbm, wo_vmem, w_sem.at[len(sources) + 1]))
    weight_copies[0].start()

    barrier = pltpu.get_barrier_semaphore()

    def signal(sem, device):
        pl.semaphore_signal(sem, inc=1, device_id=device, device_id_type=MESH)

    def greet(sp_index):
        signal(barrier, at(sp_index, 1))

    @pl.when(t == 1)
    def _():
        signal(barrier, at(s, 0))

    for step in range(1, heads):
        greet(lax.rem(plane + step, heads) * RELAY + member)

    @pl.when(t != y)
    def _():
        greet(plane * RELAY + member)

    greet(x_sp)

    @pl.when(s < last)
    def _():
        greet(s + 1)

    @pl.when(s > 0)
    def _():
        greet(s - 1)

    @pl.when(t == 0)
    def _():
        pl.semaphore_wait(barrier, 1)
        signal(pair_sem, at(s, 1))

    @pl.when(t == 1)
    def _():
        pl.semaphore_wait(pair_sem, 1)

    greetings = (
        2 * heads + 1 + 2 * jnp.where(s > 0, 1, 0) + 2 * jnp.where(s < last, 1, 0)
    )

    def meet():
        @pl.when(t == 1)
        def _():
            pl.semaphore_wait(barrier, greetings)
            signal(met_sem, at(s, 0))

        @pl.when(t == 0)
        def _():
            pl.semaphore_wait(met_sem, 1)

    small[0].wait()
    tokens_out = remote(own_tokens, other_tokens, tok_sem.at[0], tok_sem.at[1], c_dev)
    tokens_out.start()
    for copy in weight_copies[1:]:
        copy.start()
    small[2].wait()
    lam_out = remote(lam_own, lam_other, tok_sem.at[2], tok_sem.at[3], c_dev)
    lam_out.start()

    row_max[...] = jnp.full(row_max.shape, -1e30, jnp.float32)
    accum[...] = jnp.zeros(accum.shape, jnp.float32)

    small[1].wait()
    mine = pl.ds(pl.multiple_of(t * half, half), half)
    theirs = pl.ds(pl.multiple_of((1 - t) * half, half), half)
    own_f = own_tokens[...].astype(jnp.float32)
    squares = jnp.sum(own_f * own_f, axis=-1, keepdims=True)
    normed[:, mine] = (own_f * gain_ref[:, mine]).astype(jnp.bfloat16)
    tokens_out.wait()
    other_f = other_tokens[...].astype(jnp.float32)
    squares = squares + jnp.sum(other_f * other_f, axis=-1, keepdims=True)
    normed[:, theirs] = (other_f * gain_ref[:, theirs]).astype(jnp.bfloat16)
    scale = lax.rsqrt(squares / width + 1e-06)

    def project(index, scale=scale):
        weight_copies[index].wait()
        raw = jnp.dot(normed[...], w_vmem[index], preferred_element_type=jnp.float32)
        return (raw * scale).astype(jnp.bfloat16)

    half_planes = heads // 2
    own_base = jnp.where(low, 0, half_planes)
    far_base = half_planes - own_base

    def order(k):
        if k < half_planes:
            return own_base + lax.rem(plane - own_base + k, half_planes)
        return far_base + lax.rem(mirror - far_base + k - half_planes, half_planes)

    def q_copy(j):
        return remote(q_send.at[j], q_all.at[plane], q_s.at[j], q_r.at[plane], worker(j))

    def kv_copy(j):
        return remote(kv_send.at[j], kv_all.at[s], stage_s.at[j], stage_r.at[plane], worker(j))

    spare = heads + plane - own_base
    spare_block = spare * RELAY + place

    def near(k):
        return heads + order(k) - own_base

    def kv_mirror(i):
        peer = order(i)
        return remote(
            kv_send.at[heads - 1 - peer],
            kv_all.at[spare_block],
            stage_s.at[near(i)],
            stage_r.at[spare],
            worker(peer),
        )

    def q_mirror(i):
        peer = order(i)
        return remote(
            q_send.at[heads - 1 - peer],
            q_all.at[spare],
            q_s.at[near(i)],
            q_r.at[spare],
            worker(peer),
        )

    def away_only(action):
        @pl.when(t != y)
        def _():
            action()

    for index in range(2):
        projected = project(index)
        for h in range(heads):
            kv_send[h, :, index * lanes : (index + 1) * lanes] = projected[
                :, h * lanes : (h + 1) * lanes
            ]

    @pl.when(home)
    def _():
        kv_all[s] = kv_send[plane]

    @pl.when(home)
    def _():
        kv_all[spare_block] = kv_send[mirror]

    meet()

    def block(slot, which):
        return kv_all.at[slot * RELAY + which]

    def arrived(dst, recv_sem):
        remote(dst, dst, stage_s.at[0], recv_sem, x_dev).wait_recv()

    def along_x(slot):
        here = block(slot, member)
        return remote(here, here, x_s.at[slot], x_r.at[slot], x_dev)

    def across(slot):
        here = block(slot, member)
        return remote(here, here, c_s.at[slot], c_r.at[slot], c_dev)

    def onward(slot):
        from_x = block(slot, member + 1 - 2 * x)
        return remote(from_x, from_x, d_s.at[slot], d_r.at[slot], c_dev)

    def forward_stage(slot):
        along_x(slot).start()
        across(slot).start()

    def receive(slot):
        arrived(block(slot, member), stage_r.at[slot])
        forward_stage(slot)

    def forward_square(slot):
        arrived(block(slot, member + 1 - 2 * x), x_r.at[slot])
        onward(slot).start()

    def finish_plane(slot):
        arrived(block(slot, lax.rem(member + 2, RELAY)), c_r.at[slot])
        arrived(block(slot, RELAY - 1 - member), d_r.at[slot])

    def first_sends():
        for k in range(1, half_planes):
            kv_copy(order(k)).start()

        @pl.when(low)
        def _():
            kv_copy(mirror).start()

    @pl.when(home)
    def _():
        forward_stage(plane)
        first_sends()

    away_only(lambda: kv_copy(plane).start())

    exponent = (lanes // 2) ** (-0.5) * math.log2(math.e)
    projected = project(2, scale * exponent)
    for h in range(heads):
        q_send[h] = projected[:, h * lanes : (h + 1) * lanes]

    @pl.when(home)
    def _():
        q_all[plane] = q_send[plane]

    @pl.when(home)
    def _():
        q_all[spare] = q_send[mirror]

    @pl.when(t != y)
    def _():
        q_copy(plane).start()
        first_sends()

    for k in range(1, half_planes):
        q_copy(order(k)).start()

    @pl.when(high)
    def _():
        for k in range(half_planes, heads):
            q_copy(order(k)).start()

    inner = project(3).astype(jnp.float32)
    signal_f = project(4).astype(jnp.float32)
    inner_sig[...] = (inner * signal_f).astype(jnp.bfloat16)
    tail = tail_in.shape[0]
    tail_copy = remote(
        inner_sig.at[pl.ds(rows - tail, tail)],
        tail_in,
        tail_sem.at[0],
        tail_sem.at[1],
        at(lax.rem(s + 1, sp_count)),
    )

    @pl.when(s < last)
    def _():
        tail_copy.start()

    small[4].wait()
    outer[...] = project(5)
    gate = project(6).astype(jnp.float32)
    opened[...] = gate / (1.0 + jnp.exp(-gate)) * head_gain_ref[...]
    @pl.when(low)
    def _():
        for k in range(half_planes + 1, heads):
            kv_copy(order(k)).start()

    @pl.when(home)
    def _():
        forward_stage(spare)

    @pl.when(t != y)
    def _():
        kv_mirror(0).start()
        q_mirror(0).start()

    for i in range(1, half_planes):
        kv_mirror(i).start()
        q_mirror(i).start()

    away_only(lambda: receive(plane))
    for k in range(1, half_planes):
        receive(order(k))
    forward_square(plane)
    away_only(lambda: receive(spare))

    @pl.when(high)
    def _():
        receive(mirror)

    for k in range(1, half_planes):
        forward_square(order(k))
    for k in range(1, half_planes):
        receive(near(k))

    @pl.when(high)
    def _():
        for k in range(half_planes + 1, heads):
            receive(order(k))

    forward_square(spare)

    span = RELAY * rows
    lane = lax.broadcasted_iota(jnp.int32, (1, lanes), 1)
    masks = [
        of_map.astype(jnp.float32).astype(jnp.bfloat16)
        for of_map in (lane < lanes // 2, lane >= lanes // 2)
    ]

    def attend(tiles):
        def scores(qi, c, diagonal, m):
            keys = kv_all[pl.ds(c * RELAY, RELAY)].reshape(span, 2 * lanes)[:, :lanes]
            score = lax.dot_general(
                q_all[qi] * masks[m],
                keys,
                (((1,), (1,)), ((), ())),
                preferred_element_type=jnp.float32,
            )
            if diagonal:
                row = lax.broadcasted_iota(jnp.int32, (rows, span), 0) + member * rows
                col = lax.broadcasted_iota(jnp.int32, (rows, span), 1)
                score = jnp.where(row >= col, score, -1e30)
            return score

        def absorb(at_row, c, score):
            held = kv_all[pl.ds(c * RELAY, RELAY)].reshape(span, 2 * lanes)
            values = jnp.concatenate(
                [held[:, lanes:], jnp.ones((span, lanes), jnp.bfloat16)], axis=1
            )
            before = row_max[at_row]
            top = jnp.maximum(before, jnp.max(score, axis=-1, keepdims=True))
            weights = jnp.exp2(score - top[:, :1]).astype(jnp.bfloat16)
            factor = jnp.exp2(before - top)
            row_max[at_row] = top
            update = jnp.dot(weights, values, preferred_element_type=jnp.float32)
            for part in (slice(0, lanes), slice(lanes, 2 * lanes)):
                accum[at_row, :, part] = accum[at_row, :, part] * factor + update[:, part]

        items = [(*tile, m) for tile in tiles for m in range(2)]
        upcoming = scores(*items[0])
        for i, (qi, c, _, m) in enumerate(items):
            score = upcoming
            if i + 1 < len(items):
                upcoming = scores(*items[i + 1])
            absorb(2 * qi + m, c, score)

    def attend_triangle(base):
        below = [
            (base + i, base + j, False)
            for j in range(half_planes)
            for i in range(j + 1, half_planes)
        ]
        attend(below + [(base + i, base + i, True) for i in range(half_planes)])

    def attend_row(q):
        attend([(q, j, False) for j in range(half_planes)])

    lam_index = lax.broadcasted_iota(jnp.int32, (1, heads), 1)
    lam_out.wait()
    lam_row = jnp.where(home, lam_own[...], lam_other[...])

    def lambda_of(head):
        return jnp.sum(jnp.where(lam_index == head, lam_row, 0.0), axis=-1, keepdims=True)

    column = lax.broadcasted_iota(jnp.int32, (rows, lanes), 1)

    def slot_of(q, mirrored):
        return heads + q - own_base if mirrored else q

    def o_copies(q, mirrored):
        slot = slot_of(q, mirrored)
        head = mirror if mirrored else plane
        return [
            remote(o_send.at[slot], o_all.at[head], o_s.at[slot], o_r.at[head], worker(q)),
            remote(lt_send.at[slot], lt_all.at[head], lt_s.at[slot], lt_r.at[head], worker(q)),
        ]

    def p_copies(q, mirrored):
        at_row = q - half_planes
        to = half_planes + mirror if mirrored else plane
        return [
            remote(p_send.at[at_row], p_all.at[to], p_s.at[at_row], p_r.at[to], worker(q)),
            remote(pl_send.at[at_row], pl_all.at[to], pl_s.at[at_row], pl_r.at[to], worker(q)),
        ]

    def settle(q, copies, pairs):
        away = (q != plane) | (t != y)

        @pl.when(away)
        def _():
            for copy in copies:
                copy.start()

        @pl.when(jnp.logical_not(away))
        def _():
            for into, index, value in pairs:
                into[index] = value[...]

    def partial(q, mirrored):
        slot = slot_of(q, mirrored)
        at_row = q - half_planes
        logs = []
        for m in range(2):
            held = accum[2 * slot + m]
            total = held[:, lanes:]
            p_send[at_row, m * rows : (m + 1) * rows, :] = (held[:, :lanes] / total).astype(
                jnp.bfloat16
            )
            logs.append(jnp.log(total) + row_max[2 * slot + m] * math.log(2.0))
        turned = jnp.where(column == 0, logs[0], logs[1]).T
        pl_send[at_row] = turned[:2, :]
        if mirrored:
            to = half_planes + mirror
            settle(
                q,
                p_copies(q, mirrored),
                [(p_all, to, p_send.at[at_row]), (pl_all, to, pl_send.at[at_row])],
            )
        else:
            for copy in p_copies(q, mirrored):
                copy.start()

    def finalize(q, mirrored):
        slot = slot_of(q, mirrored)
        head = mirror if mirrored else plane
        maps = []
        logs = []
        for m in range(2):
            held = accum[2 * slot + m]
            total = held[:, lanes:]
            maps.append(held[:, :lanes] / total)
            logs.append(jnp.log(total) + row_max[2 * slot + m] * math.log(2.0))
        diff = maps[0] - lambda_of(head) * maps[1]
        mean = jnp.mean(diff * diff, axis=-1, keepdims=True)
        o_send[slot] = (diff * lax.rsqrt(mean + 1e-05)).astype(jnp.bfloat16)
        turned = jnp.where(column == 0, logs[0], logs[1]).T
        lt_send[slot] = turned[:2, :]
        settle(
            q,
            o_copies(q, mirrored),
            [(o_all, head, o_send.at[slot]), (lt_all, head, lt_send.at[slot])],
        )

    def q_arrived(slot):
        arrived(q_all.at[slot], q_r.at[slot])

    def convolve():
        small[3].wait()

        @pl.when(s > 0)
        def _():
            arrived(tail_in, tail_sem.at[1])

        @pl.when(s == 0)
        def _():
            tail_in[...] = jnp.zeros(tail_in.shape, jnp.bfloat16)

        lead = extended.shape[0] - rows
        extended[0:lead, :] = tail_in[tail - lead :, :].astype(jnp.float32)
        extended[lead:, :] = inner_sig[...].astype(jnp.float32)
        tap_count = taps_ref.shape[0]
        convolved = jnp.zeros((rows, local), jnp.float32)
        for position in range(tap_count):
            offset = lead - (tap_count - 1) + position
            convolved = convolved + taps_ref[position : position + 1, :] * extended[
                offset : offset + rows, :
            ]
        conv_out[...] = (outer[...].astype(jnp.float32) * convolved).astype(jnp.bfloat16)
        weight_copies[len(sources)].wait()
        conv_part[...] = jnp.dot(
            conv_out[...], wc_vmem[...], preferred_element_type=jnp.float32
        )

    def far_slots():
        return [order(k) for k in range(half_planes, heads)]

    for k in range(half_planes):
        finish_plane(order(k))

    @pl.when(low)
    def _():
        for slot in far_slots():
            q_arrived(slot)

        @pl.loop(half_planes, heads)
        def _(q):
            attend_row(q)
            partial(q, False)

    away_only(lambda: q_arrived(plane))
    for k in range(1, half_planes):
        q_arrived(order(k))
    attend_triangle(own_base)

    @pl.when(low)
    def _():
        @pl.loop(0, half_planes)
        def _(q):
            finalize(q, False)

    convolve()
    for k in range(1, half_planes):
        forward_square(near(k))
    for k in range(half_planes):
        finish_plane(near(k))
        if k == 0:
            away_only(lambda: q_arrived(spare))
        else:
            q_arrived(near(k))
    attend_triangle(heads)

    @pl.when(low)
    def _():
        @pl.loop(0, half_planes)
        def _(q):
            finalize(q, True)

    @pl.when(high)
    def _():
        for slot in far_slots():
            forward_square(slot)

        @pl.loop(half_planes, heads)
        def _(q):
            partial(q, True)

        for slot in far_slots():
            finish_plane(slot)

        attend([(half_planes + i, j, False) for j in range(half_planes) for i in range(half_planes)])

        @pl.loop(half_planes, heads)
        def _(q):
            finalize(q, False)

    weight_copies[len(sources) + 1].wait()
    half_rows = rows // 2

    def from_worker(j, here):
        @pl.when((t != y) | (plane != here))
        def _():
            arrived(o_all.at[j], o_r.at[j])
            arrived(lt_all.at[j], lt_r.at[j])

    def whole(h):
        totals_ref[h] = lt_all[h]
        part = slice(h * lanes, (h + 1) * lanes)
        head_out[:, part] = (o_all[h].astype(jnp.float32) * opened[:, part]).astype(jnp.bfloat16)

    def merged(h):
        arrived(p_all.at[h], p_r.at[h])
        arrived(pl_all.at[h], pl_r.at[h])
        second = half_planes + h

        @pl.when((t != y) | (h != mirror))
        def _():
            arrived(p_all.at[second], p_r.at[second])
            arrived(pl_all.at[second], pl_r.at[second])

        top = jnp.maximum(pl_all[h], pl_all[second])
        shares = [jnp.exp(pl_all[h] - top), jnp.exp(pl_all[second] - top)]
        total = shares[0] + shares[1]
        totals_ref[h] = top + jnp.log(total)
        turned = jnp.concatenate(
            [shares[0] / total, shares[1] / total, jnp.zeros((4, rows), jnp.float32)], axis=0
        ).T
        maps = []
        for m in range(2):
            held = slice(m * rows, (m + 1) * rows)
            maps.append(
                turned[:, m : m + 1] * p_all[h, held, :].astype(jnp.float32)
                + turned[:, 2 + m : 3 + m] * p_all[second, held, :].astype(jnp.float32)
            )
        diff = maps[0] - lam_own[:, h : h + 1] * maps[1]
        mean = jnp.mean(diff * diff, axis=-1, keepdims=True)
        part = slice(h * lanes, (h + 1) * lanes)
        head_out[:, part] = (diff * lax.rsqrt(mean + 1e-05) * opened[:, part]).astype(
            jnp.bfloat16
        )

    split = half_planes * lanes

    @pl.when(low)
    def _():
        for h in range(half_planes):
            from_worker(h, h)
            whole(h)

    @pl.when(high)
    def _():
        for h in range(half_planes):
            merged(h)

    conv_part[...] += jnp.dot(
        head_out[:, :split], wo_vmem[:split, :], preferred_element_type=jnp.float32
    )
    for h in range(half_planes, heads):

        @pl.when(low)
        def _(h=h):
            from_worker(h, heads - 1 - h)

        @pl.when(high)
        def _(h=h):
            from_worker(h, h)

        whole(h)

    pieces, _, breadth = part_send.shape

    def partial_rows(which, piece):
        there = pl.ds(pl.multiple_of(which * half_rows, half_rows), half_rows)
        columns = slice(piece * breadth, (piece + 1) * breadth)
        attn = jnp.dot(
            head_out[there, split:], wo_vmem[split:, columns], preferred_element_type=jnp.float32
        )
        return (attn + conv_part[there, columns]).astype(jnp.bfloat16)

    exchanges = [
        remote(part_send.at[i], part_recv.at[i], part_sem.at[i], part_sem.at[pieces + i], c_dev)
        for i in range(pieces)
    ]
    for i in range(pieces):
        part_send[i] = partial_rows(1 - t, i)
        exchanges[i].start()
    for i in range(pieces):
        own_rows = partial_rows(t, i).astype(jnp.float32)
        exchanges[i].wait()
        mixed_ref[:, i * breadth : (i + 1) * breadth] = (
            own_rows + part_recv[i].astype(jnp.float32)
        ).astype(jnp.bfloat16)

    def drain(slot):
        along_x(slot).wait_send()
        across(slot).wait_send()
        onward(slot).wait_send()

    def drain_o(q, copies):
        @pl.when((q != plane) | (t != y))
        def _():
            for copy in copies:
                copy.wait_send()

    for k in range(half_planes):

        def sent(k=k):
            kv_copy(order(k)).wait_send()
            q_copy(order(k)).wait_send()
            kv_mirror(k).wait_send()
            q_mirror(k).wait_send()

        if k == 0:
            away_only(sent)
        else:
            sent()
        drain(order(k))
        drain(near(k))

    @pl.when(low)
    def _():
        for slot in far_slots():
            kv_copy(slot).wait_send()
        for q in range(half_planes):
            drain_o(q, o_copies(q, False))
            drain_o(q, o_copies(q, True))
            for copy in p_copies(half_planes + q, False):
                copy.wait_send()

    @pl.when(high)
    def _():
        for slot in far_slots():
            q_copy(slot).wait_send()
            drain(slot)
        for q in range(half_planes, heads):
            drain_o(q, o_copies(q, False))
            drain_o(q, p_copies(q, True))

    @pl.when(s < last)
    def _():
        tail_copy.wait_send()


def fused(sp_count, *args):
    tokens, norm_gain, wq = args[0], args[1], args[2]
    lambdas, head_gain = args[10], args[11]
    rows, half = tokens.shape
    heads = lambdas.shape[0]
    local = wq.shape[1]
    lanes = local // heads
    slots = heads + heads // 2
    out_width = args[12].shape[1]
    bf16, f32 = jnp.bfloat16, jnp.float32
    vmem = pl.BlockSpec(memory_space=pltpu.VMEM)
    hbm = pl.BlockSpec(memory_space=pl.ANY)
    dma = pltpu.SemaphoreType.DMA
    operands = list(args)
    operands[1] = norm_gain.reshape(1, -1)
    operands[10] = lambdas.reshape(1, -1)
    operands[11] = head_gain.reshape(1, -1)
    return pl.pallas_call(
        functools.partial(fused_kernel, sp_count, heads),
        out_shape=(
            pltpu.VMEM((rows // 2, out_width), bf16),
            pltpu.VMEM((heads, 2, rows), f32),
        ),
        in_specs=[hbm] * len(operands),
        out_specs=(vmem, vmem),
        scratch_shapes=[
            pltpu.VMEM((rows, half), bf16),
            pltpu.VMEM((rows, half), bf16),
            pltpu.VMEM((1, 2 * half), f32),
            pltpu.VMEM(args[9].shape, f32),
            pltpu.VMEM((1, local), f32),
            pltpu.VMEM((1, heads), f32),
            pltpu.VMEM((1, heads), f32),
            pltpu.VMEM((rows, 2 * half), bf16),
            pltpu.VMEM((7,) + wq.shape, bf16),
            pltpu.VMEM(args[12].shape, bf16),
            pltpu.VMEM(args[13].shape, bf16),
            pltpu.VMEM((heads, rows, 2 * lanes), bf16),
            pltpu.VMEM((heads, rows, lanes), bf16),
            pltpu.VMEM((slots * RELAY, rows, 2 * lanes), bf16),
            pltpu.VMEM((slots, rows, lanes), bf16),
            pltpu.VMEM((2 * slots, rows, lanes), f32),
            pltpu.VMEM((2 * slots, rows, 2 * lanes), f32),
            pltpu.VMEM((rows, local), f32),
            pltpu.VMEM((rows, local), bf16),
            pltpu.VMEM((rows, local), bf16),
            pltpu.VMEM((16, local), bf16),
            pltpu.VMEM((rows + 8, local), f32),
            pltpu.VMEM((rows, local), bf16),
            pltpu.VMEM((rows, local), bf16),
            pltpu.VMEM((rows, out_width), f32),
            pltpu.VMEM((slots, rows, lanes), bf16),
            pltpu.VMEM((heads, rows, lanes), bf16),
            pltpu.VMEM((slots, 2, rows), f32),
            pltpu.VMEM((heads, 2, rows), f32),
            pltpu.VMEM((heads // 2, 2 * rows, lanes), bf16),
            pltpu.VMEM((heads, 2 * rows, lanes), bf16),
            pltpu.VMEM((heads // 2, 2, rows), f32),
            pltpu.VMEM((heads, 2, rows), f32),
            pltpu.VMEM((PIECES, rows // 2, out_width // PIECES), bf16),
            pltpu.VMEM((PIECES, rows // 2, out_width // PIECES), bf16),
            dma((9,)),
            dma((5,)),
            dma((4,)),
            dma((2,)),
            dma((2 * PIECES,)),
        ]
        + [dma((slots,)) for _ in range(18)]
        + [pltpu.SemaphoreType.REGULAR, pltpu.SemaphoreType.REGULAR],
        compiler_params=pltpu.CompilerParams(
            collective_id=0, has_side_effects=True, vmem_limit_bytes=(60 * 1024 - 4000) * 1024
        ),
    )(*operands)


def fits_square(mesh, heads, rows, key_columns, value_columns):
    return (
        mesh.shape["tp"] == 2
        and mesh.shape["sp"] == heads * RELAY
        and heads > 1
        and heads % 2 == 0
        and rows % 32 == 0
        and key_columns == value_columns == heads * 128
    )


def solution(mesh):
    placed = (
        P("sp", "tp"),
        P(),
        P(None, "tp"),
        P(None, "tp"),
        P(None, "tp"),
        P(None, "tp"),
        P(None, "tp"),
        P(None, "tp"),
        P(None, "tp"),
        P(None, "tp"),
        P("tp"),
        P("tp"),
        P("tp", None),
        P("tp", None),
    )

    def step(*args):
        heads = args[10].shape[0]
        if fits_square(mesh, heads, args[0].shape[0], args[2].shape[1], args[4].shape[1]):
            return fused(mesh.shape["sp"], *args)
        return per_device(*args)

    return jax.shard_map(
        step,
        mesh=mesh,
        in_specs=placed,
        out_specs=(P(("sp", "tp"), None), P("tp", None, "sp")),
        check_vma=False,
    )
```

```python
import functools
import math

import jax
import jax.numpy as jnp
from jax import lax
from jax.experimental import pallas as pl
from jax.experimental.pallas import tpu as pltpu
from jax.sharding import PartitionSpec as P

MESH = pl.DeviceIdType.MESH


def passed_along(shard, axis, by):
    count = lax.axis_size(axis)
    pairs = [(i, i + by) for i in range(count) if 0 <= i + by < count]
    return lax.ppermute(shard, axis, pairs)


def per_device(
    tokens,
    norm_gain,
    query_weight,
    key_weight,
    value_weight,
    gate_weight,
    outer_weight,
    inner_weight,
    signal_weight,
    conv_taps,
    lambdas,
    head_gain,
    attn_out_weight,
    conv_out_weight,
):
    row_count = tokens.shape[0]
    width = norm_gain.shape[0]
    weights = [
        query_weight,
        key_weight,
        value_weight,
        gate_weight,
        outer_weight,
        inner_weight,
        signal_weight,
    ]
    splits = []
    running = 0
    for weight in weights[:-1]:
        running = running + weight.shape[1]
        splits.append(running)
    joined = jnp.concatenate(weights, axis=1)
    empty = jnp.zeros((row_count, joined.shape[1]), jnp.float32)
    piece = lax.all_gather(tokens, "tp", axis=1, tiled=True)
    summed = empty
    piece_f = piece.astype(jnp.float32)
    normed_piece = (piece.astype(jnp.float32) * norm_gain).astype(jnp.bfloat16)
    raw = jnp.dot(normed_piece, joined, preferred_element_type=jnp.float32)
    squares = jnp.sum(piece_f * piece_f, axis=-1)
    scale = lax.rsqrt(squares / width + 1e-06)
    projected = (raw * scale[:, None]).astype(jnp.bfloat16)
    query, key, value, attn_gate, outer, inner, signal = jnp.split(projected, splits, axis=1)
    head_count = lambdas.shape[0]
    key_size = query_weight.shape[1] // (head_count * 2)
    value_size = value_weight.shape[1] // head_count
    score_scale = key_size ** (-0.5)
    own_index = lax.axis_index("sp")
    local_pos = jnp.arange(row_count, dtype=jnp.int32)
    query_parts = [query]
    position_parts = [own_index * row_count + local_pos]
    query_parts = [
        segment.reshape(segment.shape[0], head_count, 2, key_size) for segment in query_parts
    ]

    def absorb(current, query_rows, row_pos, key_block, value_block, key_pos):
        running_max, summed, accum = current
        score = (
            jnp.einsum("qhmd,khmd->hmqk", query_rows, key_block, preferred_element_type=jnp.float32)
            * score_scale
        )
        visible = row_pos[:, None] >= key_pos[None, :]
        masked = jnp.where(visible, score, -1e30)
        new_max = jnp.maximum(running_max, jnp.max(masked, axis=-1, keepdims=True))
        weights_now = jnp.where(visible, jnp.exp(masked - new_max), 0.0)
        factor = jnp.exp(running_max - new_max)
        summed = summed * factor + jnp.sum(weights_now, axis=-1, keepdims=True)
        accum = accum * factor + jnp.einsum(
            "hmqk,khd->hmqd",
            weights_now.astype(jnp.bfloat16),
            value_block,
            preferred_element_type=jnp.float32,
        )
        return (new_max, summed, accum)

    def fresh(rows):
        return (
            jnp.full((head_count, 2, rows, 1), -1e30, jnp.float32),
            jnp.zeros((head_count, 2, rows, 1), jnp.float32),
            jnp.zeros((head_count, 2, rows, value_size), jnp.float32),
        )

    start_states = tuple((fresh(segment.shape[0]) for segment in query_parts))
    carry = start_states
    key_piece = lax.all_gather(key, "sp", axis=0, tiled=True)
    value_piece = lax.all_gather(value, "sp", axis=0, tiled=True)
    length = key_piece.shape[0]
    block_len = 512
    key_blocks = key_piece.reshape(length // block_len, block_len, head_count, 2, key_size)
    value_blocks = value_piece.reshape(length // block_len, block_len, head_count, value_size)

    def one_block(states, item):
        key_block, value_block, block_id = item
        first_key = block_id * block_len
        key_pos = first_key + jnp.arange(block_len, dtype=jnp.int32)
        updated = []
        for current, query_rows, row_pos in zip(states, query_parts, position_parts):

            def compute(held, query_rows=query_rows, row_pos=row_pos):
                return absorb(held, query_rows, row_pos, key_block, value_block, key_pos)

            def unchanged(held):
                return held

            updated.append(
                lax.cond(first_key <= row_pos[row_pos.shape[0] - 1], compute, unchanged, current)
            )
        return (tuple(updated), None)

    carry, _ = lax.scan(
        one_block,
        carry,
        (key_blocks, value_blocks, jnp.arange(length // block_len, dtype=jnp.int32)),
    )
    states = carry
    running_max = jnp.concatenate([held[0] for held in states], axis=2)
    summed = jnp.concatenate([held[1] for held in states], axis=2)
    accum = jnp.concatenate([held[2] for held in states], axis=2)
    mapped = accum / summed
    diff = mapped[:, 0] - lambdas[:, None, None] * mapped[:, 1]
    log_totals = jnp.log(summed[..., 0]) + running_max[..., 0]
    diff = jnp.transpose(diff, (1, 0, 2))
    normed = (
        diff
        * lax.rsqrt(jnp.mean(diff * diff, axis=-1, keepdims=True) + 1e-05)
        * head_gain.reshape(head_count, value_size)
    )
    normed = normed.reshape(row_count, head_count * value_size)
    head_out = (normed * jax.nn.silu(attn_gate.astype(jnp.float32))).astype(jnp.bfloat16)
    taps = conv_taps.shape[0]
    inner_sig = (inner.astype(jnp.float32) * signal.astype(jnp.float32)).astype(jnp.bfloat16)
    before = passed_along(inner_sig[row_count - (taps - 1) :], "sp", 1)
    extended = jnp.concatenate([before, inner_sig], axis=0).astype(jnp.float32)
    convolved = jnp.zeros((row_count, inner_sig.shape[1]), jnp.float32)
    for position in range(taps):
        convolved = convolved + conv_taps[position] * extended[position : position + row_count]
    conv_out = (outer.astype(jnp.float32) * convolved).astype(jnp.bfloat16)
    mixed = lax.psum_scatter(
        (
            jnp.dot(head_out, attn_out_weight, preferred_element_type=jnp.float32)
            + jnp.dot(conv_out, conv_out_weight, preferred_element_type=jnp.float32)
        ).astype(jnp.bfloat16),
        "tp",
        scatter_dimension=0,
        tiled=True,
    )
    return (mixed, log_totals)


RELAY = 4
PIECES = 4


def fused_kernel(
    sp_count,
    heads,
    tokens_hbm,
    gain_hbm,
    wq_hbm,
    wk_hbm,
    wv_hbm,
    wg_hbm,
    wouter_hbm,
    winner_hbm,
    wsignal_hbm,
    taps_hbm,
    lambdas_hbm,
    head_gain_hbm,
    wo_hbm,
    wc_hbm,
    mixed_ref,
    totals_ref,
    own_tokens,
    other_tokens,
    gain_ref,
    taps_ref,
    head_gain_ref,
    lam_own,
    lam_other,
    normed,
    w_vmem,
    wo_vmem,
    wc_vmem,
    kv_send,
    q_send,
    kv_all,
    q_all,
    row_max,
    accum,
    opened,
    outer,
    inner_sig,
    tail_in,
    extended,
    conv_out,
    head_out,
    conv_part,
    o_send,
    o_all,
    lt_send,
    lt_all,
    p_send,
    p_all,
    pl_send,
    pl_all,
    part_send,
    part_recv,
    w_sem,
    in_sem,
    tok_sem,
    tail_sem,
    part_sem,
    stage_s,
    stage_r,
    q_s,
    q_r,
    x_s,
    x_r,
    c_s,
    c_r,
    d_s,
    d_r,
    o_s,
    o_r,
    lt_s,
    lt_r,
    p_s,
    p_r,
    pl_s,
    pl_r,
    pair_sem,
    met_sem,
):
    rows, half = own_tokens.shape
    width = 2 * half
    local = wq_hbm.shape[1]
    lanes = local // heads
    s = lax.axis_index("sp")
    t = lax.axis_index("tp")
    plane = s // RELAY
    place = lax.rem(s, RELAY)
    y = place // 2
    x = lax.rem(place, 2)
    member = 2 * t + x
    home = t == y
    low = plane < heads // 2
    high = plane >= heads // 2
    mirror = heads - 1 - plane
    last = sp_count - 1

    def at(sp_index, tp_index=None):
        return {"sp": sp_index, "tp": t if tp_index is None else tp_index}

    def remote(src, dst, send_sem, recv_sem, device):
        return pltpu.make_async_remote_copy(
            src_ref=src,
            dst_ref=dst,
            send_sem=send_sem,
            recv_sem=recv_sem,
            device_id=device,
            device_id_type=MESH,
        )

    def worker(j):
        return at(j * RELAY + member, y)

    x_sp = s + 1 - 2 * x
    x_dev = at(x_sp)
    c_dev = at(s, 1 - t)

    small = [
        pltpu.make_async_copy(ref, dst, in_sem.at[i])
        for i, (ref, dst) in enumerate(
            [
                (tokens_hbm, own_tokens),
                (gain_hbm, gain_ref),
                (lambdas_hbm, lam_own),
                (taps_hbm, taps_ref),
                (head_gain_hbm, head_gain_ref),
            ]
        )
    ]
    for copy in small:
        copy.start()
    sources = [wk_hbm, wv_hbm, wq_hbm, winner_hbm, wsignal_hbm, wouter_hbm, wg_hbm]
    weight_copies = [
        pltpu.make_async_copy(ref, w_vmem.at[i], w_sem.at[i]) for i, ref in enumerate(sources)
    ]
    weight_copies.append(pltpu.make_async_copy(wc_hbm, wc_vmem, w_sem.at[len(sources)]))
    weight_copies.append(pltpu.make_async_copy(wo_hbm, wo_vmem, w_sem.at[len(sources) + 1]))
    weight_copies[0].start()

    barrier = pltpu.get_barrier_semaphore()

    def signal(sem, device):
        pl.semaphore_signal(sem, inc=1, device_id=device, device_id_type=MESH)

    def greet(sp_index):
        signal(barrier, at(sp_index, 1))

    @pl.when(t == 1)
    def _():
        signal(barrier, at(s, 0))

    for step in range(1, heads):
        greet(lax.rem(plane + step, heads) * RELAY + member)

    @pl.when(t != y)
    def _():
        greet(plane * RELAY + member)

    greet(x_sp)

    @pl.when(s < last)
    def _():
        greet(s + 1)

    @pl.when(s > 0)
    def _():
        greet(s - 1)

    @pl.when(t == 0)
    def _():
        pl.semaphore_wait(barrier, 1)
        signal(pair_sem, at(s, 1))

    @pl.when(t == 1)
    def _():
        pl.semaphore_wait(pair_sem, 1)

    greetings = (
        2 * heads + 1 + 2 * jnp.where(s > 0, 1, 0) + 2 * jnp.where(s < last, 1, 0)
    )

    def meet():
        @pl.when(t == 1)
        def _():
            pl.semaphore_wait(barrier, greetings)
            signal(met_sem, at(s, 0))

        @pl.when(t == 0)
        def _():
            pl.semaphore_wait(met_sem, 1)

    small[0].wait()
    tokens_out = remote(own_tokens, other_tokens, tok_sem.at[0], tok_sem.at[1], c_dev)
    tokens_out.start()
    for copy in weight_copies[1:3]:
        copy.start()
    small[2].wait()
    lam_out = remote(lam_own, lam_other, tok_sem.at[2], tok_sem.at[3], c_dev)
    lam_out.start()

    row_max[...] = jnp.full(row_max.shape, -1e30, jnp.float32)
    accum[...] = jnp.zeros(accum.shape, jnp.float32)

    small[1].wait()
    mine = pl.ds(pl.multiple_of(t * half, half), half)
    theirs = pl.ds(pl.multiple_of((1 - t) * half, half), half)
    own_f = own_tokens[...].astype(jnp.float32)
    squares = jnp.sum(own_f * own_f, axis=-1, keepdims=True)
    own_normed = (own_f * gain_ref[:, mine]).astype(jnp.bfloat16)
    normed[:, mine] = own_normed
    early = []
    for index in range(3):
        weight_copies[index].wait()
        early.append(
            jnp.dot(own_normed, w_vmem[index, mine, :], preferred_element_type=jnp.float32)
        )
    for copy in weight_copies[3:]:
        copy.start()
    tokens_out.wait()
    other_f = other_tokens[...].astype(jnp.float32)
    squares = squares + jnp.sum(other_f * other_f, axis=-1, keepdims=True)
    other_normed = (other_f * gain_ref[:, theirs]).astype(jnp.bfloat16)
    normed[:, theirs] = other_normed
    scale = lax.rsqrt(squares / width + 1e-06)

    def project(index, scale=scale):
        if index < len(early):
            raw = early[index] + jnp.dot(
                other_normed, w_vmem[index, theirs, :], preferred_element_type=jnp.float32
            )
        else:
            weight_copies[index].wait()
            raw = jnp.dot(normed[...], w_vmem[index], preferred_element_type=jnp.float32)
        return (raw * scale).astype(jnp.bfloat16)

    half_planes = heads // 2
    own_base = jnp.where(low, 0, half_planes)
    far_base = half_planes - own_base

    def order(k):
        if k < half_planes:
            return own_base + lax.rem(plane - own_base + k, half_planes)
        return far_base + lax.rem(mirror - far_base + k - half_planes, half_planes)

    def q_copy(j):
        return remote(q_send.at[j], q_all.at[plane], q_s.at[j], q_r.at[plane], worker(j))

    def kv_copy(j):
        return remote(kv_send.at[j], kv_all.at[s], stage_s.at[j], stage_r.at[plane], worker(j))

    spare = heads + plane - own_base
    spare_block = spare * RELAY + place

    def near(k):
        return heads + order(k) - own_base

    def kv_mirror(i):
        peer = order(i)
        return remote(
            kv_send.at[heads - 1 - peer],
            kv_all.at[spare_block],
            stage_s.at[near(i)],
            stage_r.at[spare],
            worker(peer),
        )

    def q_mirror(i):
        peer = order(i)
        return remote(
            q_send.at[heads - 1 - peer],
            q_all.at[spare],
            q_s.at[near(i)],
            q_r.at[spare],
            worker(peer),
        )

    def away_only(action):
        @pl.when(t != y)
        def _():
            action()

    for index in range(2):
        projected = project(index)
        for h in range(heads):
            kv_send[h, :, index * lanes : (index + 1) * lanes] = projected[
                :, h * lanes : (h + 1) * lanes
            ]

    @pl.when(home)
    def _():
        kv_all[s] = kv_send[plane]

    @pl.when(home)
    def _():
        kv_all[spare_block] = kv_send[mirror]

    meet()

    def block(slot, which):
        return kv_all.at[slot * RELAY + which]

    def arrived(dst, recv_sem):
        remote(dst, dst, stage_s.at[0], recv_sem, x_dev).wait_recv()

    def along_x(slot):
        here = block(slot, member)
        return remote(here, here, x_s.at[slot], x_r.at[slot], x_dev)

    def across(slot):
        here = block(slot, member)
        return remote(here, here, c_s.at[slot], c_r.at[slot], c_dev)

    def onward(slot):
        from_x = block(slot, member + 1 - 2 * x)
        return remote(from_x, from_x, d_s.at[slot], d_r.at[slot], c_dev)

    def forward_stage(slot):
        along_x(slot).start()
        across(slot).start()

    def receive(slot):
        arrived(block(slot, member), stage_r.at[slot])
        forward_stage(slot)

    def forward_square(slot):
        arrived(block(slot, member + 1 - 2 * x), x_r.at[slot])
        onward(slot).start()

    def finish_plane(slot):
        arrived(block(slot, lax.rem(member + 2, RELAY)), c_r.at[slot])
        arrived(block(slot, RELAY - 1 - member), d_r.at[slot])

    def first_sends():
        for k in range(1, half_planes):
            kv_copy(order(k)).start()

        @pl.when(low)
        def _():
            kv_copy(mirror).start()

    @pl.when(home)
    def _():
        forward_stage(plane)
        first_sends()

    away_only(lambda: kv_copy(plane).start())

    exponent = (lanes // 2) ** (-0.5) * math.log2(math.e)
    projected = project(2, scale * exponent)
    for h in range(heads):
        q_send[h] = projected[:, h * lanes : (h + 1) * lanes]

    @pl.when(home)
    def _():
        q_all[plane] = q_send[plane]

    @pl.when(home)
    def _():
        q_all[spare] = q_send[mirror]

    def other_queries():
        for k in range(1, half_planes):
            q_copy(order(k)).start()

        @pl.when(high)
        def _():
            for k in range(half_planes, heads):
                q_copy(order(k)).start()

    @pl.when(home)
    def _():
        other_queries()

    inner = project(3).astype(jnp.float32)
    away_only(first_sends)
    signal_f = project(4).astype(jnp.float32)

    @pl.when(t != y)
    def _():
        q_copy(plane).start()
        other_queries()

    inner_sig[...] = (inner * signal_f).astype(jnp.bfloat16)
    tail = tail_in.shape[0]
    tail_copy = remote(
        inner_sig.at[pl.ds(rows - tail, tail)],
        tail_in,
        tail_sem.at[0],
        tail_sem.at[1],
        at(lax.rem(s + 1, sp_count)),
    )

    @pl.when(s < last)
    def _():
        tail_copy.start()

    small[4].wait()
    outer[...] = project(5)
    gate = project(6).astype(jnp.float32)
    opened[...] = gate / (1.0 + jnp.exp(-gate)) * head_gain_ref[...]
    @pl.when(low)
    def _():
        for k in range(half_planes + 1, heads):
            kv_copy(order(k)).start()

    @pl.when(t != y)
    def _():
        kv_mirror(0).start()
        q_mirror(0).start()

    for i in range(1, half_planes):
        kv_mirror(i).start()
        q_mirror(i).start()

    away_only(lambda: receive(plane))
    for k in range(1, half_planes):
        receive(order(k))
    def far_slots():
        return [order(k) for k in range(half_planes, heads)]

    forward_square(plane)

    @pl.when(home)
    def _():
        forward_stage(spare)

    away_only(lambda: receive(spare))

    @pl.when(high)
    def _():
        receive(mirror)

    for k in range(1, half_planes):
        forward_square(order(k))

    span = RELAY * rows
    lane = lax.broadcasted_iota(jnp.int32, (1, lanes), 1)
    masks = [
        of_map.astype(jnp.float32).astype(jnp.bfloat16)
        for of_map in (lane < lanes // 2, lane >= lanes // 2)
    ]

    def attend(tiles):
        def scores(qi, c, diagonal, m):
            keys = kv_all[pl.ds(c * RELAY, RELAY)].reshape(span, 2 * lanes)[:, :lanes]
            score = lax.dot_general(
                q_all[qi] * masks[m],
                keys,
                (((1,), (1,)), ((), ())),
                preferred_element_type=jnp.float32,
            )
            if diagonal:
                row = lax.broadcasted_iota(jnp.int32, (rows, span), 0) + member * rows
                col = lax.broadcasted_iota(jnp.int32, (rows, span), 1)
                score = jnp.where(row >= col, score, -1e30)
            return score

        def absorb(at_row, c, score):
            held = kv_all[pl.ds(c * RELAY, RELAY)].reshape(span, 2 * lanes)
            values = jnp.concatenate(
                [held[:, lanes:], jnp.ones((span, lanes), jnp.bfloat16)], axis=1
            )
            before = row_max[at_row]
            top = jnp.maximum(before, jnp.max(score, axis=-1, keepdims=True))
            weights = jnp.exp2(score - top[:, :1]).astype(jnp.bfloat16)
            factor = jnp.exp2(before - top)
            row_max[at_row] = top
            update = jnp.dot(weights, values, preferred_element_type=jnp.float32)
            for part in (slice(0, lanes), slice(lanes, 2 * lanes)):
                accum[at_row, :, part] = accum[at_row, :, part] * factor + update[:, part]

        items = [(*tile, m) for tile in tiles for m in range(2)]
        upcoming = scores(*items[0])
        for i, (qi, c, _, m) in enumerate(items):
            score = upcoming
            if i + 1 < len(items):
                upcoming = scores(*items[i + 1])
            absorb(2 * qi + m, c, score)

    def attend_triangle(base):
        below = [
            (base + i, base + j, False)
            for j in range(half_planes)
            for i in range(j + 1, half_planes)
        ]
        attend(below + [(base + i, base + i, True) for i in range(half_planes)])

    def attend_row(q):
        attend([(q, j, False) for j in range(half_planes)])

    lam_index = lax.broadcasted_iota(jnp.int32, (1, heads), 1)
    lam_out.wait()
    lam_row = jnp.where(home, lam_own[...], lam_other[...])

    def lambda_of(head):
        return jnp.sum(jnp.where(lam_index == head, lam_row, 0.0), axis=-1, keepdims=True)

    column = lax.broadcasted_iota(jnp.int32, (rows, lanes), 1)

    def slot_of(q, mirrored):
        return heads + q - own_base if mirrored else q

    def o_copies(q, mirrored):
        slot = slot_of(q, mirrored)
        head = mirror if mirrored else plane
        return [
            remote(o_send.at[slot], o_all.at[head], o_s.at[slot], o_r.at[head], worker(q)),
            remote(lt_send.at[slot], lt_all.at[head], lt_s.at[slot], lt_r.at[head], worker(q)),
        ]

    def p_copies(q, mirrored):
        at_row = q - half_planes
        to = half_planes + mirror if mirrored else plane
        return [
            remote(p_send.at[at_row], p_all.at[to], p_s.at[at_row], p_r.at[to], worker(q)),
            remote(pl_send.at[at_row], pl_all.at[to], pl_s.at[at_row], pl_r.at[to], worker(q)),
        ]

    def settle(q, copies, pairs):
        away = (q != plane) | (t != y)

        @pl.when(away)
        def _():
            for copy in copies:
                copy.start()

        @pl.when(jnp.logical_not(away))
        def _():
            for into, index, value in pairs:
                into[index] = value[...]

    def partial(q, mirrored):
        slot = slot_of(q, mirrored)
        at_row = q - half_planes
        logs = []
        for m in range(2):
            held = accum[2 * slot + m]
            total = held[:, lanes:]
            p_send[at_row, m * rows : (m + 1) * rows, :] = (held[:, :lanes] / total).astype(
                jnp.bfloat16
            )
            logs.append(jnp.log(total) + row_max[2 * slot + m] * math.log(2.0))
        turned = jnp.where(column == 0, logs[0], logs[1]).T
        pl_send[at_row] = turned[:2, :]
        if mirrored:
            to = half_planes + mirror
            settle(
                q,
                p_copies(q, mirrored),
                [(p_all, to, p_send.at[at_row]), (pl_all, to, pl_send.at[at_row])],
            )
        else:
            for copy in p_copies(q, mirrored):
                copy.start()

    def finalize(q, mirrored):
        slot = slot_of(q, mirrored)
        head = mirror if mirrored else plane
        maps = []
        logs = []
        for m in range(2):
            held = accum[2 * slot + m]
            total = held[:, lanes:]
            maps.append(held[:, :lanes] / total)
            logs.append(jnp.log(total) + row_max[2 * slot + m] * math.log(2.0))
        diff = maps[0] - lambda_of(head) * maps[1]
        mean = jnp.mean(diff * diff, axis=-1, keepdims=True)
        o_send[slot] = (diff * lax.rsqrt(mean + 1e-05)).astype(jnp.bfloat16)
        turned = jnp.where(column == 0, logs[0], logs[1]).T
        lt_send[slot] = turned[:2, :]
        settle(
            q,
            o_copies(q, mirrored),
            [(o_all, head, o_send.at[slot]), (lt_all, head, lt_send.at[slot])],
        )

    def q_arrived(slot):
        arrived(q_all.at[slot], q_r.at[slot])

    def convolve():
        small[3].wait()

        @pl.when(s > 0)
        def _():
            arrived(tail_in, tail_sem.at[1])

        @pl.when(s == 0)
        def _():
            tail_in[...] = jnp.zeros(tail_in.shape, jnp.bfloat16)

        lead = extended.shape[0] - rows
        extended[0:lead, :] = tail_in[tail - lead :, :].astype(jnp.float32)
        extended[lead:, :] = inner_sig[...].astype(jnp.float32)
        tap_count = taps_ref.shape[0]
        convolved = jnp.zeros((rows, local), jnp.float32)
        for position in range(tap_count):
            offset = lead - (tap_count - 1) + position
            convolved = convolved + taps_ref[position : position + 1, :] * extended[
                offset : offset + rows, :
            ]
        conv_out[...] = (outer[...].astype(jnp.float32) * convolved).astype(jnp.bfloat16)
        weight_copies[len(sources)].wait()
        conv_part[...] = jnp.dot(
            conv_out[...], wc_vmem[...], preferred_element_type=jnp.float32
        )

    def turn(i):
        return own_base + lax.rem(plane - own_base + 1 + i, half_planes)

    def meet_mirror():
        for k in range(1, half_planes):
            receive(near(k))
        forward_square(spare)

    @pl.when(high)
    def _():
        meet_mirror()
        for k in range(half_planes + 1, heads):
            receive(order(k))

    for k in range(half_planes):
        finish_plane(order(k))

    @pl.when(low)
    def _():
        for slot in far_slots():
            q_arrived(slot)

        @pl.loop(half_planes, heads)
        def _(q):
            attend_row(q)
            partial(q, False)

    @pl.when(low)
    def _():
        meet_mirror()

    away_only(lambda: q_arrived(plane))
    for k in range(1, half_planes):
        q_arrived(order(k))
    attend_triangle(own_base)

    @pl.when(high)
    def _():
        forward_square(mirror)

    @pl.when(low)
    def _():
        @pl.loop(0, half_planes)
        def _(i):
            finalize(turn(i), False)

    convolve()

    @pl.when(high)
    def _():
        finish_plane(mirror)
        attend([(half_planes + i, mirror, False) for i in range(half_planes)])

    for k in range(1, half_planes):
        forward_square(near(k))

    @pl.when(high)
    def _():
        for k in range(half_planes + 1, heads):
            forward_square(order(k))


    for k in range(half_planes):
        finish_plane(near(k))
        if k == 0:
            away_only(lambda: q_arrived(spare))
        else:
            q_arrived(near(k))
    @pl.loop(0, half_planes)
    def _(i):
        q = turn(i)
        for row in range(half_planes):

            @pl.when(q - own_base == row)
            def _(row=row):
                attend([(heads + row, heads + c, c == row) for c in range(row + 1)])

        @pl.when(low)
        def _():
            finalize(q, True)

        @pl.when(high)
        def _():
            partial(q, True)

    @pl.when(high)
    def _():
        for slot in far_slots()[1:]:
            finish_plane(slot)

        attend(
            [
                (half_planes + i, slot, False)
                for slot in far_slots()[1:]
                for i in range(half_planes)
            ]
        )

        @pl.loop(0, half_planes)
        def _(i):
            finalize(turn(i), False)

    weight_copies[len(sources) + 1].wait()
    half_rows = rows // 2

    def from_worker(j, here):
        @pl.when((t != y) | (plane != here))
        def _():
            arrived(o_all.at[j], o_r.at[j])
            arrived(lt_all.at[j], lt_r.at[j])

    def whole(h):
        totals_ref[h] = lt_all[h]
        part = slice(h * lanes, (h + 1) * lanes)
        head_out[:, part] = (o_all[h].astype(jnp.float32) * opened[:, part]).astype(jnp.bfloat16)

    def merged(h):
        arrived(p_all.at[h], p_r.at[h])
        arrived(pl_all.at[h], pl_r.at[h])
        second = half_planes + h

        @pl.when((t != y) | (h != mirror))
        def _():
            arrived(p_all.at[second], p_r.at[second])
            arrived(pl_all.at[second], pl_r.at[second])

        top = jnp.maximum(pl_all[h], pl_all[second])
        shares = [jnp.exp(pl_all[h] - top), jnp.exp(pl_all[second] - top)]
        total = shares[0] + shares[1]
        totals_ref[h] = top + jnp.log(total)
        turned = jnp.concatenate(
            [shares[0] / total, shares[1] / total, jnp.zeros((4, rows), jnp.float32)], axis=0
        ).T
        maps = []
        for m in range(2):
            held = slice(m * rows, (m + 1) * rows)
            maps.append(
                turned[:, m : m + 1] * p_all[h, held, :].astype(jnp.float32)
                + turned[:, 2 + m : 3 + m] * p_all[second, held, :].astype(jnp.float32)
            )
        own_lam = jnp.sum(jnp.where(lam_index == h, lam_own[...], 0.0), axis=-1, keepdims=True)
        diff = maps[0] - own_lam * maps[1]
        mean = jnp.mean(diff * diff, axis=-1, keepdims=True)
        part = pl.ds(pl.multiple_of(h * lanes, lanes), lanes)
        head_out[:, part] = (diff * lax.rsqrt(mean + 1e-05) * opened[:, part]).astype(
            jnp.bfloat16
        )

    split = half_planes * lanes

    @pl.when(low)
    def _():
        for h in range(half_planes):
            from_worker(h, h)
            whole(h)

    @pl.when(high)
    def _():
        @pl.loop(0, half_planes)
        def _(i):
            merged(lax.rem(mirror + jnp.where(home, 0, 1) + i, half_planes))

    conv_part[...] += jnp.dot(
        head_out[:, :split], wo_vmem[:split, :], preferred_element_type=jnp.float32
    )
    for h in range(half_planes, heads):

        @pl.when(low)
        def _(h=h):
            from_worker(h, heads - 1 - h)

        @pl.when(high)
        def _(h=h):
            from_worker(h, h)

        whole(h)

    pieces, _, breadth = part_send.shape

    def partial_rows(which, piece):
        there = pl.ds(pl.multiple_of(which * half_rows, half_rows), half_rows)
        columns = slice(piece * breadth, (piece + 1) * breadth)
        attn = jnp.dot(
            head_out[there, split:], wo_vmem[split:, columns], preferred_element_type=jnp.float32
        )
        return (attn + conv_part[there, columns]).astype(jnp.bfloat16)

    exchanges = [
        remote(part_send.at[i], part_recv.at[i], part_sem.at[i], part_sem.at[pieces + i], c_dev)
        for i in range(pieces)
    ]
    for i in range(pieces):
        part_send[i] = partial_rows(1 - t, i)
        exchanges[i].start()
    for i in range(pieces):
        own_rows = partial_rows(t, i).astype(jnp.float32)
        exchanges[i].wait()
        mixed_ref[:, i * breadth : (i + 1) * breadth] = (
            own_rows + part_recv[i].astype(jnp.float32)
        ).astype(jnp.bfloat16)

    def drain(slot):
        along_x(slot).wait_send()
        across(slot).wait_send()
        onward(slot).wait_send()

    def drain_o(q, copies):
        @pl.when((q != plane) | (t != y))
        def _():
            for copy in copies:
                copy.wait_send()

    for k in range(half_planes):

        def sent(k=k):
            kv_copy(order(k)).wait_send()
            q_copy(order(k)).wait_send()
            kv_mirror(k).wait_send()
            q_mirror(k).wait_send()

        if k == 0:
            away_only(sent)
        else:
            sent()
        drain(order(k))
        drain(near(k))

    @pl.when(low)
    def _():
        for slot in far_slots():
            kv_copy(slot).wait_send()
        for q in range(half_planes):
            drain_o(q, o_copies(q, False))
            drain_o(q, o_copies(q, True))
            for copy in p_copies(half_planes + q, False):
                copy.wait_send()

    @pl.when(high)
    def _():
        for slot in far_slots():
            q_copy(slot).wait_send()
            drain(slot)
        for q in range(half_planes, heads):
            drain_o(q, o_copies(q, False))
            drain_o(q, p_copies(q, True))

    @pl.when(s < last)
    def _():
        tail_copy.wait_send()


def fused(sp_count, *args):
    tokens, norm_gain, wq = args[0], args[1], args[2]
    lambdas, head_gain = args[10], args[11]
    rows, half = tokens.shape
    heads = lambdas.shape[0]
    local = wq.shape[1]
    lanes = local // heads
    slots = heads + heads // 2
    out_width = args[12].shape[1]
    bf16, f32 = jnp.bfloat16, jnp.float32
    vmem = pl.BlockSpec(memory_space=pltpu.VMEM)
    hbm = pl.BlockSpec(memory_space=pl.ANY)
    dma = pltpu.SemaphoreType.DMA
    operands = list(args)
    operands[1] = norm_gain.reshape(1, -1)
    operands[10] = lambdas.reshape(1, -1)
    operands[11] = head_gain.reshape(1, -1)
    return pl.pallas_call(
        functools.partial(fused_kernel, sp_count, heads),
        out_shape=(
            pltpu.VMEM((rows // 2, out_width), bf16),
            pltpu.VMEM((heads, 2, rows), f32),
        ),
        in_specs=[hbm] * len(operands),
        out_specs=(vmem, vmem),
        scratch_shapes=[
            pltpu.VMEM((rows, half), bf16),
            pltpu.VMEM((rows, half), bf16),
            pltpu.VMEM((1, 2 * half), f32),
            pltpu.VMEM(args[9].shape, f32),
            pltpu.VMEM((1, local), f32),
            pltpu.VMEM((1, heads), f32),
            pltpu.VMEM((1, heads), f32),
            pltpu.VMEM((rows, 2 * half), bf16),
            pltpu.VMEM((7,) + wq.shape, bf16),
            pltpu.VMEM(args[12].shape, bf16),
            pltpu.VMEM(args[13].shape, bf16),
            pltpu.VMEM((heads, rows, 2 * lanes), bf16),
            pltpu.VMEM((heads, rows, lanes), bf16),
            pltpu.VMEM((slots * RELAY, rows, 2 * lanes), bf16),
            pltpu.VMEM((slots, rows, lanes), bf16),
            pltpu.VMEM((2 * slots, rows, lanes), f32),
            pltpu.VMEM((2 * slots, rows, 2 * lanes), f32),
            pltpu.VMEM((rows, local), f32),
            pltpu.VMEM((rows, local), bf16),
            pltpu.VMEM((rows, local), bf16),
            pltpu.VMEM((16, local), bf16),
            pltpu.VMEM((rows + 8, local), f32),
            pltpu.VMEM((rows, local), bf16),
            pltpu.VMEM((rows, local), bf16),
            pltpu.VMEM((rows, out_width), f32),
            pltpu.VMEM((slots, rows, lanes), bf16),
            pltpu.VMEM((heads, rows, lanes), bf16),
            pltpu.VMEM((slots, 2, rows), f32),
            pltpu.VMEM((heads, 2, rows), f32),
            pltpu.VMEM((heads // 2, 2 * rows, lanes), bf16),
            pltpu.VMEM((heads, 2 * rows, lanes), bf16),
            pltpu.VMEM((heads // 2, 2, rows), f32),
            pltpu.VMEM((heads, 2, rows), f32),
            pltpu.VMEM((PIECES, rows // 2, out_width // PIECES), bf16),
            pltpu.VMEM((PIECES, rows // 2, out_width // PIECES), bf16),
            dma((9,)),
            dma((5,)),
            dma((4,)),
            dma((2,)),
            dma((2 * PIECES,)),
        ]
        + [dma((slots,)) for _ in range(18)]
        + [pltpu.SemaphoreType.REGULAR, pltpu.SemaphoreType.REGULAR],
        compiler_params=pltpu.CompilerParams(
            collective_id=0, has_side_effects=True, vmem_limit_bytes=58000 * 1024
        ),
    )(*operands)


def fits_square(mesh, heads, rows, key_columns, value_columns):
    return (
        mesh.shape["tp"] == 2
        and mesh.shape["sp"] == heads * RELAY
        and heads > 1
        and heads % 2 == 0
        and rows % 32 == 0
        and key_columns == value_columns == heads * 128
    )


def solution(mesh):
    placed = (
        P("sp", "tp"),
        P(),
        P(None, "tp"),
        P(None, "tp"),
        P(None, "tp"),
        P(None, "tp"),
        P(None, "tp"),
        P(None, "tp"),
        P(None, "tp"),
        P(None, "tp"),
        P("tp"),
        P("tp"),
        P("tp", None),
        P("tp", None),
    )

    def step(*args):
        heads = args[10].shape[0]
        if fits_square(mesh, heads, args[0].shape[0], args[2].shape[1], args[4].shape[1]):
            return fused(mesh.shape["sp"], *args)
        return per_device(*args)

    return jax.shard_map(
        step,
        mesh=mesh,
        in_specs=placed,
        out_specs=(P(("sp", "tp"), None), P("tp", None, "sp")),
        check_vma=False,
    )
```

```python
import functools
import math

import jax
import jax.numpy as jnp
from jax import lax
from jax.experimental import pallas as pl
from jax.experimental.pallas import tpu as pltpu
from jax.sharding import PartitionSpec as P

MESH = pl.DeviceIdType.MESH


def passed_along(shard, axis, by):
    count = lax.axis_size(axis)
    pairs = [(i, i + by) for i in range(count) if 0 <= i + by < count]
    return lax.ppermute(shard, axis, pairs)


def per_device(
    tokens,
    norm_gain,
    query_weight,
    key_weight,
    value_weight,
    gate_weight,
    outer_weight,
    inner_weight,
    signal_weight,
    conv_taps,
    lambdas,
    head_gain,
    attn_out_weight,
    conv_out_weight,
):
    row_count = tokens.shape[0]
    width = norm_gain.shape[0]
    weights = [
        query_weight,
        key_weight,
        value_weight,
        gate_weight,
        outer_weight,
        inner_weight,
        signal_weight,
    ]
    splits = []
    running = 0
    for weight in weights[:-1]:
        running = running + weight.shape[1]
        splits.append(running)
    joined = jnp.concatenate(weights, axis=1)
    empty = jnp.zeros((row_count, joined.shape[1]), jnp.float32)
    piece = lax.all_gather(tokens, "tp", axis=1, tiled=True)
    summed = empty
    piece_f = piece.astype(jnp.float32)
    normed_piece = (piece.astype(jnp.float32) * norm_gain).astype(jnp.bfloat16)
    raw = jnp.dot(normed_piece, joined, preferred_element_type=jnp.float32)
    squares = jnp.sum(piece_f * piece_f, axis=-1)
    scale = lax.rsqrt(squares / width + 1e-06)
    projected = (raw * scale[:, None]).astype(jnp.bfloat16)
    query, key, value, attn_gate, outer, inner, signal = jnp.split(projected, splits, axis=1)
    head_count = lambdas.shape[0]
    key_size = query_weight.shape[1] // (head_count * 2)
    value_size = value_weight.shape[1] // head_count
    score_scale = key_size ** (-0.5)
    own_index = lax.axis_index("sp")
    local_pos = jnp.arange(row_count, dtype=jnp.int32)
    query_parts = [query]
    position_parts = [own_index * row_count + local_pos]
    query_parts = [
        segment.reshape(segment.shape[0], head_count, 2, key_size) for segment in query_parts
    ]

    def absorb(current, query_rows, row_pos, key_block, value_block, key_pos):
        running_max, summed, accum = current
        score = (
            jnp.einsum("qhmd,khmd->hmqk", query_rows, key_block, preferred_element_type=jnp.float32)
            * score_scale
        )
        visible = row_pos[:, None] >= key_pos[None, :]
        masked = jnp.where(visible, score, -1e30)
        new_max = jnp.maximum(running_max, jnp.max(masked, axis=-1, keepdims=True))
        weights_now = jnp.where(visible, jnp.exp(masked - new_max), 0.0)
        factor = jnp.exp(running_max - new_max)
        summed = summed * factor + jnp.sum(weights_now, axis=-1, keepdims=True)
        accum = accum * factor + jnp.einsum(
            "hmqk,khd->hmqd",
            weights_now.astype(jnp.bfloat16),
            value_block,
            preferred_element_type=jnp.float32,
        )
        return (new_max, summed, accum)

    def fresh(rows):
        return (
            jnp.full((head_count, 2, rows, 1), -1e30, jnp.float32),
            jnp.zeros((head_count, 2, rows, 1), jnp.float32),
            jnp.zeros((head_count, 2, rows, value_size), jnp.float32),
        )

    start_states = tuple((fresh(segment.shape[0]) for segment in query_parts))
    carry = start_states
    key_piece = lax.all_gather(key, "sp", axis=0, tiled=True)
    value_piece = lax.all_gather(value, "sp", axis=0, tiled=True)
    length = key_piece.shape[0]
    block_len = 512
    key_blocks = key_piece.reshape(length // block_len, block_len, head_count, 2, key_size)
    value_blocks = value_piece.reshape(length // block_len, block_len, head_count, value_size)

    def one_block(states, item):
        key_block, value_block, block_id = item
        first_key = block_id * block_len
        key_pos = first_key + jnp.arange(block_len, dtype=jnp.int32)
        updated = []
        for current, query_rows, row_pos in zip(states, query_parts, position_parts):

            def compute(held, query_rows=query_rows, row_pos=row_pos):
                return absorb(held, query_rows, row_pos, key_block, value_block, key_pos)

            def unchanged(held):
                return held

            updated.append(
                lax.cond(first_key <= row_pos[row_pos.shape[0] - 1], compute, unchanged, current)
            )
        return (tuple(updated), None)

    carry, _ = lax.scan(
        one_block,
        carry,
        (key_blocks, value_blocks, jnp.arange(length // block_len, dtype=jnp.int32)),
    )
    states = carry
    running_max = jnp.concatenate([held[0] for held in states], axis=2)
    summed = jnp.concatenate([held[1] for held in states], axis=2)
    accum = jnp.concatenate([held[2] for held in states], axis=2)
    mapped = accum / summed
    diff = mapped[:, 0] - lambdas[:, None, None] * mapped[:, 1]
    log_totals = jnp.log(summed[..., 0]) + running_max[..., 0]
    diff = jnp.transpose(diff, (1, 0, 2))
    normed = (
        diff
        * lax.rsqrt(jnp.mean(diff * diff, axis=-1, keepdims=True) + 1e-05)
        * head_gain.reshape(head_count, value_size)
    )
    normed = normed.reshape(row_count, head_count * value_size)
    head_out = (normed * jax.nn.silu(attn_gate.astype(jnp.float32))).astype(jnp.bfloat16)
    taps = conv_taps.shape[0]
    inner_sig = (inner.astype(jnp.float32) * signal.astype(jnp.float32)).astype(jnp.bfloat16)
    before = passed_along(inner_sig[row_count - (taps - 1) :], "sp", 1)
    extended = jnp.concatenate([before, inner_sig], axis=0).astype(jnp.float32)
    convolved = jnp.zeros((row_count, inner_sig.shape[1]), jnp.float32)
    for position in range(taps):
        convolved = convolved + conv_taps[position] * extended[position : position + row_count]
    conv_out = (outer.astype(jnp.float32) * convolved).astype(jnp.bfloat16)
    mixed = lax.psum_scatter(
        (
            jnp.dot(head_out, attn_out_weight, preferred_element_type=jnp.float32)
            + jnp.dot(conv_out, conv_out_weight, preferred_element_type=jnp.float32)
        ).astype(jnp.bfloat16),
        "tp",
        scatter_dimension=0,
        tiled=True,
    )
    return (mixed, log_totals)


RELAY = 4
PIECES = 4


def fused_kernel(
    sp_count,
    heads,
    tokens_hbm,
    gain_hbm,
    wq_hbm,
    wk_hbm,
    wv_hbm,
    wg_hbm,
    wouter_hbm,
    winner_hbm,
    wsignal_hbm,
    taps_hbm,
    lambdas_hbm,
    head_gain_hbm,
    wo_hbm,
    wc_hbm,
    mixed_ref,
    totals_ref,
    own_tokens,
    other_tokens,
    gain_ref,
    taps_ref,
    head_gain_ref,
    lam_own,
    lam_other,
    normed,
    w_vmem,
    wo_vmem,
    wc_vmem,
    kv_send,
    q_send,
    kv_all,
    q_all,
    row_max,
    accum,
    opened,
    outer,
    inner_sig,
    tail_in,
    extended,
    conv_out,
    head_out,
    conv_part,
    o_send,
    o_all,
    lt_send,
    lt_all,
    p_send,
    p_all,
    pl_send,
    pl_all,
    part_send,
    part_recv,
    w_sem,
    in_sem,
    tok_sem,
    tail_sem,
    part_sem,
    stage_s,
    stage_r,
    q_s,
    q_r,
    x_s,
    x_r,
    c_s,
    c_r,
    d_s,
    d_r,
    o_s,
    o_r,
    lt_s,
    lt_r,
    p_s,
    p_r,
    pl_s,
    pl_r,
    pair_sem,
    met_sem,
):
    rows, half = own_tokens.shape
    width = 2 * half
    local = wq_hbm.shape[1]
    lanes = local // heads
    s = lax.axis_index("sp")
    t = lax.axis_index("tp")
    plane = s // RELAY
    place = lax.rem(s, RELAY)
    y = place // 2
    x = lax.rem(place, 2)
    member = 2 * t + x
    home = t == y
    low = plane < heads // 2
    high = plane >= heads // 2
    mirror = heads - 1 - plane
    last = sp_count - 1

    def at(sp_index, tp_index=None):
        return {"sp": sp_index, "tp": t if tp_index is None else tp_index}

    def remote(src, dst, send_sem, recv_sem, device):
        return pltpu.make_async_remote_copy(
            src_ref=src,
            dst_ref=dst,
            send_sem=send_sem,
            recv_sem=recv_sem,
            device_id=device,
            device_id_type=MESH,
        )

    def worker(j):
        return at(j * RELAY + member, y)

    x_sp = s + 1 - 2 * x
    x_dev = at(x_sp)
    c_dev = at(s, 1 - t)

    small = [
        pltpu.make_async_copy(ref, dst, in_sem.at[i])
        for i, (ref, dst) in enumerate(
            [
                (tokens_hbm, own_tokens),
                (gain_hbm, gain_ref),
                (lambdas_hbm, lam_own),
                (taps_hbm, taps_ref),
                (head_gain_hbm, head_gain_ref),
            ]
        )
    ]
    for copy in small:
        copy.start()
    sources = [wk_hbm, wv_hbm, wq_hbm, winner_hbm, wsignal_hbm, wouter_hbm, wg_hbm]
    weight_copies = [
        pltpu.make_async_copy(ref, w_vmem.at[i], w_sem.at[i]) for i, ref in enumerate(sources)
    ]
    weight_copies.append(pltpu.make_async_copy(wc_hbm, wc_vmem, w_sem.at[len(sources)]))
    weight_copies.append(pltpu.make_async_copy(wo_hbm, wo_vmem, w_sem.at[len(sources) + 1]))
    weight_copies[0].start()

    barrier = pltpu.get_barrier_semaphore()

    def signal(sem, device):
        pl.semaphore_signal(sem, inc=1, device_id=device, device_id_type=MESH)

    def greet(sp_index):
        signal(barrier, at(sp_index, 1))

    @pl.when(t == 1)
    def _():
        signal(barrier, at(s, 0))

    for step in range(1, heads):
        greet(lax.rem(plane + step, heads) * RELAY + member)

    @pl.when(t != y)
    def _():
        greet(plane * RELAY + member)

    greet(x_sp)

    @pl.when(s < last)
    def _():
        greet(s + 1)

    @pl.when(s > 0)
    def _():
        greet(s - 1)

    @pl.when(t == 0)
    def _():
        pl.semaphore_wait(barrier, 1)
        signal(pair_sem, at(s, 1))

    @pl.when(t == 1)
    def _():
        pl.semaphore_wait(pair_sem, 1)

    greetings = (
        2 * heads + 1 + 2 * jnp.where(s > 0, 1, 0) + 2 * jnp.where(s < last, 1, 0)
    )

    def meet():
        @pl.when(t == 1)
        def _():
            pl.semaphore_wait(barrier, greetings)
            signal(met_sem, at(s, 0))

        @pl.when(t == 0)
        def _():
            pl.semaphore_wait(met_sem, 1)

    small[0].wait()
    tokens_out = remote(own_tokens, other_tokens, tok_sem.at[0], tok_sem.at[1], c_dev)
    tokens_out.start()
    for copy in weight_copies[1:3]:
        copy.start()
    small[2].wait()
    lam_out = remote(lam_own, lam_other, tok_sem.at[2], tok_sem.at[3], c_dev)
    lam_out.start()

    row_max[...] = jnp.full(row_max.shape, -1e30, jnp.float32)
    accum[...] = jnp.zeros(accum.shape, jnp.float32)

    small[1].wait()
    mine = pl.ds(pl.multiple_of(t * half, half), half)
    theirs = pl.ds(pl.multiple_of((1 - t) * half, half), half)
    own_f = own_tokens[...].astype(jnp.float32)
    squares = jnp.sum(own_f * own_f, axis=-1, keepdims=True)
    own_normed = (own_f * gain_ref[:, mine]).astype(jnp.bfloat16)
    normed[:, mine] = own_normed
    early = []
    for index in range(3):
        weight_copies[index].wait()
        early.append(
            jnp.dot(own_normed, w_vmem[index, mine, :], preferred_element_type=jnp.float32)
        )
    for copy in weight_copies[3:]:
        copy.start()
    tokens_out.wait()
    other_f = other_tokens[...].astype(jnp.float32)
    squares = squares + jnp.sum(other_f * other_f, axis=-1, keepdims=True)
    other_normed = (other_f * gain_ref[:, theirs]).astype(jnp.bfloat16)
    normed[:, theirs] = other_normed
    scale = lax.rsqrt(squares / width + 1e-06)

    def project(index, scale=scale):
        if index < len(early):
            raw = early[index] + jnp.dot(
                other_normed, w_vmem[index, theirs, :], preferred_element_type=jnp.float32
            )
        else:
            weight_copies[index].wait()
            raw = jnp.dot(normed[...], w_vmem[index], preferred_element_type=jnp.float32)
        return (raw * scale).astype(jnp.bfloat16)

    half_planes = heads // 2
    own_base = jnp.where(low, 0, half_planes)
    far_base = half_planes - own_base

    def order(k):
        if k < half_planes:
            return own_base + lax.rem(plane - own_base + k, half_planes)
        return far_base + lax.rem(mirror - far_base + k - half_planes, half_planes)

    def q_copy(j):
        return remote(q_send.at[j], q_all.at[plane], q_s.at[j], q_r.at[plane], worker(j))

    def kv_copy(j):
        return remote(kv_send.at[j], kv_all.at[s], stage_s.at[j], stage_r.at[plane], worker(j))

    spare = heads + plane - own_base
    spare_block = spare * RELAY + place

    def near(k):
        return heads + order(k) - own_base

    def kv_mirror(i):
        peer = order(i)
        return remote(
            kv_send.at[heads - 1 - peer],
            kv_all.at[spare_block],
            stage_s.at[near(i)],
            stage_r.at[spare],
            worker(peer),
        )

    def q_mirror(i):
        peer = order(i)
        return remote(
            q_send.at[heads - 1 - peer],
            q_all.at[spare],
            q_s.at[near(i)],
            q_r.at[spare],
            worker(peer),
        )

    def away_only(action):
        @pl.when(t != y)
        def _():
            action()

    for index in range(2):
        projected = project(index)
        for h in range(heads):
            kv_send[h, :, index * lanes : (index + 1) * lanes] = projected[
                :, h * lanes : (h + 1) * lanes
            ]

    @pl.when(home)
    def _():
        kv_all[s] = kv_send[plane]

    @pl.when(home)
    def _():
        kv_all[spare_block] = kv_send[mirror]

    meet()

    def block(slot, which):
        return kv_all.at[slot * RELAY + which]

    def arrived(dst, recv_sem):
        remote(dst, dst, stage_s.at[0], recv_sem, x_dev).wait_recv()

    def along_x(slot):
        here = block(slot, member)
        return remote(here, here, x_s.at[slot], x_r.at[slot], x_dev)

    def across(slot):
        here = block(slot, member)
        return remote(here, here, c_s.at[slot], c_r.at[slot], c_dev)

    def onward(slot):
        from_x = block(slot, member + 1 - 2 * x)
        return remote(from_x, from_x, d_s.at[slot], d_r.at[slot], c_dev)

    def forward_stage(slot):
        along_x(slot).start()
        across(slot).start()

    def receive(slot):
        arrived(block(slot, member), stage_r.at[slot])
        forward_stage(slot)

    def forward_square(slot):
        arrived(block(slot, member + 1 - 2 * x), x_r.at[slot])
        onward(slot).start()

    def finish_plane(slot):
        arrived(block(slot, lax.rem(member + 2, RELAY)), c_r.at[slot])
        arrived(block(slot, RELAY - 1 - member), d_r.at[slot])

    def first_sends():
        for k in range(1, half_planes):
            kv_copy(order(k)).start()

        @pl.when(low)
        def _():
            kv_copy(mirror).start()

    @pl.when(home)
    def _():
        forward_stage(plane)
        first_sends()

    away_only(lambda: kv_copy(plane).start())

    exponent = (lanes // 2) ** (-0.5) * math.log2(math.e)
    projected = project(2, scale * exponent)
    for h in range(heads):
        q_send[h] = projected[:, h * lanes : (h + 1) * lanes]

    @pl.when(home)
    def _():
        q_all[plane] = q_send[plane]

    @pl.when(home)
    def _():
        q_all[spare] = q_send[mirror]

    def other_queries():
        for k in range(1, half_planes):
            q_copy(order(k)).start()

        @pl.when(high)
        def _():
            for k in range(half_planes, heads):
                q_copy(order(k)).start()

    @pl.when(home)
    def _():
        other_queries()

    inner = project(3).astype(jnp.float32)
    away_only(first_sends)
    signal_f = project(4).astype(jnp.float32)

    @pl.when(t != y)
    def _():
        q_copy(plane).start()
        other_queries()

    inner_sig[...] = (inner * signal_f).astype(jnp.bfloat16)
    tail = tail_in.shape[0]
    tail_copy = remote(
        inner_sig.at[pl.ds(rows - tail, tail)],
        tail_in,
        tail_sem.at[0],
        tail_sem.at[1],
        at(lax.rem(s + 1, sp_count)),
    )

    @pl.when(s < last)
    def _():
        tail_copy.start()

    small[4].wait()
    outer[...] = project(5)
    gate = project(6).astype(jnp.float32)
    opened[...] = gate / (1.0 + jnp.exp(-gate)) * head_gain_ref[...]
    @pl.when(low)
    def _():
        for k in range(half_planes + 1, heads):
            kv_copy(order(k)).start()

    @pl.when(t != y)
    def _():
        kv_mirror(0).start()
        q_mirror(0).start()

    for i in range(1, half_planes):
        kv_mirror(i).start()
        q_mirror(i).start()

    away_only(lambda: receive(plane))
    for k in range(1, half_planes):
        receive(order(k))
    def far_slots():
        return [order(k) for k in range(half_planes, heads)]

    forward_square(plane)

    @pl.when(home)
    def _():
        forward_stage(spare)

    away_only(lambda: receive(spare))

    @pl.when(high)
    def _():
        receive(mirror)

    for k in range(1, half_planes):
        forward_square(order(k))

    span = RELAY * rows
    lane = lax.broadcasted_iota(jnp.int32, (1, lanes), 1)
    masks = [
        of_map.astype(jnp.float32).astype(jnp.bfloat16)
        for of_map in (lane < lanes // 2, lane >= lanes // 2)
    ]

    def attend(tiles):
        def scores(qi, c, diagonal, m):
            keys = kv_all[pl.ds(c * RELAY, RELAY)].reshape(span, 2 * lanes)[:, :lanes]
            score = lax.dot_general(
                q_all[qi] * masks[m],
                keys,
                (((1,), (1,)), ((), ())),
                preferred_element_type=jnp.float32,
            )
            if diagonal:
                row = lax.broadcasted_iota(jnp.int32, (rows, span), 0) + member * rows
                col = lax.broadcasted_iota(jnp.int32, (rows, span), 1)
                score = jnp.where(row >= col, score, -1e30)
            return score

        def absorb(at_row, c, score):
            held = kv_all[pl.ds(c * RELAY, RELAY)].reshape(span, 2 * lanes)
            values = jnp.concatenate(
                [held[:, lanes:], jnp.ones((span, lanes), jnp.bfloat16)], axis=1
            )
            before = row_max[at_row]
            top = jnp.maximum(before, jnp.max(score, axis=-1, keepdims=True))
            weights = jnp.exp2(score - top[:, :1]).astype(jnp.bfloat16)
            factor = jnp.exp2(before - top)
            row_max[at_row] = top
            update = jnp.dot(weights, values, preferred_element_type=jnp.float32)
            for part in (slice(0, lanes), slice(lanes, 2 * lanes)):
                accum[at_row, :, part] = accum[at_row, :, part] * factor + update[:, part]

        items = [(*tile, m) for tile in tiles for m in range(2)]
        upcoming = scores(*items[0])
        for i, (qi, c, _, m) in enumerate(items):
            score = upcoming
            if i + 1 < len(items):
                upcoming = scores(*items[i + 1])
            absorb(2 * qi + m, c, score)

    def attend_triangle(base):
        below = [
            (base + i, base + j, False)
            for j in range(half_planes)
            for i in range(j + 1, half_planes)
        ]
        attend(below + [(base + i, base + i, True) for i in range(half_planes)])

    def attend_row(q):
        attend([(q, j, False) for j in range(half_planes)])

    lam_index = lax.broadcasted_iota(jnp.int32, (1, heads), 1)
    lam_out.wait()
    lam_row = jnp.where(home, lam_own[...], lam_other[...])

    def lambda_of(head):
        return jnp.sum(jnp.where(lam_index == head, lam_row, 0.0), axis=-1, keepdims=True)

    column = lax.broadcasted_iota(jnp.int32, (rows, lanes), 1)

    def slot_of(q, mirrored):
        return heads + q - own_base if mirrored else q

    def o_copies(q, mirrored):
        slot = slot_of(q, mirrored)
        head = mirror if mirrored else plane
        return [
            remote(o_send.at[slot], o_all.at[head], o_s.at[slot], o_r.at[head], worker(q)),
            remote(lt_send.at[slot], lt_all.at[head], lt_s.at[slot], lt_r.at[head], worker(q)),
        ]

    def p_copies(q, mirrored):
        at_row = q - half_planes
        to = half_planes + mirror if mirrored else plane
        return [
            remote(p_send.at[at_row], p_all.at[to], p_s.at[at_row], p_r.at[to], worker(q)),
            remote(pl_send.at[at_row], pl_all.at[to], pl_s.at[at_row], pl_r.at[to], worker(q)),
        ]

    def settle(q, copies, pairs):
        away = (q != plane) | (t != y)

        @pl.when(away)
        def _():
            for copy in copies:
                copy.start()

        @pl.when(jnp.logical_not(away))
        def _():
            for into, index, value in pairs:
                into[index] = value[...]

    def partial(q, mirrored):
        slot = slot_of(q, mirrored)
        at_row = q - half_planes
        logs = []
        for m in range(2):
            held = accum[2 * slot + m]
            total = held[:, lanes:]
            p_send[at_row, m * rows : (m + 1) * rows, :] = (held[:, :lanes] / total).astype(
                jnp.bfloat16
            )
            logs.append(jnp.log(total) + row_max[2 * slot + m] * math.log(2.0))
        turned = jnp.where(column == 0, logs[0], logs[1]).T
        pl_send[at_row] = turned[:2, :]
        if mirrored:
            to = half_planes + mirror
            settle(
                q,
                p_copies(q, mirrored),
                [(p_all, to, p_send.at[at_row]), (pl_all, to, pl_send.at[at_row])],
            )
        else:
            for copy in p_copies(q, mirrored):
                copy.start()

    def finalize(q, mirrored):
        slot = slot_of(q, mirrored)
        head = mirror if mirrored else plane
        maps = []
        logs = []
        for m in range(2):
            held = accum[2 * slot + m]
            total = held[:, lanes:]
            maps.append(held[:, :lanes] / total)
            logs.append(jnp.log(total) + row_max[2 * slot + m] * math.log(2.0))
        diff = maps[0] - lambda_of(head) * maps[1]
        mean = jnp.mean(diff * diff, axis=-1, keepdims=True)
        o_send[slot] = (diff * lax.rsqrt(mean + 1e-05)).astype(jnp.bfloat16)
        turned = jnp.where(column == 0, logs[0], logs[1]).T
        lt_send[slot] = turned[:2, :]
        settle(
            q,
            o_copies(q, mirrored),
            [(o_all, head, o_send.at[slot]), (lt_all, head, lt_send.at[slot])],
        )

    def q_arrived(slot):
        arrived(q_all.at[slot], q_r.at[slot])

    def convolve():
        small[3].wait()

        @pl.when(s > 0)
        def _():
            arrived(tail_in, tail_sem.at[1])

        @pl.when(s == 0)
        def _():
            tail_in[...] = jnp.zeros(tail_in.shape, jnp.bfloat16)

        lead = extended.shape[0] - rows
        extended[0:lead, :] = tail_in[tail - lead :, :].astype(jnp.float32)
        extended[lead:, :] = inner_sig[...].astype(jnp.float32)
        tap_count = taps_ref.shape[0]
        convolved = jnp.zeros((rows, local), jnp.float32)
        for position in range(tap_count):
            offset = lead - (tap_count - 1) + position
            convolved = convolved + taps_ref[position : position + 1, :] * extended[
                offset : offset + rows, :
            ]
        conv_out[...] = (outer[...].astype(jnp.float32) * convolved).astype(jnp.bfloat16)
        weight_copies[len(sources)].wait()
        conv_part[...] = jnp.dot(
            conv_out[...], wc_vmem[...], preferred_element_type=jnp.float32
        )

    def turn(i):
        return own_base + lax.rem(plane - own_base + jnp.where(home, 1, 0) + i, half_planes)

    def meet_mirror():
        for k in range(1, half_planes):
            receive(near(k))
        forward_square(spare)

    @pl.when(high)
    def _():
        meet_mirror()
        for k in range(half_planes + 1, heads):
            receive(order(k))

    for k in range(half_planes):
        finish_plane(order(k))

    @pl.when(low)
    def _():
        for slot in far_slots():
            q_arrived(slot)

        @pl.loop(half_planes, heads)
        def _(q):
            attend_row(q)
            partial(q, False)

    @pl.when(low)
    def _():
        meet_mirror()

    away_only(lambda: q_arrived(plane))
    for k in range(1, half_planes):
        q_arrived(order(k))
    attend_triangle(own_base)

    @pl.when(high)
    def _():
        forward_square(mirror)

    @pl.when(low)
    def _():
        @pl.loop(0, half_planes)
        def _(i):
            finalize(turn(i), False)

    convolve()

    @pl.when(high)
    def _():
        finish_plane(mirror)
        attend([(half_planes + i, mirror, False) for i in range(half_planes)])

    for k in range(1, half_planes):
        forward_square(near(k))

    @pl.when(high)
    def _():
        for k in range(half_planes + 1, heads):
            forward_square(order(k))


    for k in range(half_planes):
        finish_plane(near(k))
        if k == 0:
            away_only(lambda: q_arrived(spare))
        else:
            q_arrived(near(k))
    @pl.loop(0, half_planes)
    def _(i):
        q = turn(i)
        for row in range(half_planes):

            @pl.when(q - own_base == row)
            def _(row=row):
                attend([(heads + row, heads + c, c == row) for c in range(row + 1)])

        @pl.when(low)
        def _():
            finalize(q, True)

        @pl.when(high)
        def _():
            partial(q, True)

    @pl.when(high)
    def _():
        for slot in far_slots()[1:]:
            finish_plane(slot)

        attend(
            [
                (half_planes + i, slot, False)
                for slot in far_slots()[1:]
                for i in range(half_planes)
            ]
        )

        @pl.loop(0, half_planes)
        def _(i):
            finalize(turn(i), False)

    weight_copies[len(sources) + 1].wait()
    half_rows = rows // 2

    def from_worker(j, here):
        @pl.when((t != y) | (plane != here))
        def _():
            arrived(o_all.at[j], o_r.at[j])
            arrived(lt_all.at[j], lt_r.at[j])

    def whole(h):
        totals_ref[h] = lt_all[h]
        part = slice(h * lanes, (h + 1) * lanes)
        head_out[:, part] = (o_all[h].astype(jnp.float32) * opened[:, part]).astype(jnp.bfloat16)

    def merged(h):
        arrived(p_all.at[h], p_r.at[h])
        arrived(pl_all.at[h], pl_r.at[h])
        second = half_planes + h

        @pl.when((t != y) | (h != mirror))
        def _():
            arrived(p_all.at[second], p_r.at[second])
            arrived(pl_all.at[second], pl_r.at[second])

        top = jnp.maximum(pl_all[h], pl_all[second])
        shares = [jnp.exp(pl_all[h] - top), jnp.exp(pl_all[second] - top)]
        total = shares[0] + shares[1]
        totals_ref[h] = top + jnp.log(total)
        turned = jnp.concatenate(
            [shares[0] / total, shares[1] / total, jnp.zeros((4, rows), jnp.float32)], axis=0
        ).T
        maps = []
        for m in range(2):
            held = slice(m * rows, (m + 1) * rows)
            maps.append(
                turned[:, m : m + 1] * p_all[h, held, :].astype(jnp.float32)
                + turned[:, 2 + m : 3 + m] * p_all[second, held, :].astype(jnp.float32)
            )
        own_lam = jnp.sum(jnp.where(lam_index == h, lam_own[...], 0.0), axis=-1, keepdims=True)
        diff = maps[0] - own_lam * maps[1]
        mean = jnp.mean(diff * diff, axis=-1, keepdims=True)
        part = pl.ds(pl.multiple_of(h * lanes, lanes), lanes)
        head_out[:, part] = (diff * lax.rsqrt(mean + 1e-05) * opened[:, part]).astype(
            jnp.bfloat16
        )

    split = half_planes * lanes

    @pl.when(low)
    def _():
        for h in range(half_planes):
            from_worker(h, h)
            whole(h)

    @pl.when(high)
    def _():
        @pl.loop(0, half_planes)
        def _(i):
            merged(lax.rem(mirror + i, half_planes))

    conv_part[...] += jnp.dot(
        head_out[:, :split], wo_vmem[:split, :], preferred_element_type=jnp.float32
    )
    for h in range(half_planes, heads):

        @pl.when(low)
        def _(h=h):
            from_worker(h, heads - 1 - h)

        @pl.when(high)
        def _(h=h):
            from_worker(h, h)

        whole(h)

    pieces, _, breadth = part_send.shape

    def partial_rows(which, piece):
        there = pl.ds(pl.multiple_of(which * half_rows, half_rows), half_rows)
        columns = slice(piece * breadth, (piece + 1) * breadth)
        attn = jnp.dot(
            head_out[there, split:], wo_vmem[split:, columns], preferred_element_type=jnp.float32
        )
        return (attn + conv_part[there, columns]).astype(jnp.bfloat16)

    exchanges = [
        remote(part_send.at[i], part_recv.at[i], part_sem.at[i], part_sem.at[pieces + i], c_dev)
        for i in range(pieces)
    ]
    for i in range(pieces):
        part_send[i] = partial_rows(1 - t, i)
        exchanges[i].start()
    for i in range(pieces):
        own_rows = partial_rows(t, i).astype(jnp.float32)
        exchanges[i].wait()
        mixed_ref[:, i * breadth : (i + 1) * breadth] = (
            own_rows + part_recv[i].astype(jnp.float32)
        ).astype(jnp.bfloat16)

    def drain(slot):
        along_x(slot).wait_send()
        across(slot).wait_send()
        onward(slot).wait_send()

    def drain_o(q, copies):
        @pl.when((q != plane) | (t != y))
        def _():
            for copy in copies:
                copy.wait_send()

    for k in range(half_planes):

        def sent(k=k):
            kv_copy(order(k)).wait_send()
            q_copy(order(k)).wait_send()
            kv_mirror(k).wait_send()
            q_mirror(k).wait_send()

        if k == 0:
            away_only(sent)
        else:
            sent()
        drain(order(k))
        drain(near(k))

    @pl.when(low)
    def _():
        for slot in far_slots():
            kv_copy(slot).wait_send()
        for q in range(half_planes):
            drain_o(q, o_copies(q, False))
            drain_o(q, o_copies(q, True))
            for copy in p_copies(half_planes + q, False):
                copy.wait_send()

    @pl.when(high)
    def _():
        for slot in far_slots():
            q_copy(slot).wait_send()
            drain(slot)
        for q in range(half_planes, heads):
            drain_o(q, o_copies(q, False))
            drain_o(q, p_copies(q, True))

    @pl.when(s < last)
    def _():
        tail_copy.wait_send()


def fused(sp_count, *args):
    tokens, norm_gain, wq = args[0], args[1], args[2]
    lambdas, head_gain = args[10], args[11]
    rows, half = tokens.shape
    heads = lambdas.shape[0]
    local = wq.shape[1]
    lanes = local // heads
    slots = heads + heads // 2
    out_width = args[12].shape[1]
    bf16, f32 = jnp.bfloat16, jnp.float32
    vmem = pl.BlockSpec(memory_space=pltpu.VMEM)
    hbm = pl.BlockSpec(memory_space=pl.ANY)
    dma = pltpu.SemaphoreType.DMA
    operands = list(args)
    operands[1] = norm_gain.reshape(1, -1)
    operands[10] = lambdas.reshape(1, -1)
    operands[11] = head_gain.reshape(1, -1)
    return pl.pallas_call(
        functools.partial(fused_kernel, sp_count, heads),
        out_shape=(
            pltpu.VMEM((rows // 2, out_width), bf16),
            pltpu.VMEM((heads, 2, rows), f32),
        ),
        in_specs=[hbm] * len(operands),
        out_specs=(vmem, vmem),
        scratch_shapes=[
            pltpu.VMEM((rows, half), bf16),
            pltpu.VMEM((rows, half), bf16),
            pltpu.VMEM((1, 2 * half), f32),
            pltpu.VMEM(args[9].shape, f32),
            pltpu.VMEM((1, local), f32),
            pltpu.VMEM((1, heads), f32),
            pltpu.VMEM((1, heads), f32),
            pltpu.VMEM((rows, 2 * half), bf16),
            pltpu.VMEM((7,) + wq.shape, bf16),
            pltpu.VMEM(args[12].shape, bf16),
            pltpu.VMEM(args[13].shape, bf16),
            pltpu.VMEM((heads, rows, 2 * lanes), bf16),
            pltpu.VMEM((heads, rows, lanes), bf16),
            pltpu.VMEM((slots * RELAY, rows, 2 * lanes), bf16),
            pltpu.VMEM((slots, rows, lanes), bf16),
            pltpu.VMEM((2 * slots, rows, lanes), f32),
            pltpu.VMEM((2 * slots, rows, 2 * lanes), f32),
            pltpu.VMEM((rows, local), f32),
            pltpu.VMEM((rows, local), bf16),
            pltpu.VMEM((rows, local), bf16),
            pltpu.VMEM((16, local), bf16),
            pltpu.VMEM((rows + 8, local), f32),
            pltpu.VMEM((rows, local), bf16),
            pltpu.VMEM((rows, local), bf16),
            pltpu.VMEM((rows, out_width), f32),
            pltpu.VMEM((slots, rows, lanes), bf16),
            pltpu.VMEM((heads, rows, lanes), bf16),
            pltpu.VMEM((slots, 2, rows), f32),
            pltpu.VMEM((heads, 2, rows), f32),
            pltpu.VMEM((heads // 2, 2 * rows, lanes), bf16),
            pltpu.VMEM((heads, 2 * rows, lanes), bf16),
            pltpu.VMEM((heads // 2, 2, rows), f32),
            pltpu.VMEM((heads, 2, rows), f32),
            pltpu.VMEM((PIECES, rows // 2, out_width // PIECES), bf16),
            pltpu.VMEM((PIECES, rows // 2, out_width // PIECES), bf16),
            dma((9,)),
            dma((5,)),
            dma((4,)),
            dma((2,)),
            dma((2 * PIECES,)),
        ]
        + [dma((slots,)) for _ in range(18)]
        + [pltpu.SemaphoreType.REGULAR, pltpu.SemaphoreType.REGULAR],
        compiler_params=pltpu.CompilerParams(
            collective_id=0, has_side_effects=True, vmem_limit_bytes=58000 * 1024
        ),
    )(*operands)


def fits_square(mesh, heads, rows, key_columns, value_columns):
    return (
        mesh.shape["tp"] == 2
        and mesh.shape["sp"] == heads * RELAY
        and heads > 1
        and heads % 2 == 0
        and rows % 32 == 0
        and key_columns == value_columns == heads * 128
    )


def solution(mesh):
    placed = (
        P("sp", "tp"),
        P(),
        P(None, "tp"),
        P(None, "tp"),
        P(None, "tp"),
        P(None, "tp"),
        P(None, "tp"),
        P(None, "tp"),
        P(None, "tp"),
        P(None, "tp"),
        P("tp"),
        P("tp"),
        P("tp", None),
        P("tp", None),
    )

    def step(*args):
        heads = args[10].shape[0]
        if fits_square(mesh, heads, args[0].shape[0], args[2].shape[1], args[4].shape[1]):
            return fused(mesh.shape["sp"], *args)
        return per_device(*args)

    return jax.shard_map(
        step,
        mesh=mesh,
        in_specs=placed,
        out_specs=(P(("sp", "tp"), None), P("tp", None, "sp")),
        check_vma=False,
    )
```
